256 devices in a mesh: sp: 64 (over z, y, core), tp: 4 (over x).
Axes of the slice: x: 4, y: 4, z: 8, core: 2. Of those that a mesh axis runs over, the one named last changes fastest.
Arguments:
- cotangent: bfloat16 [8192, 2048], P('sp', 'tp'), may hold values from -16 to 16
- mixer_out: bfloat16 [8192, 2048], P('sp', 'tp'), may hold values from -6 to 6
- route_ids: int32 [8192, 2], P('sp'), may hold values from 0 to 63, all different within a row; in each aligned block of 128 rows (0 to 127, 128 to 255, ...) at most 8 rows name the same one
- route_weights: float32 [8192, 2], P('sp'), may hold values from 0.2 to 1
- conv_out: bfloat16 [8192, 2048], P('sp', 'tp'), may hold values from -6 to 6
- recur_gate: bfloat16 [8192, 2048], P('sp', 'tp'), may hold values from 0.007 to 1
- input_gate: bfloat16 [8192, 2048], P('sp', 'tp'), may hold values from 0.099609375 to 0.8984375
- gate_pre: bfloat16 [8192, 2048], P('sp', 'tp'), may hold values from -6 to 6
- states_before: bfloat16 [8192, 2048], P('sp', 'tp'), may hold values from -4 to 4
- decay_rate: float32 [2048], P('tp'), may hold values from 4e-07 to 0.008
- out_proj: bfloat16 [2048, 2048], P(None, 'tp'), may hold values from -0.125 to 0.125
- recur_map: bfloat16 [4, 512, 512], P('tp'), may hold values from -0.25 to 0.25
- input_map: bfloat16 [4, 512, 512], P('tp'), may hold values from -0.25 to 0.25
- expert_gate: bfloat16 [64, 2048, 1024], P('sp', None, 'tp'), may hold values from -0.125 to 0.125
- expert_up: bfloat16 [64, 2048, 1024], P('sp', None, 'tp'), may hold values from -0.125 to 0.125
- expert_down: bfloat16 [64, 1024, 2048], P('sp', 'tp'), may hold values from -0.1875 to 0.1875
Outputs:
- grad_expert_gate: bfloat16 [64, 2048, 1024], P('sp', None, 'tp')
- grad_expert_up: bfloat16 [64, 2048, 1024], P('sp', None, 'tp')
- grad_expert_down: bfloat16 [64, 1024, 2048], P('sp', 'tp')
- grad_out_proj: float32 [2048, 2048], P('sp', 'tp')
- grad_conv: bfloat16 [8192, 2048], P('sp', 'tp')
- grad_gate_pre: bfloat16 [8192, 2048], P('sp', 'tp')
The draws below stay inside these ranges and needn't reach their ends.
Inputs may be any that keep to these rules, and one draw needn't show every extreme that they name: `route_ids`: the two experts of a token differ. In every aligned block of 128 tokens no expert is named by more than 8 routes, and in some block some expert by exactly 8.
All inputs are finite; a program needn't handle non-finite values.
Results may differ from the reference program's by a relative error of at most 0.0093.
Values may be sent and summed in bfloat16 or wider, within the bound.
A program may use at most 64 MiB of HBM per device.

```python
import math
import jax
import jax.numpy as jnp
import numpy as np
from jax import lax

D = 2048
LRU = 2048
BLOCKS = 4
BLOCK_W = 512
FF = 1024
TOK_DEV = 128
TOKENS = 8192
EXPERTS = 64
CAP = 8
N_SP = 64


def draw_recur_gate(key, part):
    key_one, key_two = jax.random.split(key)
    span_count = TOKENS // 128
    base_gate = jax.random.uniform(key_one, (TOKENS, LRU), jnp.float32, 0.5, 1.0)
    factor = jnp.exp(jax.random.uniform(key_two, (span_count, 1, 1), jnp.float32, math.log(0.15), 0.0))
    return (base_gate.reshape(span_count, 128, LRU) * factor).reshape(TOKENS, LRU).astype(jnp.bfloat16)


def draw_decay_rate(key, part):
    key_one, key_two, key_three = jax.random.split(key, 3)
    fast_share = 0.5
    fast_mask = jax.random.bernoulli(key_one, fast_share, (LRU,))
    slow_rate = jnp.exp(jax.random.uniform(key_two, (LRU,), jnp.float32, math.log(0.03), math.log(0.25))) / TOKENS
    fast_rate = jnp.exp(jax.random.uniform(key_three, (LRU,), jnp.float32, math.log(0.002), math.log(0.008)))
    return jnp.where(fast_mask, fast_rate, slow_rate).astype(jnp.float32)


def with_spikes(entries, own_key, source, target, shards_of, factor):
    owner, partner = [(jnp.arange(entries.shape[axis_at]) // (entries.shape[axis_at] // shards_of)).reshape([-1 if axis == axis_at else 1 for axis in range(entries.ndim)]) for axis_at in (source, target)]
    chosen = jax.random.permutation(own_key, shards_of)[partner]
    strong = (owner == chosen) | (owner == (partner + shards_of // 2) % shards_of)
    return jnp.where(strong, factor * entries, entries)


def steps_of(own_key, extent, cuts, smallest, largest):
    level, own = 1.0, jax.random.fold_in(own_key, 6)
    for position, parts in cuts:
        steps = jnp.exp(jax.random.uniform(jax.random.fold_in(own, position), (parts,), jnp.float32, smallest / len(cuts), largest / len(cuts)))
        level = level * jnp.repeat(steps, extent[position] // parts).reshape([-1 if axis == position else 1 for axis in range(len(extent))])
    return level


def shared_out(rng, own, number, rows, number_of, top, reach, skew):
    order = jax.random.permutation(rng, number_of)
    packed, ordinary = load_shares(number_of, rows * top, reach, skew, True), load_shares(number_of, rows * top, reach, skew, False)
    places = jnp.arange(number_of)

    def named(tallies, turn):
        used = int((tallies > 0).sum())
        fixed = max(1, used // 4)
        moved = fixed + (places - fixed + turn * (used - fixed)) % max(1, number_of - fixed)
        return jnp.zeros((number_of,), jnp.int32).at[order[jnp.where(places < fixed, places, moved)]].set(jnp.asarray(tallies, jnp.int32))

    tallies = jnp.where(number % 4 == 0, named(packed, number // 4), named(ordinary, number - number // 4 - 1))
    mixed = jax.random.permutation(jax.random.fold_in(own, 3), number_of)
    donor, taker = mixed[0:number_of // 2 * 2:2], mixed[1:number_of // 2 * 2:2]
    margin = jnp.minimum(tallies[donor] - 1, reach - tallies[taker]) // 2
    margin = jnp.where((donor == order[0]) | (taker == order[0]) | (tallies[taker] == 0), 0, jnp.maximum(margin, 0))
    moved = jax.random.randint(jax.random.fold_in(own, 4), (number_of // 2,), 0, 1 << 20) % (margin + 1)
    tallies = tallies.at[donor].add(-moved).at[taker].add(moved)
    items = jnp.searchsorted(jnp.cumsum(tallies), jnp.arange(rows * top), side="right").astype(jnp.int32)
    listing = items.reshape(top, rows).T
    listing = listing[jax.random.permutation(jax.random.fold_in(own, 1), rows)]
    turn = jax.random.randint(jax.random.fold_in(own, 2), (rows, 1), 0, top)
    return jnp.take_along_axis(listing, (jnp.arange(top)[None, :] + turn) % top, axis=1)


def load_shares(amount, total, limit, lean, full):
    loads = [(1 << 20) // math.isqrt(standing ** lean) + 1 for standing in range(1, amount + 1)]
    largest = limit if full else min(limit, max(-(-total // amount), total * loads[0] // sum(loads)))
    least = 1 if total - largest >= amount - 1 else 0
    given, rest = [largest] + [least] * (amount - 1), total - largest - least * (amount - 1)
    while rest > 0:
        free = [i for i in range(1, amount) if given[i] < largest] or [i for i in range(1, amount) if given[i] < limit]
        mass, left = sum([loads[i] for i in free]), rest
        for i in free:
            extra = min(limit - given[i], max(1, left * loads[i] // mass), rest)
            given[i] = given[i] + extra
            rest = rest - extra
    return np.array(given)


def scatter_about(stream_key, dims, deviation, reach, cuts=(), held_as=jnp.bfloat16):
    loudness = steps_of(stream_key, dims, cuts, -0.22, 0.18) if cuts else 1.0
    values = jax.random.normal(stream_key, dims, jnp.float32) * deviation * loudness
    return jnp.minimum(jnp.maximum(values, -reach), reach).astype(held_as)


def noise_with(own_key, dims, width, reach, shards, heavy, kind=jnp.bfloat16):
    array = width * jax.random.normal(own_key, dims, jnp.float32)
    if shards:
        array = array * steps_of(own_key, dims, shards, -0.22, 0.18)
    return jnp.clip(with_spikes(array, jax.random.fold_in(own_key, 3), *heavy), -reach, reach).astype(kind)


def setup_inputs(seed: int = 0) -> dict:
    key_list = jax.random.split(jax.random.key(seed), 17)
    cotangent = noise_with(key_list[0], (TOKENS, D), 1.0, 16.0, ((0, 64), (1, 4)), (0, 1, 64, 4.0))
    mixer_out = scatter_about(key_list[1], (TOKENS, D), 1.0, 6.0, ((0, 64), (1, 4)))
    route_ids_keys = jax.random.split(jax.random.fold_in(key_list[2], 1), TOKENS // TOK_DEV)
    route_ids_turns = jax.random.permutation(jax.random.fold_in(key_list[2], 3), TOKENS // TOK_DEV)
    route_ids = jax.vmap(lambda own, number: shared_out(jax.random.fold_in(key_list[2], 2), own, number, TOK_DEV, EXPERTS, 2, CAP, 2))(route_ids_keys, route_ids_turns).reshape((TOKENS, 2))
    route_weights = jnp.clip(0.2 + 0.8 * jax.random.uniform(key_list[3], (TOKENS, 2), jnp.float32) ** steps_of(key_list[3], (TOKENS, 2), ((0, 64),), -0.2, 0.2), 0.2, 1.0)
    conv_out = scatter_about(key_list[4], (TOKENS, LRU), 1.0, 6.0, ((0, 64), (1, 4)))
    recur_gate = draw_recur_gate(jax.random.fold_in(key_list[16], 71), 0)
    input_gate = jnp.clip(0.099609375 + 0.7988281 * jax.random.uniform(key_list[6], (TOKENS, LRU), jnp.float32) ** steps_of(key_list[6], (TOKENS, LRU), ((0, 64), (1, 4)), -0.2, 0.2), 0.099609375, 0.8984375).astype(jnp.bfloat16)
    gate_pre = scatter_about(key_list[7], (TOKENS, LRU), 1.0, 6.0, ((0, 64), (1, 4)))
    states_before = scatter_about(key_list[8], (TOKENS, LRU), 0.5, 4.0, ((0, 64), (1, 4)))
    decay_rate = draw_decay_rate(jax.random.fold_in(key_list[16], 71), 0)
    out_proj = scatter_about(key_list[10], (D, LRU), LRU ** -0.5, 0.125, ((1, 4),))
    recur_map = scatter_about(key_list[11], (BLOCKS, BLOCK_W, BLOCK_W), BLOCK_W ** -0.5, 0.25, ((0, 4),))
    input_map = scatter_about(key_list[12], (BLOCKS, BLOCK_W, BLOCK_W), BLOCK_W ** -0.5, 0.25, ((0, 4),))
    expert_gate = scatter_about(key_list[13], (EXPERTS, D, FF), D ** -0.5, 0.125, ((0, 64), (2, 4)))
    expert_up = scatter_about(key_list[14], (EXPERTS, D, FF), D ** -0.5, 0.125, ((0, 64), (2, 4)))
    expert_down = scatter_about(key_list[15], (EXPERTS, FF, D), FF ** -0.5, 0.1875, ((0, 64), (1, 4)))
    return dict(cotangent=cotangent, mixer_out=mixer_out, route_ids=route_ids, route_weights=route_weights, conv_out=conv_out, recur_gate=recur_gate, input_gate=input_gate, gate_pre=gate_pre, states_before=states_before, decay_rate=decay_rate, out_proj=out_proj, recur_map=recur_map, input_map=input_map, expert_gate=expert_gate, expert_up=expert_up, expert_down=expert_down)


def silu_parts(values):
    sig = jax.nn.sigmoid(values)
    return (values * sig, sig * (1.0 + values * (1.0 - sig)))

def route_slots(route_block):
    flat_ids = route_block.reshape(-1)
    onehot = (flat_ids[:, None] == jnp.arange(EXPERTS, dtype=jnp.int32)[None, :]).astype(jnp.int32)
    before = jnp.cumsum(onehot, axis=0) - onehot
    slot_rank = lax.optimization_barrier(jnp.sum(before * onehot, axis=1))
    return (flat_ids * CAP + slot_rank).astype(jnp.int32)

def link_steps(earlier, later):
    return (earlier[0] * later[0], later[0] * earlier[1] + later[1])

def reference(cotangent, mixer_out, route_ids, route_weights, conv_out, recur_gate, input_gate, gate_pre, states_before, decay_rate, out_proj, recur_map, input_map, expert_gate, expert_up, expert_down):
    slot_pos = jax.vmap(route_slots)(route_ids.reshape(N_SP, TOK_DEV, 2))
    expert_of = slot_pos // CAP
    slot_rank = slot_pos % CAP
    source = jnp.arange(N_SP, dtype=jnp.int32)[:, None]
    place = (expert_of * (N_SP * CAP) + source * CAP + slot_rank).astype(jnp.int32).reshape(-1)
    token_of = (source * TOK_DEV + jnp.arange(2 * TOK_DEV, dtype=jnp.int32)[None, :] // 2).astype(jnp.int32)
    table = jnp.full((EXPERTS * N_SP * CAP,), TOKENS, jnp.int32).at[place].set(token_of.reshape(-1))
    slot_weight = jnp.zeros((EXPERTS * N_SP * CAP,), jnp.float32).at[place].set(route_weights.astype(jnp.float32).reshape(-1))
    table = table.reshape(EXPERTS, N_SP * CAP)
    slot_weight = slot_weight.reshape(EXPERTS, N_SP * CAP)
    x_padded = jnp.concatenate([mixer_out, jnp.zeros((1, D), jnp.bfloat16)], axis=0)
    g_padded = jnp.concatenate([cotangent, jnp.zeros((1, D), jnp.bfloat16)], axis=0)

    def expert_step(routed_sum, inputs):
        row_index, weight, w_gate, w_up, w_down = inputs
        row_data = x_padded[row_index]
        routed_cot = (g_padded[row_index].astype(jnp.float32) * weight[:, None]).astype(jnp.bfloat16)
        pre_gate = jnp.dot(row_data, w_gate, preferred_element_type=jnp.float32)
        pre_up = jnp.dot(row_data, w_up, preferred_element_type=jnp.float32)
        gate_act, slope = silu_parts(pre_gate)
        active = (gate_act * pre_up).astype(jnp.bfloat16)
        d_active = jnp.dot(routed_cot, w_down.T, preferred_element_type=jnp.float32)
        grad_down = jnp.dot(active.T, routed_cot, preferred_element_type=jnp.float32).astype(jnp.bfloat16)
        d_gate = (d_active * pre_up * slope).astype(jnp.bfloat16)
        d_up = (d_active * gate_act).astype(jnp.bfloat16)
        grad_gate = jnp.dot(row_data.T, d_gate, preferred_element_type=jnp.float32).astype(jnp.bfloat16)
        grad_up = jnp.dot(row_data.T, d_up, preferred_element_type=jnp.float32).astype(jnp.bfloat16)
        route_grad = (jnp.dot(d_gate, w_gate.T, preferred_element_type=jnp.float32) + jnp.dot(d_up, w_up.T, preferred_element_type=jnp.float32)).astype(jnp.bfloat16)
        routed_sum = routed_sum.at[row_index].add(route_grad.astype(jnp.float32))
        return (routed_sum, (grad_gate, grad_up, grad_down))
    routed_sum, expert_grads = lax.scan(expert_step, jnp.zeros((TOKENS + 1, D), jnp.float32), (table, slot_weight, expert_gate, expert_up, expert_down))
    grad_expert_gate, grad_expert_up, grad_expert_down = expert_grads
    out_grad = (cotangent.astype(jnp.float32) + routed_sum[:TOKENS]).astype(jnp.bfloat16)
    rate = decay_rate.astype(jnp.float32)[None, :]
    recur_f = recur_gate.astype(jnp.float32)
    input_f = input_gate.astype(jnp.float32)
    conv_f = conv_out.astype(jnp.float32)
    before_f = states_before.astype(jnp.float32)
    log_decay = -8.0 * recur_f * rate
    decay_now = jnp.exp(log_decay)
    at_start = (jnp.arange(TOKENS, dtype=jnp.int32) == 0)[:, None]
    norm_factor = jnp.where(at_start, 1.0, jnp.sqrt(-jnp.expm1(2.0 * log_decay)))
    norm_slope = jnp.where(at_start, 0.0, -jnp.exp(2.0 * log_decay) / norm_factor)
    drive = input_f * conv_f
    state = decay_now * before_f + norm_factor * drive
    gate, gelu_back = jax.vjp(jax.nn.gelu, gate_pre.astype(jnp.float32))
    mixed = (state * gate).astype(jnp.bfloat16)
    d_mixed = jnp.dot(out_grad, out_proj, preferred_element_type=jnp.float32)
    grad_out_proj = jnp.dot(out_grad.T, mixed, preferred_element_type=jnp.float32)
    grad_gate_pre = gelu_back(d_mixed * state)[0].astype(jnp.bfloat16)
    decay_next = jnp.concatenate([decay_now[1:], jnp.ones((1, LRU), jnp.float32)], axis=0)
    _, state_grad = lax.associative_scan(link_steps, (decay_next, d_mixed * gate), axis=0, reverse=True)
    d_log = state_grad * (decay_now * before_f + norm_slope * drive)
    d_recur_pre = (d_log * (-8.0 * rate) * recur_f * (1.0 - recur_f)).astype(jnp.bfloat16)
    d_input_pre = (state_grad * norm_factor * conv_f * input_f * (1.0 - input_f)).astype(jnp.bfloat16)
    through_recur = jnp.einsum('tbj,bij->tbi', d_recur_pre.astype(jnp.float32).reshape(TOKENS, BLOCKS, BLOCK_W), recur_map.astype(jnp.float32))
    through_input = jnp.einsum('tbj,bij->tbi', d_input_pre.astype(jnp.float32).reshape(TOKENS, BLOCKS, BLOCK_W), input_map.astype(jnp.float32))
    grad_conv = (state_grad * norm_factor * input_f + (through_recur + through_input).reshape(TOKENS, LRU)).astype(jnp.bfloat16)
    return (grad_expert_gate, grad_expert_up, grad_expert_down, grad_out_proj, grad_conv, grad_gate_pre)
```

```python
import functools

import jax
import jax.numpy as jnp
from jax import lax
from jax.experimental import pallas as pl
from jax.experimental.pallas import tpu as pltpu
from jax.sharding import Mesh
from jax.sharding import PartitionSpec as P

SP = ("sp_0", "sp_1", "sp_2")


MESH_ID = pl.DeviceIdType.MESH
AXES = (*SP, "tp")


def near_first(count):
    return sorted(range(count), key=lambda k: (min(k, count - k), k))


def slot_hits(ids, experts, capacity):
    tokens = ids.shape[1]
    slots = experts * capacity
    first, second = ids[0:1, :], ids[1:2, :]
    expert = lax.broadcasted_iota(jnp.int32, (experts, tokens), 0)
    named = jnp.where((expert == first) | (expert == second), 1.0, 0.0).astype(jnp.bfloat16)
    at = lax.broadcasted_iota(jnp.int32, (tokens, tokens), 0)
    later = lax.broadcasted_iota(jnp.int32, (tokens, tokens), 1)
    earlier = jnp.where(at < later, 1.0, 0.0).astype(jnp.bfloat16)
    before = jnp.dot(named, earlier, preferred_element_type=jnp.float32)
    of_slot = lax.broadcasted_iota(jnp.int32, (slots, experts), 0)
    of_expert = lax.broadcasted_iota(jnp.int32, (slots, experts), 1)
    spread = jnp.where(of_slot // capacity == of_expert, 1.0, 0.0).astype(jnp.bfloat16)
    rank = jnp.dot(spread, before.astype(jnp.bfloat16), preferred_element_type=jnp.float32)
    slot = lax.broadcasted_iota(jnp.int32, (slots, tokens), 0)
    free = rank == (slot % capacity).astype(jnp.float32)
    return free & (slot // capacity == first), free & (slot // capacity == second)


def dispatch_kernel(
    sizes, ids_ref, weights_ref, mixer_ref, cot_ref, rows_ref, cots_ref, hits_ref,
    send_rows, send_cots, a_send, a_recv, own_send, own_recv, pass_send, pass_recv, met,
):
    nz, ny, nc, nx = sizes
    plane = ny * nc
    z, y, c, x = (lax.axis_index(a) for a in AXES)
    width = cot_ref.shape[1]
    right, left = lax.rem(x + 1, nx), lax.rem(x + nx - 1, nx)
    across = lax.rem(x + 2, nx)
    me = (z * ny + y) * nc + c

    def partner(j, sign):
        dz, dy, dc = j // plane, (j // nc) % ny, j % nc
        return (
            lax.rem(z + sign * dz + nz, nz),
            lax.rem(y + sign * dy + ny, ny),
            lax.rem(c + sign * dc + nc, nc),
        )

    barrier = pltpu.get_barrier_semaphore()

    def greet(sem, first, stop, step):
        def one(k, carry):
            pl.semaphore_signal(
                sem, inc=1, device_id=(*partner(k * step, 1), x), device_id_type=MESH_ID
            )
            return carry

        lax.fori_loop(first, stop, one, 0)

    greet(barrier, 1, nz, plane)
    greet(barrier, 1, plane, 1)
    for side in (left, right):
        pl.semaphore_signal(barrier, inc=1, device_id=(z, y, c, side), device_id_type=MESH_ID)

    experts = nz * plane
    first, second = slot_hits(ids_ref[...], experts, rows_ref.shape[1])
    hits = jnp.where(first | second, 1.0, 0.0).astype(jnp.bfloat16)
    hits_ref[...] = hits
    weights = weights_ref[...]
    weight = jnp.sum(
        jnp.where(first, weights[0:1, :], 0.0) + jnp.where(second, weights[1:2, :], 0.0),
        axis=1,
        keepdims=True,
    )
    shape = send_rows.shape
    rows = jnp.dot(hits, mixer_ref[...], preferred_element_type=jnp.float32)
    send_rows[...] = rows.reshape(shape).astype(jnp.bfloat16)
    cots = jnp.dot(hits, cot_ref[...], preferred_element_type=jnp.float32) * weight
    send_cots[...] = cots.reshape(shape).astype(jnp.bfloat16)

    pl.semaphore_wait(barrier, nz - 1 + plane - 1 + 2)
    greet(met, 1, plane, 1)
    pl.semaphore_wait(met, plane - 1)

    def columns(part):
        return pl.ds(pl.multiple_of(part * width, width), width)

    pairs = ((send_rows, rows_ref), (send_cots, cots_ref))

    def local(k):
        source, target = pairs[k]
        return pltpu.make_async_copy(
            source.at[me], target.at[me, :, columns(x)], a_recv.at[k, 0]
        )

    def sent(k, j):
        dz, dy, dc = partner(j, 1)
        source, target = pairs[k]
        return pltpu.make_async_remote_copy(
            src_ref=source.at[(dz * ny + dy) * nc + dc],
            dst_ref=target.at[me, :, columns(x)],
            send_sem=a_send.at[k, j],
            recv_sem=a_recv.at[k, j],
            device_id=(dz, dy, dc, x),
            device_id_type=MESH_ID,
        )

    def arriving(k, j):
        sz, sy, sc = partner(j, -1)
        source, target = pairs[k]
        return pltpu.make_async_remote_copy(
            src_ref=source.at[me],
            dst_ref=target.at[(sz * ny + sy) * nc + sc, :, columns(x)],
            send_sem=a_send.at[k, j],
            recv_sem=a_recv.at[k, j],
            device_id=(sz, sy, sc, x),
            device_id_type=MESH_ID,
        )

    for k in (0, 1):
        local(k).start()
    order = near_first(nz)
    for dz in order:

        def send(j, carry):
            for k in (0, 1):
                sent(k, j).start()
            return carry

        lax.fori_loop(max(dz * plane, 1), (dz + 1) * plane, send, 0)

    def block(ref, dz, half, part):
        start = lax.rem(z - dz + nz, nz) * plane
        count = plane
        if half is not None:
            count = plane // 2
            start = start + half * count
        return ref.at[pl.ds(start, count), :, columns(part)]

    def own(k, dz, way):
        ref = pairs[k][1]
        here = block(ref, dz, None, x)
        return pltpu.make_async_remote_copy(
            src_ref=here,
            dst_ref=here,
            send_sem=own_send.at[way, k, dz],
            recv_sem=own_recv.at[way, k, dz],
            device_id=(z, y, c, (right, left)[way]),
            device_id_type=MESH_ID,
        )

    def own_here(k, dz, way):
        ref = pairs[k][1]
        here = block(ref, dz, None, (left, right)[way])
        return pltpu.make_async_remote_copy(
            src_ref=here,
            dst_ref=here,
            send_sem=own_send.at[way, k, dz],
            recv_sem=own_recv.at[way, k, dz],
            device_id=(z, y, c, (left, right)[way]),
            device_id_type=MESH_ID,
        )

    def passed(k, dz, way):
        ref = pairs[k][1]
        here = block(ref, dz, way, (left, right)[way])
        return pltpu.make_async_remote_copy(
            src_ref=here,
            dst_ref=here,
            send_sem=pass_send.at[way, k, dz],
            recv_sem=pass_recv.at[way, k, dz],
            device_id=(z, y, c, (right, left)[way]),
            device_id_type=MESH_ID,
        )

    def passed_here(k, dz, way):
        ref = pairs[k][1]
        here = block(ref, dz, way, across)
        return pltpu.make_async_remote_copy(
            src_ref=here,
            dst_ref=here,
            send_sem=pass_send.at[way, k, dz],
            recv_sem=pass_recv.at[way, k, dz],
            device_id=(z, y, c, (left, right)[way]),
            device_id_type=MESH_ID,
        )

    def hand_on(dz):
        for k in (0, 1):
            for way in (0, 1):
                own_here(k, dz, way).wait_recv()
                passed(k, dz, way).start()

    for at, dz in enumerate(order):
        if dz == 0:
            for k in (0, 1):
                local(k).wait()

        def arrive(j, carry):
            for k in (0, 1):
                arriving(k, j).wait_recv()
            return carry

        lax.fori_loop(max(dz * plane, 1), (dz + 1) * plane, arrive, 0)
        for k in (0, 1):
            for way in (0, 1):
                own(k, dz, way).start()
        if at:
            hand_on(order[at - 1])
    hand_on(order[-1])
    for dz in order:
        for k in (0, 1):
            for way in (0, 1):
                passed_here(k, dz, way).wait_recv()

    def drain(j, carry):
        for k in (0, 1):
            sent(k, j).wait_send()
        return carry

    lax.fori_loop(1, nz * plane, drain, 0)
    for dz in order:
        for k in (0, 1):
            for way in (0, 1):
                own(k, dz, way).wait_send()
                passed(k, dz, way).wait_send()


def dispatched(ids, weights, mixer_out, cotangent):
    sizes = tuple(lax.axis_size(a) for a in AXES)
    nz, ny, nc, nx = sizes
    experts = nz * ny * nc
    tokens, width = cotangent.shape
    capacity = 4 * tokens // experts
    full = jax.ShapeDtypeStruct((experts, capacity, nx * width), jnp.bfloat16)
    vmem = pl.BlockSpec(memory_space=pltpu.VMEM)
    dma = pltpu.SemaphoreType.DMA
    return pl.pallas_call(
        functools.partial(dispatch_kernel, sizes),
        out_shape=(full, full, jax.ShapeDtypeStruct((experts * capacity, tokens), jnp.bfloat16)),
        in_specs=[vmem] * 4,
        out_specs=(vmem,) * 3,
        scratch_shapes=[
            pltpu.VMEM((experts, capacity, width), jnp.bfloat16),
            pltpu.VMEM((experts, capacity, width), jnp.bfloat16),
            dma((2, experts)),
            dma((2, experts)),
            dma((2, 2, nz)),
            dma((2, 2, nz)),
            dma((2, 2, nz)),
            dma((2, 2, nz)),
            pltpu.SemaphoreType.REGULAR,
        ],
        compiler_params=pltpu.CompilerParams(collective_id=0, has_side_effects=True),
        name="dispatch",
    )(ids.T, weights.T, mixer_out, cotangent)


def sent_together(arrays, axis, split_dim, concat_dim, along):
    widths = [a.shape[along] for a in arrays]
    both = jnp.concatenate(arrays, axis=along)
    whole = lax.all_to_all(both, axis, split_axis=split_dim, concat_axis=concat_dim, tiled=True)
    return tuple(jnp.split(whole, [sum(widths[:k]) for k in range(1, len(widths))], axis=along))


def laid_out(pieces, dim):
    pieces = jnp.moveaxis(pieces, 0, dim)
    shape = pieces.shape
    return pieces.reshape(*shape[:dim], shape[dim] * shape[dim + 1], *shape[dim + 2 :])


def from_everyone(shard, axis):
    devices = lax.axis_size(axis)
    return lax.all_to_all(
        jnp.broadcast_to(shard[None], (devices, *shard.shape)), axis, 0, 0, tiled=True
    )


def gathered_copies(shard, axis, dim):
    return laid_out(from_everyone(shard, axis), dim)


def side_by_side(arrays, axis, dim, along):
    ends, at = ([], 0)
    for a in arrays[:-1]:
        at += a.shape[along]
        ends.append(at)
    both = jnp.concatenate(arrays, axis=along)
    return tuple(jnp.split(gathered_copies(both, axis, dim), ends, axis=along))


def cut_along(shard, dim, devices):
    before, after = (shard.shape[:dim], shard.shape[dim + 1 :])
    return jnp.moveaxis(shard.reshape(*before, devices, -1, *after), dim, 0)


def sent_and_summed(shard, axis, dim):
    pieces = cut_along(shard, dim, lax.axis_size(axis))
    arrived = lax.all_to_all(pieces, axis, split_axis=0, concat_axis=0, tiled=True)
    return arrived.astype(jnp.float32).sum(axis=0)


def summed_rows(shard, axes, dim):
    far, near = axes
    own = sent_and_summed(cut_along(shard, dim, lax.axis_size(far)), near, dim + 1)
    return jnp.sum(
        lax.all_to_all(own.astype(jnp.bfloat16), far, 0, 0, tiled=True).astype(jnp.float32), axis=0
    )


def all_in_one(shard, axis):
    leaves = jax.tree.leaves(shard)
    order = sorted(range(len(leaves)), key=lambda k: -leaves[k].size)
    width = (1, *leaves[order[0]].shape)[-1]
    lines = [
        jnp.pad(leaves[k].reshape(-1), (0, -leaves[k].size % width)).reshape(-1, width)
        for k in order
    ]
    both, at, found = (from_everyone(jnp.concatenate(lines), axis), 0, {})
    for k, line in zip(order, lines):
        share = both[:, at : at + len(line)].reshape(len(both), -1)
        found[k] = share[:, : leaves[k].size].reshape(-1, *leaves[k].shape)
        at += len(line)
    numbers = iter(range(len(leaves)))
    return jax.tree.map(lambda _: found[next(numbers)], shard)


def joined_by_halves(pieces, combine):
    while len(jax.tree.leaves(pieces)[0]) > 1:
        pieces = jax.vmap(combine)(
            *(jax.tree.map(lambda part: part[side::2], pieces) for side in (0, 1))
        )
    return jax.tree.map(lambda part: part[0], pieces)


def carried_in(shard, axis, combine, identity):
    devices, place = (lax.axis_size(axis), lax.axis_index(axis))
    passed = jnp.arange(devices) > place

    def kept(part, zero, own):
        part = jnp.where(
            passed.reshape(-1, *(1 for _ in own.shape)), part, jnp.asarray(zero, own.dtype)
        )
        return part[::-1]

    pieces = all_in_one(shard, axis)
    return joined_by_halves(jax.tree.map(kept, pieces, identity, shard), combine)


def silu_parts(values):
    sig = jax.nn.sigmoid(values)
    return (values * sig, sig * (1.0 + values * (1.0 - sig)))


def route_slots(route_block, experts, capacity):
    flat_ids = route_block.reshape(-1)
    onehot = (flat_ids[:, None] == jnp.arange(experts, dtype=jnp.int32)[None, :]).astype(jnp.int32)
    before = jnp.cumsum(onehot, axis=0) - onehot
    slot_rank = jnp.sum(before * onehot, axis=1)
    return flat_ids * capacity + slot_rank


def link_steps(earlier, later):
    return (earlier[0] * later[0], later[0] * earlier[1] + later[1])


def join_carry(earlier, later):
    return (later[0] * earlier[0], later[1] + later[0] * earlier[1])


def contract_rows(left, right):
    return lax.dot_general(
        left, right, (((0,), (0,)), ((), ())), preferred_element_type=jnp.float32
    )


def body(
    cotangent,
    mixer_out,
    route_ids,
    route_weights,
    conv_out,
    recur_gate,
    input_gate,
    gate_pre,
    states_before,
    decay_rate,
    out_proj,
    recur_map,
    input_map,
    expert_gate,
    expert_up,
    expert_down,
):
    row_count = cotangent.shape[0]
    got_rows, got_cot, dispatch = dispatched(route_ids, route_weights, mixer_out, cotangent)
    got_rows = got_rows.reshape(-1, got_rows.shape[2])
    got_cot = got_cot.reshape(got_rows.shape)
    w_gate = expert_gate[0]
    w_up = expert_up[0]
    w_down = expert_down[0]
    pre_gate = jnp.dot(got_rows, w_gate, preferred_element_type=jnp.float32)
    pre_up = jnp.dot(got_rows, w_up, preferred_element_type=jnp.float32)
    gate_act, slope = silu_parts(pre_gate)
    active = (gate_act * pre_up).astype(jnp.bfloat16)
    d_active = lax.dot_general(
        got_cot, w_down, (((1,), (1,)), ((), ())), preferred_element_type=jnp.float32
    )
    grad_down = contract_rows(active, got_cot).astype(jnp.bfloat16)
    d_gate = (d_active * pre_up * slope).astype(jnp.bfloat16)
    d_up = (d_active * gate_act).astype(jnp.bfloat16)
    grad_gate = contract_rows(got_rows, d_gate).astype(jnp.bfloat16)
    grad_up = contract_rows(got_rows, d_up).astype(jnp.bfloat16)
    partial_grad = lax.dot_general(
        d_gate, w_gate, (((1,), (1,)), ((), ())), preferred_element_type=jnp.float32
    ) + lax.dot_general(d_up, w_up, (((1,), (1,)), ((), ())), preferred_element_type=jnp.float32)
    summed = sent_and_summed(partial_grad.astype(jnp.bfloat16), "tp", 1).astype(jnp.bfloat16)
    returned = lax.all_to_all(summed, SP, split_axis=0, concat_axis=0, tiled=True)
    grad_part = (cotangent.astype(jnp.float32) + contract_rows(dispatch, returned)).astype(
        jnp.bfloat16
    )
    out_grad = gathered_copies(grad_part, "tp", 1)
    channels = conv_out.shape[1]
    rate = decay_rate[None, :]
    recur_f = recur_gate.astype(jnp.float32)
    input_f = input_gate.astype(jnp.float32)
    conv_f = conv_out.astype(jnp.float32)
    before_f = states_before.astype(jnp.float32)
    log_decay = -8.0 * recur_f * rate
    decay_now = jnp.exp(log_decay)
    position = lax.axis_index(SP) * row_count + jnp.arange(row_count, dtype=jnp.int32)
    at_start = (position == 0)[:, None]
    norm_factor = jnp.where(at_start, 1.0, jnp.sqrt(-jnp.expm1(2.0 * log_decay)))
    norm_slope = jnp.where(at_start, 0.0, -jnp.exp(2.0 * log_decay) / norm_factor)
    drive = input_f * conv_f
    state = decay_now * before_f + norm_factor * drive
    gate, gelu_back = jax.vjp(jax.nn.gelu, gate_pre.astype(jnp.float32))
    mixed = (state * gate).astype(jnp.bfloat16)
    d_mixed = jnp.dot(out_grad, out_proj, preferred_element_type=jnp.float32)
    grad_out_proj = summed_rows(
        contract_rows(out_grad, mixed).astype(jnp.bfloat16), (("sp_0", "sp_1"), "sp_2"), 0
    )
    grad_gate_pre = gelu_back(d_mixed * state)[0].astype(jnp.bfloat16)
    decay_next = jnp.concatenate([decay_now[1:], jnp.ones((1, channels), jnp.float32)], axis=0)
    carry_weight, local_grad = lax.associative_scan(
        link_steps, (decay_next, d_mixed * gate), axis=0, reverse=True
    )
    span_decay = decay_now[0] * carry_weight[0]
    span_start = decay_now[0] * local_grad[0]
    identity = (jnp.ones((channels,), jnp.float32), jnp.zeros((channels,), jnp.float32))
    _, incoming = carried_in((span_decay, span_start), SP, join_carry, identity)
    state_grad = local_grad + carry_weight * incoming[None, :]
    d_log = state_grad * (decay_now * before_f + norm_slope * drive)
    d_recur_pre = (d_log * (-8.0 * rate) * recur_f * (1.0 - recur_f)).astype(jnp.bfloat16)
    d_input_pre = (state_grad * norm_factor * conv_f * input_f * (1.0 - input_f)).astype(
        jnp.bfloat16
    )
    groups = recur_map.shape[0]
    width = recur_map.shape[1]
    through_recur = jnp.einsum(
        "tbj,bij->tbi",
        d_recur_pre.reshape(row_count, groups, width),
        recur_map,
        preferred_element_type=jnp.float32,
    )
    through_input = jnp.einsum(
        "tbj,bij->tbi",
        d_input_pre.reshape(row_count, groups, width),
        input_map,
        preferred_element_type=jnp.float32,
    )
    grad_conv = (
        state_grad * norm_factor * input_f
        + (through_recur + through_input).reshape(row_count, channels)
    ).astype(jnp.bfloat16)
    return (
        grad_gate[None],
        grad_up[None],
        grad_down[None],
        grad_out_proj,
        grad_conv,
        grad_gate_pre,
    )


def solution(mesh):
    torus = Mesh(mesh.devices.reshape(8, 4, 2, mesh.shape["tp"]), ("sp_0", "sp_1", "sp_2", "tp"))
    in_specs = (
        P(SP, "tp"),
        P(SP, "tp"),
        P(SP, None),
        P(SP, None),
        P(SP, "tp"),
        P(SP, "tp"),
        P(SP, "tp"),
        P(SP, "tp"),
        P(SP, "tp"),
        P("tp"),
        P(None, "tp"),
        P("tp", None, None),
        P("tp", None, None),
        P(SP, None, "tp"),
        P(SP, None, "tp"),
        P(SP, "tp", None),
    )
    out_specs = (
        P(SP, None, "tp"),
        P(SP, None, "tp"),
        P(SP, "tp", None),
        P(SP, "tp"),
        P(SP, "tp"),
        P(SP, "tp"),
    )
    return jax.shard_map(body, mesh=torus, in_specs=in_specs, out_specs=out_specs, check_vma=False)
```

```python
import functools

import jax
import jax.numpy as jnp
from jax import lax
from jax.experimental import pallas as pl
from jax.experimental.pallas import tpu as pltpu
from jax.sharding import Mesh
from jax.sharding import PartitionSpec as P

SP = ("sp_0", "sp_1", "sp_2")
AXES = (*SP, "tp")
MESH_ID = pl.DeviceIdType.MESH
BF16 = jnp.bfloat16
F32 = jnp.float32
PIECES = 2


def near_first(count):
    return sorted(range(count), key=lambda k: (min(k, count - k), k))


def slot_hits(ids, experts, capacity):
    tokens = ids.shape[1]
    slots = experts * capacity
    first, second = ids[0:1, :], ids[1:2, :]
    expert = lax.broadcasted_iota(jnp.int32, (experts, tokens), 0)
    named = jnp.where((expert == first) | (expert == second), 1.0, 0.0).astype(jnp.bfloat16)
    at = lax.broadcasted_iota(jnp.int32, (tokens, tokens), 0)
    later = lax.broadcasted_iota(jnp.int32, (tokens, tokens), 1)
    earlier = jnp.where(at < later, 1.0, 0.0).astype(jnp.bfloat16)
    before = jnp.dot(named, earlier, preferred_element_type=jnp.float32)
    of_slot = lax.broadcasted_iota(jnp.int32, (slots, experts), 0)
    of_expert = lax.broadcasted_iota(jnp.int32, (slots, experts), 1)
    spread = jnp.where(of_slot // capacity == of_expert, 1.0, 0.0).astype(jnp.bfloat16)
    rank = jnp.dot(spread, before.astype(jnp.bfloat16), preferred_element_type=jnp.float32)
    slot = lax.broadcasted_iota(jnp.int32, (slots, tokens), 0)
    free = rank == (slot % capacity).astype(jnp.float32)
    return free & (slot // capacity == first), free & (slot // capacity == second)


def dot(left, right, at_left=1, at_right=0):
    return lax.dot_general(
        left, right, (((at_left,), (at_right,)), ((), ())), preferred_element_type=F32
    )


def layer_kernel(sizes, *refs):
    names = IN_NAMES + OUT_NAMES + SCRATCH_NAMES
    r = dict(zip(names, refs, strict=True))
    nz, ny, nc, nx = sizes
    plane = ny * nc
    experts = nz * plane
    z, y, c, x = (lax.axis_index(a) for a in AXES)
    tokens, width = r["cot"].shape
    capacity = r["rows"].shape[1]
    me = (z * ny + y) * nc + c
    mine = y * nc + c
    right, left = lax.rem(x + 1, nx), lax.rem(x + nx - 1, nx)
    across = lax.rem(x + 2, nx)
    up, down = lax.rem(y + 1, ny), lax.rem(y + ny - 1, ny)
    over = lax.rem(y + 2, ny)
    twin = nc - 1 - c
    group = plane * capacity
    order = near_first(nz)
    waits = []

    def columns(part):
        return pl.ds(pl.multiple_of(part * width, width), width)

    def partner(j, sign):
        dz, dy, dc = j // plane, (j // nc) % ny, j % nc
        return (
            lax.rem(z + sign * dz + nz, nz),
            lax.rem(y + sign * dy + ny, ny),
            lax.rem(c + sign * dc + nc, nc),
        )

    def remote(source, target, send, recv, device):
        return pltpu.make_async_remote_copy(
            src_ref=source,
            dst_ref=target,
            send_sem=send,
            recv_sem=recv,
            device_id=device,
            device_id_type=MESH_ID,
        )

    loads = {
        name: pltpu.make_async_copy(r[name], r[name + "_in"], r["load_sem"].at[k])
        for k, name in enumerate(LOADED)
    }
    for name in LOADED:
        loads[name].start()

    barrier = pltpu.get_barrier_semaphore()

    def greet(sem, first, stop, step):
        def one(k, carry):
            pl.semaphore_signal(
                sem, inc=1, device_id=(*partner(k * step, 1), x), device_id_type=MESH_ID
            )
            return carry

        lax.fori_loop(first, stop, one, 0)

    greet(barrier, 1, nz, plane)
    greet(barrier, 1, plane, 1)
    for side in (left, right):
        pl.semaphore_signal(barrier, inc=1, device_id=(z, y, c, side), device_id_type=MESH_ID)

    first, second = slot_hits(r["ids"][...], experts, capacity)
    hits = jnp.where(first | second, 1.0, 0.0).astype(BF16)
    r["hits"][...] = hits
    weights = r["weights"][...]
    weight = jnp.sum(
        jnp.where(first, weights[0:1, :], 0.0) + jnp.where(second, weights[1:2, :], 0.0),
        axis=1,
        keepdims=True,
    )
    shape = r["send_rows"].shape
    r["send_rows"][...] = dot(hits, r["mixer"][...]).reshape(shape).astype(BF16)
    r["send_cots"][...] = (dot(hits, r["cot"][...]) * weight).reshape(shape).astype(BF16)

    pl.semaphore_wait(barrier, nz - 1 + plane - 1 + 2)
    greet(r["met"], 1, plane, 1)
    pl.semaphore_wait(r["met"], plane - 1)

    pairs = ((r["send_rows"], r["rows"]), (r["send_cots"], r["cots"]))

    def local(k):
        source, target = pairs[k]
        return pltpu.make_async_copy(
            source.at[me], target.at[me, :, columns(x)], r["a_recv"].at[k, 0]
        )

    def sent(k, j):
        dz, dy, dc = partner(j, 1)
        source, target = pairs[k]
        return remote(
            source.at[(dz * ny + dy) * nc + dc],
            target.at[me, :, columns(x)],
            r["a_send"].at[k, j],
            r["a_recv"].at[k, j],
            (dz, dy, dc, x),
        )

    def arriving(k, j):
        sz, sy, sc = partner(j, -1)
        source, target = pairs[k]
        return remote(
            source.at[me],
            target.at[(sz * ny + sy) * nc + sc, :, columns(x)],
            r["a_send"].at[k, j],
            r["a_recv"].at[k, j],
            (sz, sy, sc, x),
        )

    for k in (0, 1):
        local(k).start()
    for dz in order:

        def send(j, carry):
            for k in (0, 1):
                sent(k, j).start()
            return carry

        lax.fori_loop(max(dz * plane, 1), (dz + 1) * plane, send, 0)

    for name in RECURRENCE:
        loads[name].wait()
    recur = r["recur_gate_in"][...].astype(F32)
    rate = r["decay_rate_in"][...]
    log_decay = -8.0 * recur * rate
    decay = jnp.exp(log_decay)
    norm = r["norm_in"][...]
    position = lax.broadcasted_iota(jnp.int32, (tokens, width), 0)
    at_start = (position + me * tokens) == 0
    slope = jnp.where(at_start, 0.0, -jnp.exp(2.0 * log_decay) / norm)
    conv = r["conv_in"][...].astype(F32)
    entry = r["input_gate_in"][...].astype(F32)
    drive = entry * conv
    before = r["states_in"][...].astype(F32)
    state = decay * before + norm * drive
    r["by_recur"][...] = (
        (decay * before + slope * drive) * (-8.0 * rate) * recur * (1.0 - recur)
    )
    r["by_input"][...] = norm * conv * entry * (1.0 - entry)
    r["by_conv"][...] = norm * entry
    pre = r["gate_pre_in"][...].astype(F32)
    root = 0.7978845608028654
    bent = jnp.tanh(root * (pre + 0.044715 * (pre * pre * pre)))
    cdf = 0.5 * (1.0 + bent)
    gate = pre * cdf
    gelu_slope = cdf + 0.5 * pre * (1.0 - bent * bent) * root * (1.0 + 3.0 * 0.044715 * (pre * pre))
    r["gate"][...] = gate
    r["mixed"][...] = (state * gate).astype(BF16)
    r["by_gate"][...] = state * gelu_slope
    r["first_decay"][...] = decay[0:8, :]
    following = pltpu.roll(decay, tokens - 1, 0)
    last = position == tokens - 1
    reach = jnp.where(last, 0.0, following)
    carry_weight = jnp.where(last, 1.0, following)
    step = 1
    level = 0
    while step < tokens:
        r["reach"][level] = reach
        moved = pltpu.roll(reach, tokens - step, 0)
        reach = reach * moved
        moved = pltpu.roll(carry_weight, tokens - step, 0)
        carry_weight = carry_weight * jnp.where(position < tokens - step, moved, 1.0)
        step *= 2
        level += 1
    r["carry_weight"][...] = carry_weight
    for name in LOADED:
        if name not in RECURRENCE:
            loads[name].wait()

    def start_of(dz):
        return lax.rem(z - dz + nz, nz) * plane

    def ring_block(ref, dz, half, part):
        start, count = start_of(dz), plane
        if half is not None:
            count = plane // 2
            start = start + half * count
        return ref.at[pl.ds(start, count), :, columns(part)]

    sides = (left, right)
    others = (right, left)

    def own(k, dz, way, arrives):
        here = ring_block(pairs[k][1], dz, None, sides[way] if arrives else x)
        return remote(
            here, here, r["own_send"].at[way, k, dz], r["own_recv"].at[way, k, dz],
            (z, y, c, sides[way] if arrives else others[way]),
        )

    def passed(k, dz, way, arrives):
        here = ring_block(pairs[k][1], dz, way, across if arrives else sides[way])
        return remote(
            here, here, r["pass_send"].at[way, k, dz], r["pass_recv"].at[way, k, dz],
            (z, y, c, sides[way] if arrives else others[way]),
        )

    both_ways = [(k, way) for k in (0, 1) for way in (0, 1)]

    def hand_on(dz):
        for k, way in both_ways:
            own(k, dz, way, True).wait_recv()
            passed(k, dz, way, False).start()

    def settle(dz):
        for k, way in both_ways:
            passed(k, dz, way, True).wait_recv()

    def as_rows(ref, starts, cols):
        return jnp.concatenate(
            [ref[pl.ds(s, plane), :, cols].reshape(group, -1) for s in starts], axis=0
        )

    def keep(ref, starts, cols, value):
        for k, s in enumerate(starts):
            part = value[k * group : (k + 1) * group]
            ref[pl.ds(s, plane), :, cols] = part.reshape(plane, capacity, -1).astype(BF16)

    def expert_rows(dzs):
        starts = [start_of(dz) for dz in dzs]
        for name in ("acc_gate", "acc_up", "acc_down"):
            r[name][...] = jnp.zeros_like(r[name])

        def gather(t, carry):
            cols = columns(t)
            row_part = as_rows(r["rows"], starts, cols)
            r["acc_gate"][...] += dot(row_part, r["w_gate_in"][cols, :])
            r["acc_up"][...] += dot(row_part, r["w_up_in"][cols, :])
            cot_part = as_rows(r["cots"], starts, cols)
            r["acc_down"][...] += dot(cot_part, r["w_down_in"][:, cols], 1, 1)
            return carry

        lax.fori_loop(0, nx, gather, 0)
        pre_gate, pre_up, d_active = r["acc_gate"][...], r["acc_up"][...], r["acc_down"][...]
        sig = jax.nn.sigmoid(pre_gate)
        silu = pre_gate * sig
        silu_slope = sig * (1.0 + pre_gate * (1.0 - sig))
        d_gate = d_active * pre_up * silu_slope
        d_up = d_active * silu
        whole = slice(None)
        keep(r["active"], starts, whole, silu * pre_up)
        keep(r["d_gate"], starts, whole, d_gate)
        keep(r["d_up"], starts, whole, d_up)
        d_gate, d_up = d_gate.astype(BF16), d_up.astype(BF16)

        def spread(t, carry):
            cols = columns(t)
            value = dot(d_gate, r["w_gate_in"][cols, :], 1, 1)
            value += dot(d_up, r["w_up_in"][cols, :], 1, 1)
            keep(r["partial"], starts, cols, value)
            return carry

        lax.fori_loop(0, nx, spread, 0)

    def half_sum(dz, way, arrives):
        return remote(
            ring_block(r["partial"], dz, way, across),
            r["half_in"].at[way, dz],
            r["half_send"].at[way, dz],
            r["half_recv"].at[way, dz],
            (z, y, c, sides[way] if arrives else others[way]),
        )

    def unit_sum(dz, way, arrives):
        return remote(
            r["unit_out"].at[way, dz],
            r["unit_in"].at[way, dz],
            r["unit_send"].at[way, dz],
            r["unit_recv"].at[way, dz],
            (z, y, c, sides[way] if arrives else others[way]),
        )

    def sum_one(dz):
        for way in (0, 1):
            half_sum(dz, way, False).start()

    def sum_two(dz):
        start = start_of(dz)
        for way in (0, 1):
            half_sum(dz, way, True).wait_recv()
            value = r["partial"][pl.ds(start, plane), :, columns(others[way])].astype(F32)
            more = r["half_in"][way, dz].astype(F32)
            half = plane // 2
            parts = [value[:half], value[half:]]
            parts[way] = parts[way] + more
            r["unit_out"][way, dz] = jnp.concatenate(parts, axis=0).astype(BF16)
            unit_sum(dz, way, False).start()

    def returned(j):
        dz, dy, dc = partner(j, -1)
        return remote(
            r["back_out"].at[(dz * ny + dy) * nc + dc],
            r["back_in"].at[me],
            r["back_send"].at[j],
            r["back_recv"].at[j],
            (dz, dy, dc, x),
        )

    def returning(j):
        sz, sy, sc = partner(j, 1)
        return remote(
            r["back_out"].at[me],
            r["back_in"].at[(sz * ny + sy) * nc + sc],
            r["back_send"].at[j],
            r["back_recv"].at[j],
            (sz, sy, sc, x),
        )

    def back_local():
        return pltpu.make_async_copy(
            r["back_out"].at[me], r["back_in"].at[me], r["back_recv"].at[0]
        )

    def sum_three(dz):
        start = start_of(dz)
        value = r["partial"][pl.ds(start, plane), :, columns(x)].astype(F32)
        for way in (0, 1):
            unit_sum(dz, way, True).wait_recv()
            value = value + r["unit_in"][way, dz].astype(F32)
        r["back_out"][pl.ds(start, plane)] = value.astype(BF16)

        def give(j, carry):
            returned(j).start()
            return carry

        lax.fori_loop(max(dz * plane, 1), (dz + 1) * plane, give, 0)
        if dz == 0:
            back_local().start()

    chunks = [order[k : k + 2] for k in range(0, nz, 2)]

    def sums(stage, k):
        if 0 <= k < len(chunks):
            for dz in chunks[k]:
                stage(dz)

    for at, dz in enumerate(order):
        if dz == 0:
            for k in (0, 1):
                local(k).wait()

        def arrive(j, carry):
            for k in (0, 1):
                arriving(k, j).wait_recv()
            return carry

        lax.fori_loop(max(dz * plane, 1), (dz + 1) * plane, arrive, 0)
        for k, way in both_ways:
            own(k, dz, way, False).start()
        if at:
            hand_on(order[at - 1])
        if at >= 2:
            settle(order[at - 2])
        if at >= 3 and at % 2:
            k = (at - 3) // 2
            sums(sum_two, k - 1)
            sums(sum_three, k - 2)
            expert_rows(chunks[k])
            sums(sum_one, k)
    hand_on(order[-1])
    k = len(chunks) - 1
    sums(sum_two, k - 1)
    sums(sum_three, k - 2)
    settle(order[-2])
    settle(order[-1])
    expert_rows(chunks[k])
    sums(sum_one, k)
    sums(sum_three, k - 1)

    def rows_of(name, cols):
        return r[name][:, :, cols].reshape(experts * capacity, -1)

    whole = slice(None)

    def grad_in(name):
        def part(t, carry):
            cols = columns(t)
            value = dot(rows_of("rows", cols), rows_of("d_" + name, whole), 0, 0)
            r["g_" + name][cols, :] = value.astype(BF16)
            return carry

        lax.fori_loop(0, nx, part, 0)

    def grad_down():
        def part(t, carry):
            cols = columns(t)
            value = dot(rows_of("active", whole), rows_of("cots", cols), 0, 0)
            r["g_down"][:, cols] = value.astype(BF16)
            return carry

        lax.fori_loop(0, nx, part, 0)

    stores = {
        name: pltpu.make_async_copy(r["g_" + name], r["grad_" + name], r["store_sem"].at[k])
        for k, name in enumerate(("gate", "up", "down"))
    }
    sums(sum_two, k)
    grad_in("gate")
    stores["gate"].start()
    sums(sum_three, k)
    grad_in("up")
    stores["up"].start()

    back_local().wait()

    def come(j, carry):
        returning(j).wait_recv()
        return carry

    lax.fori_loop(1, experts, come, 0)
    routed = dot(r["hits"][...], r["back_in"][...].reshape(experts * capacity, width), 0, 0)
    r["out_grad"][:, columns(x)] = (r["cot"][...].astype(F32) + routed).astype(BF16)

    half_rows = tokens // 2

    def grad_own(way, arrives):
        here = r["out_grad"].at[:, columns(sides[way] if arrives else x)]
        return remote(
            here, here, r["og_send"].at[way], r["og_recv"].at[way],
            (z, y, c, sides[way] if arrives else others[way]),
        )

    def grad_passed(way, arrives):
        here = r["out_grad"].at[
            pl.ds(way * half_rows, half_rows), columns(across if arrives else sides[way])
        ]
        return remote(
            here, here, r["og_send"].at[2 + way], r["og_recv"].at[2 + way],
            (z, y, c, sides[way] if arrives else others[way]),
        )

    for way in (0, 1):
        grad_own(way, False).start()
    grad_down()
    stores["down"].start()
    for way in (0, 1):
        grad_own(way, True).wait_recv()
        grad_passed(way, False).start()
    for way in (0, 1):
        grad_passed(way, True).wait_recv()

    lines = r["proj_out"].shape[0]
    per_part = nz // nx

    def term(t, carry):
        value = dot(r["out_grad"][:, columns(t)], r["mixed"][...], 0, 0)
        r["term"][pl.ds(t * per_part, per_part)] = value.reshape(
            per_part, ny, nc, lines, width
        ).astype(BF16)
        return carry

    lax.fori_loop(0, nx, term, 0)
    cut = lines // PIECES

    def rows_in(p):
        return pl.ds(p * cut, cut)

    def core_sum(p):
        return remote(
            r["term"].at[:, :, twin, rows_in(p), :],
            r["core_in"].at[:, :, rows_in(p), :],
            r["core_send"].at[p],
            r["core_recv"].at[p],
            (z, y, twin, x),
        )

    for p in range(PIECES):
        core_sum(p).start()

    r["d_mixed"][...] = jnp.zeros_like(r["d_mixed"])

    def mix(t, carry):
        cols = columns(t)
        r["d_mixed"][...] += dot(r["out_grad"][:, cols], r["out_proj_in"][cols, :])
        return carry

    lax.fori_loop(0, nx, mix, 0)
    d_mixed = r["d_mixed"][...]
    r["gate_grad"][...] = (d_mixed * r["by_gate"][...]).astype(BF16)
    local_grad = d_mixed * r["gate"][...]
    step, level = 1, 0
    while step < tokens:
        local_grad = local_grad + r["reach"][level] * pltpu.roll(local_grad, tokens - step, 0)
        step *= 2
        level += 1
    r["local_grad"][...] = local_grad
    head = r["first_decay"][0:1, :]
    link = jnp.concatenate(
        [
            head * r["carry_weight"][0:1, :],
            head * local_grad[0:1, :],
            jnp.zeros((6, width), F32),
        ],
        axis=0,
    )
    r["near_links"][mine] = link

    def near_link(j, arrives):
        _, py, pc = partner(j, -1 if arrives else 1)
        slot = py * nc + pc if arrives else mine
        here = r["near_links"].at[slot]
        return remote(here, here, r["near_send"].at[j], r["near_recv"].at[j], (z, py, pc, x))

    for j in range(1, plane):
        near_link(j, False).start()

    def up_half(p, way, arrives):
        half = nz // 2
        return remote(
            r["core_out"].at[pl.ds(way * half, half), over, rows_in(p), :],
            r["line_half"].at[way, :, rows_in(p), :],
            r["line_send"].at[way, p],
            r["line_recv"].at[way, p],
            (z, (down, up)[way] if arrives else (up, down)[way], c, x),
        )

    def up_unit(p, way, arrives):
        return remote(
            r["line_out"].at[way, :, rows_in(p), :],
            r["line_in"].at[way, :, rows_in(p), :],
            r["line_send"].at[2 + way, p],
            r["line_recv"].at[2 + way, p],
            (z, (down, up)[way] if arrives else (up, down)[way], c, x),
        )

    for p in range(PIECES):
        core_sum(p).wait_recv()

        def add(k, carry):
            value = r["term"][k, :, pl.ds(c, 1), rows_in(p), :].reshape(ny, cut, width)
            value = value.astype(F32) + r["core_in"][k, :, rows_in(p), :].astype(F32)
            r["core_out"][k, :, rows_in(p), :] = value.astype(BF16)
            return carry

        lax.fori_loop(0, nz, add, 0)
        for way in (0, 1):
            up_half(p, way, False).start()

    for j in range(1, plane):
        near_link(j, True).wait_recv()
    one, zero = jnp.ones((1, width), F32), jnp.zeros((1, width), F32)
    all_weight, all_start, near_weight, near_start = one, zero, one, zero
    for q in range(plane - 1, -1, -1):
        a, b = r["near_links"][q, 0:1, :], r["near_links"][q, 1:2, :]
        all_weight, all_start = a * all_weight, b + a * all_start
        later = q > mine
        near_start = jnp.where(later, b + a * near_start, near_start)
        near_weight = jnp.where(later, a * near_weight, near_weight)
    r["far_links"][z] = jnp.concatenate(
        [all_weight, all_start, jnp.zeros((6, width), F32)], axis=0
    )

    def far_link(dz, arrives):
        pz, _, _ = partner(dz * plane, -1 if arrives else 1)
        here = r["far_links"].at[pz if arrives else z]
        return remote(here, here, r["far_send"].at[dz], r["far_recv"].at[dz], (pz, y, c, x))

    for dz in range(1, nz):
        far_link(dz, False).start()

    for p in range(PIECES):
        for way in (0, 1):
            up_half(p, way, True).wait_recv()
            half = nz // 2
            target = (up, down)[way]
            for part in (0, 1):
                place = pl.ds(part * half, half)
                value = r["core_out"][place, target, rows_in(p), :].astype(F32)
                if part == way:
                    value = value + r["line_half"][way, :, rows_in(p), :].astype(F32)
                r["line_out"][way, place, rows_in(p), :] = value.astype(BF16)
            up_unit(p, way, False).start()

    def far_sum(p, dz, arrives):
        pz, _, _ = partner(dz * plane, -1 if arrives else 1)
        return remote(
            r["last_out"].at[z if arrives else pz, rows_in(p), :],
            r["last_in"].at[pz if arrives else z, rows_in(p), :],
            r["last_send"].at[p, dz],
            r["last_recv"].at[p, dz],
            (pz, y, c, x),
        )

    for p in range(PIECES):
        for way in (0, 1):
            up_unit(p, way, True).wait_recv()
        value = r["core_out"][:, y, rows_in(p), :].astype(F32)
        for way in (0, 1):
            value = value + r["line_in"][way, :, rows_in(p), :].astype(F32)
        r["last_out"][:, rows_in(p), :] = value.astype(BF16)
        for dz in range(1, nz):
            far_sum(p, dz, False).start()
        r["last_in"][z, rows_in(p), :] = r["last_out"][z, rows_in(p), :]

    for dz in range(1, nz):
        far_link(dz, True).wait_recv()
    far_start = zero
    for q in range(nz - 1, -1, -1):
        a, b = r["far_links"][q, 0:1, :], r["far_links"][q, 1:2, :]
        far_start = jnp.where(q > z, b + a * far_start, far_start)
    incoming = near_start + near_weight * far_start
    state_grad = r["local_grad"][...] + r["carry_weight"][...] * incoming
    d_recur = (state_grad * r["by_recur"][...]).astype(BF16)
    d_input = (state_grad * r["by_input"][...]).astype(BF16)
    through = dot(d_recur, r["recur_map_in"][0], 1, 1) + dot(d_input, r["input_map_in"][0], 1, 1)
    r["conv_grad"][...] = (state_grad * r["by_conv"][...] + through).astype(BF16)

    for p in range(PIECES):
        for dz in range(1, nz):
            far_sum(p, dz, True).wait_recv()
        r["proj_out"][rows_in(p), :] = jnp.sum(
            r["last_in"][:, rows_in(p), :].astype(F32), axis=0
        )

    def drain(j, carry):
        for k in (0, 1):
            sent(k, j).wait_send()
        returned(j).wait_send()
        return carry

    lax.fori_loop(1, experts, drain, 0)
    for dz in range(nz):
        for k, way in both_ways:
            own(k, dz, way, False).wait_send()
            passed(k, dz, way, False).wait_send()
        for way in (0, 1):
            half_sum(dz, way, False).wait_send()
            unit_sum(dz, way, False).wait_send()
    for way in (0, 1):
        grad_own(way, False).wait_send()
        grad_passed(way, False).wait_send()
    for j in range(1, plane):
        near_link(j, False).wait_send()
    for dz in range(1, nz):
        far_link(dz, False).wait_send()
    for p in range(PIECES):
        core_sum(p).wait_send()
        for way in (0, 1):
            up_half(p, way, False).wait_send()
            up_unit(p, way, False).wait_send()
        for dz in range(1, nz):
            far_sum(p, dz, False).wait_send()
    for name in ("gate", "up", "down"):
        stores[name].wait()


HELD = ("ids", "weights", "mixer", "cot")
RECURRENCE = (
    "recur_gate", "decay_rate", "norm", "conv", "input_gate", "states", "gate_pre",
)
LOADED = (*RECURRENCE, "w_gate", "w_up", "w_down", "out_proj", "recur_map", "input_map")
IN_NAMES = HELD + LOADED
OUT_NAMES = ("grad_gate", "grad_up", "grad_down", "proj_out", "conv_grad", "gate_grad")


def scratch_of(sizes, tokens, width, hidden, held):
    nz, ny, nc, nx = sizes
    plane = ny * nc
    experts = nz * plane
    capacity = 4 * tokens // experts
    features = nx * width
    lines = features // experts
    group = plane * capacity
    levels = tokens.bit_length() - 1
    dma = pltpu.SemaphoreType.DMA
    per_token = lambda kind: pltpu.VMEM((tokens, width), kind)
    shapes = {name + "_in": pltpu.VMEM(a.shape, a.dtype) for name, a in held.items()}
    shapes |= {
        "rows": pltpu.VMEM((experts, capacity, features), BF16),
        "cots": pltpu.VMEM((experts, capacity, features), BF16),
        "hits": pltpu.VMEM((experts * capacity, tokens), BF16),
        "send_rows": pltpu.VMEM((experts, capacity, width), BF16),
        "send_cots": pltpu.VMEM((experts, capacity, width), BF16),
        "acc_gate": pltpu.VMEM((2 * group, hidden), F32),
        "acc_up": pltpu.VMEM((2 * group, hidden), F32),
        "acc_down": pltpu.VMEM((2 * group, hidden), F32),
        "active": pltpu.VMEM((experts, capacity, hidden), BF16),
        "d_gate": pltpu.VMEM((experts, capacity, hidden), BF16),
        "d_up": pltpu.VMEM((experts, capacity, hidden), BF16),
        "partial": pltpu.VMEM((experts, capacity, features), BF16),
        "g_gate": pltpu.VMEM((features, hidden), BF16),
        "g_up": pltpu.VMEM((features, hidden), BF16),
        "g_down": pltpu.VMEM((hidden, features), BF16),
        "half_in": pltpu.VMEM((2, nz, plane // 2, capacity, width), BF16),
        "unit_out": pltpu.VMEM((2, nz, plane, capacity, width), BF16),
        "unit_in": pltpu.VMEM((2, nz, plane, capacity, width), BF16),
        "back_out": pltpu.VMEM((experts, capacity, width), BF16),
        "back_in": pltpu.VMEM((experts, capacity, width), BF16),
        "out_grad": pltpu.VMEM((tokens, features), BF16),
        "by_recur": per_token(F32),
        "by_input": per_token(F32),
        "by_conv": per_token(F32),
        "by_gate": per_token(F32),
        "gate": per_token(F32),
        "mixed": per_token(BF16),
        "first_decay": pltpu.VMEM((8, width), F32),
        "reach": pltpu.VMEM((levels, tokens, width), F32),
        "carry_weight": per_token(F32),
        "d_mixed": per_token(F32),
        "local_grad": per_token(F32),
        "term": pltpu.VMEM((nz, ny, nc, lines, width), BF16),
        "core_in": pltpu.VMEM((nz, ny, lines, width), BF16),
        "core_out": pltpu.VMEM((nz, ny, lines, width), BF16),
        "line_half": pltpu.VMEM((2, nz // 2, lines, width), BF16),
        "line_out": pltpu.VMEM((2, nz, lines, width), BF16),
        "line_in": pltpu.VMEM((2, nz, lines, width), BF16),
        "last_out": pltpu.VMEM((nz, lines, width), BF16),
        "last_in": pltpu.VMEM((nz, lines, width), BF16),
        "near_links": pltpu.VMEM((plane, 8, width), F32),
        "far_links": pltpu.VMEM((nz, 8, width), F32),
        "met": pltpu.SemaphoreType.REGULAR,
        "load_sem": dma((len(held),)),
        "store_sem": dma((3,)),
    }
    for name, shape in {
        "a": (2, experts),
        "own": (2, 2, nz),
        "pass": (2, 2, nz),
        "half": (2, nz),
        "unit": (2, nz),
        "back": (experts,),
        "og": (4,),
        "near": (plane,),
        "far": (nz,),
        "core": (PIECES,),
        "line": (4, PIECES),
        "last": (PIECES, nz),
    }.items():
        shapes[name + "_send"] = dma(shape)
        shapes[name + "_recv"] = dma(shape)
    return shapes


SIZES = (8, 4, 2, 4)
SCRATCH_NAMES = tuple(
    scratch_of(SIZES, 128, 512, 256, {n: jax.ShapeDtypeStruct((8, 128), F32) for n in LOADED})
)


def layer(held, loaded):
    sizes = tuple(lax.axis_size(a) for a in AXES)
    nz, ny, nc, nx = sizes
    tokens, width = held[3].shape
    named = dict(zip(LOADED, loaded, strict=True))
    hidden = named["w_gate"].shape[1]
    features = nx * width
    shapes = scratch_of(sizes, tokens, width, hidden, named)
    vmem = pl.BlockSpec(memory_space=pltpu.VMEM)
    left = pl.BlockSpec(memory_space=pl.ANY)
    return pl.pallas_call(
        functools.partial(layer_kernel, sizes),
        out_shape=(
            jax.ShapeDtypeStruct((features, hidden), BF16),
            jax.ShapeDtypeStruct((features, hidden), BF16),
            jax.ShapeDtypeStruct((hidden, features), BF16),
            jax.ShapeDtypeStruct((features // (nz * ny * nc), width), F32),
            jax.ShapeDtypeStruct((tokens, width), BF16),
            jax.ShapeDtypeStruct((tokens, width), BF16),
        ),
        in_specs=[vmem] * len(HELD) + [left] * len(LOADED),
        out_specs=(left,) * 3 + (vmem,) * 3,
        scratch_shapes=list(shapes.values()),
        compiler_params=pltpu.CompilerParams(
            collective_id=0, has_side_effects=True, vmem_limit_bytes=60 * 2**20
        ),
        name="layer",
    )(*held, *loaded)


def body(
    cotangent,
    mixer_out,
    route_ids,
    route_weights,
    conv_out,
    recur_gate,
    input_gate,
    gate_pre,
    states_before,
    decay_rate,
    out_proj,
    recur_map,
    input_map,
    expert_gate,
    expert_up,
    expert_down,
):
    row_count = cotangent.shape[0]
    rate = decay_rate[None, :]
    log_decay = -8.0 * recur_gate.astype(F32) * rate
    position = lax.axis_index(SP) * row_count + jnp.arange(row_count, dtype=jnp.int32)
    at_start = (position == 0)[:, None]
    norm_factor = jnp.where(at_start, 1.0, jnp.sqrt(-jnp.expm1(2.0 * log_decay)))
    grads = layer(
        (route_ids.T, route_weights.T, mixer_out, cotangent),
        (
            recur_gate,
            rate,
            norm_factor,
            conv_out,
            input_gate,
            states_before,
            gate_pre,
            expert_gate[0],
            expert_up[0],
            expert_down[0],
            out_proj,
            recur_map,
            input_map,
        ),
    )
    return (grads[0][None], grads[1][None], grads[2][None], *grads[3:])


def solution(mesh):
    torus = Mesh(mesh.devices.reshape(8, 4, 2, mesh.shape["tp"]), ("sp_0", "sp_1", "sp_2", "tp"))
    in_specs = (
        P(SP, "tp"),
        P(SP, "tp"),
        P(SP, None),
        P(SP, None),
        P(SP, "tp"),
        P(SP, "tp"),
        P(SP, "tp"),
        P(SP, "tp"),
        P(SP, "tp"),
        P("tp"),
        P(None, "tp"),
        P("tp", None, None),
        P("tp", None, None),
        P(SP, None, "tp"),
        P(SP, None, "tp"),
        P(SP, "tp", None),
    )
    out_specs = (
        P(SP, None, "tp"),
        P(SP, None, "tp"),
        P(SP, "tp", None),
        P(SP, "tp"),
        P(SP, "tp"),
        P(SP, "tp"),
    )
    return jax.shard_map(body, mesh=torus, in_specs=in_specs, out_specs=out_specs, check_vma=False)
```

```python
import functools
import types

import jax
import jax.numpy as jnp
from jax import lax
from jax.experimental import pallas as pl
from jax.experimental.pallas import tpu as pltpu
from jax.sharding import Mesh
from jax.sharding import PartitionSpec as P

SP = ("sp_0", "sp_1", "sp_2")
AXES = (*SP, "tp")
MESH_ID = pl.DeviceIdType.MESH
BF16 = jnp.bfloat16
F32 = jnp.float32


def near_first(count):
    return sorted(range(count), key=lambda k: (min(k, count - k), k))


def slot_hits(ids, experts, capacity):
    tokens = ids.shape[1]
    slots = experts * capacity
    first, second = ids[0:1, :], ids[1:2, :]
    expert = lax.broadcasted_iota(jnp.int32, (experts, tokens), 0)
    named = jnp.where((expert == first) | (expert == second), 1.0, 0.0).astype(jnp.bfloat16)
    at = lax.broadcasted_iota(jnp.int32, (tokens, tokens), 0)
    later = lax.broadcasted_iota(jnp.int32, (tokens, tokens), 1)
    earlier = jnp.where(at < later, 1.0, 0.0).astype(jnp.bfloat16)
    before = jnp.dot(named, earlier, preferred_element_type=jnp.float32)
    of_slot = lax.broadcasted_iota(jnp.int32, (slots, experts), 0)
    of_expert = lax.broadcasted_iota(jnp.int32, (slots, experts), 1)
    spread = jnp.where(of_slot // capacity == of_expert, 1.0, 0.0).astype(jnp.bfloat16)
    rank = jnp.dot(spread, before.astype(jnp.bfloat16), preferred_element_type=jnp.float32)
    slot = lax.broadcasted_iota(jnp.int32, (slots, tokens), 0)
    free = rank == (slot % capacity).astype(jnp.float32)
    return free & (slot // capacity == first), free & (slot // capacity == second)


def dot(left, right, at_left=1, at_right=0):
    return lax.dot_general(
        left, right, (((at_left,), (at_right,)), ((), ())), preferred_element_type=F32
    )


def expm1_of(v):
    series = jnp.ones_like(v)
    for n in range(11, 1, -1):
        series = 1.0 + v * series * (1.0 / n)
    return jnp.where(jnp.abs(v) < 0.5, v * series, jnp.exp(v) - 1.0)


def layer_kernel(sizes, *refs):
    names = IN_NAMES + OUT_NAMES + SCRATCH_NAMES
    r = types.SimpleNamespace(**dict(zip(names, refs, strict=True)))
    nz, ny, nc, nx = sizes
    plane = ny * nc
    experts = nz * plane
    z, y, c, x = (lax.axis_index(a) for a in AXES)
    tokens, width = r.cot_in.shape
    capacity = r.sending.shape[2]
    me = (z * ny + y) * nc + c
    mine = y * nc + c
    right, left = lax.rem(x + 1, nx), lax.rem(x + nx - 1, nx)
    across = lax.rem(x + 2, nx)
    up, down = lax.rem(y + 1, ny), lax.rem(y + ny - 1, ny)
    over = lax.rem(y + 2, ny)
    twin = nc - 1 - c
    group = plane * capacity
    order = near_first(nz)[1:] + [0]
    waits = []

    def columns(part):
        return pl.ds(pl.multiple_of(part * width, width), width)

    def partner(j, sign):
        dz, dy, dc = j // plane, (j // nc) % ny, j % nc
        return (
            lax.rem(z + sign * dz + nz, nz),
            lax.rem(y + sign * dy + ny, ny),
            lax.rem(c + sign * dc + nc, nc),
        )

    def remote(source, target, send, recv, device):
        return pltpu.make_async_remote_copy(
            src_ref=source,
            dst_ref=target,
            send_sem=send,
            recv_sem=recv,
            device_id=device,
            device_id_type=MESH_ID,
        )

    loads = {
        name: pltpu.make_async_copy(getattr(r, name), getattr(r, name + "_in"), r.load_sem.at[k])
        for k, name in enumerate(LOADED)
    }
    for name in LOADED:
        loads[name].start()

    barrier = pltpu.get_barrier_semaphore()

    def greet(sem, first, stop, step):
        def one(k, carry):
            pl.semaphore_signal(
                sem, inc=1, device_id=(*partner(k * step, 1), x), device_id_type=MESH_ID
            )
            return carry

        lax.fori_loop(first, stop, one, 0)

    greet(barrier, 1, nz, plane)
    greet(barrier, 1, plane, 1)
    for side in (left, right):
        pl.semaphore_signal(barrier, inc=1, device_id=(z, y, c, side), device_id_type=MESH_ID)

    for name in HELD:
        loads[name].wait()
    first, second = slot_hits(r.ids_in[...], experts, capacity)
    hits = jnp.where(first | second, 1.0, 0.0).astype(BF16)
    r.hits[...] = hits
    weights = r.weights_in[...]
    weight = jnp.sum(
        jnp.where(first, weights[0:1, :], 0.0) + jnp.where(second, weights[1:2, :], 0.0),
        axis=1,
        keepdims=True,
    )
    shape = (experts, capacity, width)
    r.sending[:, 0] = dot(hits, r.mixer_in[...]).reshape(shape).astype(BF16)
    r.sending[:, 1] = (dot(hits, r.cot_in[...]) * weight).reshape(shape).astype(BF16)

    pl.semaphore_wait(barrier, nz - 1 + plane - 1 + 2)
    greet(r.met, 1, plane, 1)
    pl.semaphore_wait(r.met, plane - 1)

    def only_wait(like, sem):
        return remote(like, like, sem, sem, (z, y, twin, x))

    def sent(j):
        dz, dy, dc = partner(j, 1)
        return remote(
            r.sending.at[(dz * ny + dy) * nc + dc],
            r.pack.at[me, :, :, columns(x)],
            r.a_send.at[0],
            r.a_recv.at[j // plane],
            (dz, dy, dc, x),
        )

    pltpu.make_async_copy(
        r.sending.at[me], r.pack.at[me, :, :, columns(x)], r.a_recv.at[0]
    ).start()
    for dz in order:

        def send(j, carry):
            sent(j).start()
            return carry

        lax.fori_loop(max(dz * plane, 1), (dz + 1) * plane, send, 0)

    for name in RECURRENCE:
        loads[name].wait()
    recur = r.recur_gate_in[...].astype(F32)
    rate = r.decay_rate_in[...]
    log_decay = -8.0 * recur * rate
    decay = jnp.exp(log_decay)
    position = lax.broadcasted_iota(jnp.int32, (tokens, width), 0)
    at_start = (position + me * tokens) == 0
    norm = jnp.where(at_start, 1.0, jnp.sqrt(-expm1_of(2.0 * log_decay)))
    slope = jnp.where(at_start, 0.0, -jnp.exp(2.0 * log_decay) / norm)
    conv = r.conv_in[...].astype(F32)
    entry = r.input_gate_in[...].astype(F32)
    drive = entry * conv
    before = r.states_in[...].astype(F32)
    state = decay * before + norm * drive
    r.by_recur[...] = (
        (decay * before + slope * drive) * (-8.0 * rate) * recur * (1.0 - recur)
    )
    r.by_input[...] = norm * conv * entry * (1.0 - entry)
    r.by_conv[...] = norm * entry
    pre = r.gate_pre_in[...].astype(F32)
    root = 0.7978845608028654
    bent = jnp.tanh(root * (pre + 0.044715 * (pre * pre * pre)))
    cdf = 0.5 * (1.0 + bent)
    gate = pre * cdf
    gelu_slope = cdf + 0.5 * pre * (1.0 - bent * bent) * root * (1.0 + 3.0 * 0.044715 * (pre * pre))
    r.gate[...] = gate
    r.mixed[...] = (state * gate).astype(BF16)
    r.by_gate[...] = state * gelu_slope
    r.first_decay[...] = decay[0:8, :]
    following = pltpu.roll(decay, tokens - 1, 0)
    last = position == tokens - 1
    reach = jnp.where(last, 0.0, following)
    carry_weight = jnp.where(last, 1.0, following)
    step = 1
    level = 0
    while step < tokens:
        r.reach[level] = reach
        moved = pltpu.roll(reach, tokens - step, 0)
        reach = reach * moved
        moved = pltpu.roll(carry_weight, tokens - step, 0)
        carry_weight = carry_weight * jnp.where(position < tokens - step, moved, 1.0)
        step *= 2
        level += 1
    r.carry_weight[...] = carry_weight
    for name in LOADED:
        if name not in HELD + RECURRENCE:
            loads[name].wait()

    def start_of(dz):
        return lax.rem(z - dz + nz, nz) * plane

    def ring_block(ref, dz, half, part):
        start, count = start_of(dz), plane
        if half is not None:
            count = plane // 2
            start = start + half * count
        return ref.at[pl.ds(start, count), ..., columns(part)]

    sides = (left, right)
    others = (right, left)

    def own(dz, way, arrives):
        here = ring_block(r.pack, dz, None, sides[way] if arrives else x)
        return remote(
            here, here, r.own_send.at[way, 0], r.own_recv.at[way, dz],
            (z, y, c, sides[way] if arrives else others[way]),
        )

    def passed(dz, way, arrives):
        here = ring_block(r.pack, dz, way, across if arrives else sides[way])
        return remote(
            here, here, r.hand_send.at[way, 0], r.hand_recv.at[way, dz],
            (z, y, c, sides[way] if arrives else others[way]),
        )

    def hand_on(dz):
        for way in (0, 1):
            own(dz, way, True).wait_recv()
            passed(dz, way, False).start()

    def settle(dz):
        for way in (0, 1):
            passed(dz, way, True).wait_recv()

    def as_rows(kind, starts, cols):
        return jnp.concatenate(
            [r.pack[pl.ds(s, plane), kind, :, cols].reshape(group, -1) for s in starts], axis=0
        )

    def keep(ref, starts, cols, value):
        for k, s in enumerate(starts):
            part = value[k * group : (k + 1) * group]
            ref[pl.ds(s, plane), :, cols] = part.reshape(plane, capacity, -1).astype(BF16)

    def expert_rows(dzs):
        starts = [start_of(dz) for dz in dzs]
        size = pl.ds(0, len(dzs) * group)
        sums_of = [acc.at[size] for acc in (r.acc_gate, r.acc_up, r.acc_down)]
        for acc in sums_of:
            acc[...] = jnp.zeros(acc.shape, F32)

        def gather(t, carry):
            cols = columns(t)
            row_part = as_rows(0, starts, cols)
            sums_of[0][...] += dot(row_part, r.w_gate_in[cols, :])
            sums_of[1][...] += dot(row_part, r.w_up_in[cols, :])
            cot_part = as_rows(1, starts, cols)
            sums_of[2][...] += dot(cot_part, r.w_down_in[:, cols], 1, 1)
            return carry

        lax.fori_loop(0, nx, gather, 0)
        pre_gate, pre_up, d_active = (acc[...] for acc in sums_of)
        sig = jax.nn.sigmoid(pre_gate)
        silu = pre_gate * sig
        silu_slope = sig * (1.0 + pre_gate * (1.0 - sig))
        d_gate = d_active * pre_up * silu_slope
        d_up = d_active * silu
        whole = slice(None)
        keep(r.active, starts, whole, silu * pre_up)
        keep(r.d_gate, starts, whole, d_gate)
        keep(r.d_up, starts, whole, d_up)
        d_gate, d_up = d_gate.astype(BF16), d_up.astype(BF16)

        def spread(t, carry):
            cols = columns(t)
            value = dot(d_gate, r.w_gate_in[cols, :], 1, 1)
            value += dot(d_up, r.w_up_in[cols, :], 1, 1)
            keep(r.partial, starts, cols, value)
            return carry

        lax.fori_loop(0, nx, spread, 0)

    def half_sum(dz, way, arrives):
        return remote(
            ring_block(r.partial, dz, way, across),
            r.half_in.at[way, dz],
            r.half_send.at[way, 0],
            r.half_recv.at[way, dz],
            (z, y, c, sides[way] if arrives else others[way]),
        )

    def unit_sum(dz, way, arrives):
        return remote(
            r.unit_out.at[way, dz],
            r.unit_in.at[way, dz],
            r.unit_send.at[way, 0],
            r.unit_recv.at[way, dz],
            (z, y, c, sides[way] if arrives else others[way]),
        )

    def sum_one(dz):
        for way in (0, 1):
            half_sum(dz, way, False).start()

    def sum_two(dz):
        start = start_of(dz)
        for way in (0, 1):
            half_sum(dz, way, True).wait_recv()
            value = r.partial[pl.ds(start, plane), :, columns(others[way])].astype(F32)
            more = r.half_in[way, dz].astype(F32)
            half = plane // 2
            parts = [value[:half], value[half:]]
            parts[way] = parts[way] + more
            r.unit_out[way, dz] = jnp.concatenate(parts, axis=0).astype(BF16)
            unit_sum(dz, way, False).start()

    def returned(j):
        dz, dy, dc = partner(j, -1)
        return remote(
            r.back_out.at[(dz * ny + dy) * nc + dc],
            r.back_in.at[me],
            r.back_send.at[0],
            r.back_recv.at[0],
            (dz, dy, dc, x),
        )

    def back_local():
        return pltpu.make_async_copy(
            r.back_out.at[me], r.back_in.at[me], r.back_recv.at[0]
        )

    def sum_three(dz):
        start = start_of(dz)
        value = r.partial[pl.ds(start, plane), :, columns(x)].astype(F32)
        for way in (0, 1):
            unit_sum(dz, way, True).wait_recv()
            value = value + r.unit_in[way, dz].astype(F32)
        r.back_out[pl.ds(start, plane)] = value.astype(BF16)

        def give(j, carry):
            returned(j).start()
            return carry

        lax.fori_loop(max(dz * plane, 1), (dz + 1) * plane, give, 0)
        if dz == 0:
            back_local().start()

    chunks = [order[k : k + 2] for k in range(0, nz - 2, 2)] + [[dz] for dz in order[-2:]]

    def sums(stage, k):
        for dz in chunks[k] if k >= 0 else ():
            stage(dz)

    def rows_of(ref):
        return ref[...].reshape(experts * capacity, -1)

    def packed(kind, cols):
        return r.pack[:, kind, :, cols].reshape(experts * capacity, -1)

    def grad_in(slope_ref, grad_ref, begin, end):
        def part(t, carry):
            cols = columns(t)
            grad_ref[cols, :] = dot(packed(0, cols), rows_of(slope_ref), 0, 0).astype(BF16)
            return carry

        lax.fori_loop(begin, end, part, 0)

    def grad_down(begin, end):
        def part(t, carry):
            cols = columns(t)
            r.grad_down[:, cols] = dot(rows_of(r.active), packed(1, cols), 0, 0).astype(BF16)
            return carry

        lax.fori_loop(begin, end, part, 0)

    for at, dz in enumerate(order):
        only_wait(ring_block(r.pack, dz, None, x), r.a_recv.at[dz]).wait_recv()
        for way in (0, 1):
            own(dz, way, False).start()
        if at:
            hand_on(order[at - 1])
        if at >= 2:
            settle(order[at - 2])
        if at >= 3 and at % 2:
            k = (at - 3) // 2
            sums(sum_two, k - 1)
            sums(sum_three, k - 2)
            expert_rows(chunks[k])
            sums(sum_one, k)
    hand_on(order[-1])
    k = len(chunks) - 2
    sums(sum_two, k - 1)
    sums(sum_three, k - 2)
    settle(order[-2])
    expert_rows(chunks[k])
    sums(sum_one, k)
    sums(sum_three, k - 1)
    settle(order[-1])
    expert_rows(chunks[k + 1])
    sums(sum_one, k + 1)
    sums(sum_two, k)
    grad_in(r.d_gate, r.grad_gate, 0, 2)
    sums(sum_two, k + 1)
    sums(sum_three, k)
    grad_in(r.d_gate, r.grad_gate, 2, nx)
    sums(sum_three, k + 1)
    grad_in(r.d_up, r.grad_up, 0, nx)

    only_wait(r.back_in, r.back_recv.at[0]).wait_recv()
    routed = dot(r.hits[...], r.back_in[...].reshape(experts * capacity, width), 0, 0)
    r.out_grad[:, columns(x)] = (r.cot_in[...].astype(F32) + routed).astype(BF16)

    half_rows = tokens // 2

    def grad_own(way, arrives):
        here = r.out_grad.at[:, columns(sides[way] if arrives else x)]
        return remote(
            here, here, r.og_send.at[way], r.og_recv.at[way],
            (z, y, c, sides[way] if arrives else others[way]),
        )

    def grad_passed(way, arrives):
        here = r.out_grad.at[
            pl.ds(way * half_rows, half_rows), columns(across if arrives else sides[way])
        ]
        return remote(
            here, here, r.og_send.at[2 + way], r.og_recv.at[2 + way],
            (z, y, c, sides[way] if arrives else others[way]),
        )

    for way in (0, 1):
        grad_own(way, False).start()

    lines = r.proj_out.shape[0]
    pair = nz // nx

    def planes(t):
        return pl.ds(t * pair, pair)

    def core_sum(t):
        return remote(
            r.term.at[planes(t), :, twin],
            r.core_in.at[planes(t)],
            r.core_send.at[t],
            r.core_recv.at[t],
            (z, y, twin, x),
        )

    def line_half(t, way, arrives):
        return remote(
            r.core_out.at[t * pair + way, over],
            r.line_half.at[way, t],
            r.line_send.at[way, t],
            r.line_recv.at[way, t],
            (z, (down, up)[way] if arrives else (up, down)[way], c, x),
        )

    def line_unit(t, way, arrives):
        return remote(
            r.line_out.at[way, planes(t)],
            r.line_in.at[way, planes(t)],
            r.line_send.at[2 + way, t],
            r.line_recv.at[2 + way, t],
            (z, (down, up)[way] if arrives else (up, down)[way], c, x),
        )

    def start_term(t):
        value = dot(r.out_grad[:, columns(t)], r.mixed[...], 0, 0)
        r.term[planes(t)] = value.reshape(pair, ny, nc, lines, width).astype(BF16)
        core_sum(t).start()

    def add_core(t):
        core_sum(t).wait_recv()
        for k in range(pair):
            row = t * pair + k
            value = r.term[row, :, pl.ds(c, 1)].reshape(ny, lines, width).astype(F32)
            r.core_out[row] = (value + r.core_in[row].astype(F32)).astype(BF16)
        for way in (0, 1):
            line_half(t, way, False).start()

    def add_half(t):
        for way in (0, 1):
            line_half(t, way, True).wait_recv()
            target = (up, down)[way]
            for k in range(pair):
                row = t * pair + k
                value = r.core_out[row, target].astype(F32)
                if k == way:
                    value = value + r.line_half[way, t].astype(F32)
                r.line_out[way, row] = value.astype(BF16)
            line_unit(t, way, False).start()

    def add_line(t):
        for way in (0, 1):
            line_unit(t, way, True).wait_recv()
        for k in range(pair):
            row = t * pair + k
            value = r.core_out[row, y].astype(F32)
            for way in (0, 1):
                value = value + r.line_in[way, row].astype(F32)
            r.last_out[row] = value.astype(BF16)

            @pl.when(row != z)
            def _():
                remote(
                    r.last_out.at[row],
                    r.last_in.at[z],
                    r.last_send.at[0],
                    r.last_recv.at[0],
                    (row, y, c, x),
                ).start()

    start_term(x)
    grad_down(0, 2)
    add_core(x)
    for way in (0, 1):
        grad_own(way, True).wait_recv()
        grad_passed(way, False).start()
    start_term(left)
    start_term(right)
    add_half(x)
    add_core(left)
    add_core(right)
    for way in (0, 1):
        grad_passed(way, True).wait_recv()
    start_term(across)

    r.d_mixed[...] = jnp.zeros_like(r.d_mixed)

    def mix(t, carry):
        cols = columns(t)
        r.d_mixed[...] += dot(r.out_grad[:, cols], r.out_proj_in[cols, :])
        return carry

    lax.fori_loop(0, nx, mix, 0)
    d_mixed = r.d_mixed[...]
    r.gate_grad[...] = (d_mixed * r.by_gate[...]).astype(BF16)
    local_grad = d_mixed * r.gate[...]
    step, level = 1, 0
    while step < tokens:
        local_grad = local_grad + r.reach[level] * pltpu.roll(local_grad, tokens - step, 0)
        step *= 2
        level += 1
    r.local_grad[...] = local_grad
    head = r.first_decay[0:1, :]
    link = jnp.concatenate(
        [
            head * r.carry_weight[0:1, :],
            head * local_grad[0:1, :],
            jnp.zeros((6, width), F32),
        ],
        axis=0,
    )
    r.near_links[mine] = link

    def near_link(j):
        _, py, pc = partner(j, 1)
        here = r.near_links.at[mine]
        return remote(here, here, r.near_send.at[0], r.near_recv.at[0], (z, py, pc, x))

    for j in range(1, plane):
        near_link(j).start()
    add_core(across)
    add_half(left)
    add_half(right)
    add_line(x)

    only_wait(r.near_links.at[pl.ds(0, plane - 1)], r.near_recv.at[0]).wait_recv()
    one, zero = jnp.ones((1, width), F32), jnp.zeros((1, width), F32)
    all_weight, all_start, near_weight, near_start = one, zero, one, zero
    for q in range(plane - 1, -1, -1):
        a, b = r.near_links[q, 0:1, :], r.near_links[q, 1:2, :]
        all_weight, all_start = a * all_weight, b + a * all_start
        later = q > mine
        near_start = jnp.where(later, b + a * near_start, near_start)
        near_weight = jnp.where(later, a * near_weight, near_weight)
    r.far_links[z] = jnp.concatenate(
        [all_weight, all_start, jnp.zeros((6, width), F32)], axis=0
    )

    def far_link(dz):
        pz, _, _ = partner(dz * plane, 1)
        here = r.far_links.at[z]
        return remote(here, here, r.far_send.at[0], r.far_recv.at[0], (pz, y, c, x))

    for dz in range(1, nz):
        far_link(dz).start()
    add_half(across)
    add_line(left)
    add_line(right)
    grad_down(2, nx)
    add_line(across)

    only_wait(r.far_links.at[pl.ds(0, nz - 1)], r.far_recv.at[0]).wait_recv()
    far_start = zero
    for q in range(nz - 1, -1, -1):
        a, b = r.far_links[q, 0:1, :], r.far_links[q, 1:2, :]
        far_start = jnp.where(q > z, b + a * far_start, far_start)
    incoming = near_start + near_weight * far_start
    state_grad = r.local_grad[...] + r.carry_weight[...] * incoming
    d_recur = (state_grad * r.by_recur[...]).astype(BF16)
    d_input = (state_grad * r.by_input[...]).astype(BF16)
    through = dot(d_recur, r.recur_map_in[0], 1, 1) + dot(d_input, r.input_map_in[0], 1, 1)
    r.conv_grad[...] = (state_grad * r.by_conv[...] + through).astype(BF16)

    only_wait(r.last_in.at[pl.ds(0, nz - 1)], r.last_recv.at[0]).wait_recv()
    total = r.last_out[z].astype(F32)
    for dz in range(1, nz):
        total = total + r.last_in[lax.rem(z + dz, nz)].astype(F32)
    r.proj_out[...] = total

    ahead = pl.ds(0, experts // 2)
    only_wait(r.sending.at[pl.ds(0, experts - 1)], r.a_send.at[0]).wait_send()
    only_wait(r.back_out.at[pl.ds(0, experts - 1)], r.back_send.at[0]).wait_send()
    for way in (0, 1):
        only_wait(r.pack.at[..., columns(x)], r.own_send.at[way, 0]).wait_send()
        only_wait(r.pack.at[ahead, :, :, columns(x)], r.hand_send.at[way, 0]).wait_send()
        only_wait(r.partial.at[ahead, :, columns(x)], r.half_send.at[way, 0]).wait_send()
        only_wait(r.unit_out.at[way], r.unit_send.at[way, 0]).wait_send()
        grad_own(way, False).wait_send()
        grad_passed(way, False).wait_send()
    only_wait(r.near_links.at[pl.ds(0, plane - 1)], r.near_send.at[0]).wait_send()
    only_wait(r.far_links.at[pl.ds(0, nz - 1)], r.far_send.at[0]).wait_send()
    for t in range(nx):
        core_sum(t).wait_send()
        for way in (0, 1):
            line_half(t, way, False).wait_send()
            line_unit(t, way, False).wait_send()
    only_wait(r.last_out.at[pl.ds(0, nz - 1)], r.last_send.at[0]).wait_send()


HELD = ("ids", "weights", "mixer", "cot")
RECURRENCE = (
    "recur_gate", "decay_rate", "conv", "input_gate", "states", "gate_pre",
)
LOADED = (*HELD, *RECURRENCE, "w_gate", "w_up", "w_down", "out_proj", "recur_map", "input_map")
IN_NAMES = LOADED
OUT_NAMES = ("grad_gate", "grad_up", "grad_down", "proj_out", "conv_grad", "gate_grad")


def scratch_of(sizes, tokens, width, hidden, held):
    nz, ny, nc, nx = sizes
    plane = ny * nc
    experts = nz * plane
    capacity = 4 * tokens // experts
    features = nx * width
    lines = features // experts
    group = plane * capacity
    levels = tokens.bit_length() - 1
    dma = pltpu.SemaphoreType.DMA
    per_token = lambda kind: pltpu.VMEM((tokens, width), kind)
    shapes = {name + "_in": pltpu.VMEM(a.shape, a.dtype) for name, a in held.items()}
    shapes |= dict(
        pack=pltpu.VMEM((experts, 2, capacity, features), BF16),
        sending=pltpu.VMEM((experts, 2, capacity, width), BF16),
        hits=pltpu.VMEM((experts * capacity, tokens), BF16),
        acc_gate=pltpu.VMEM((2 * group, hidden), F32),
        acc_up=pltpu.VMEM((2 * group, hidden), F32),
        acc_down=pltpu.VMEM((2 * group, hidden), F32),
        active=pltpu.VMEM((experts, capacity, hidden), BF16),
        d_gate=pltpu.VMEM((experts, capacity, hidden), BF16),
        d_up=pltpu.VMEM((experts, capacity, hidden), BF16),
        partial=pltpu.VMEM((experts, capacity, features), BF16),
        half_in=pltpu.VMEM((2, nz, plane // 2, capacity, width), BF16),
        unit_out=pltpu.VMEM((2, nz, plane, capacity, width), BF16),
        unit_in=pltpu.VMEM((2, nz, plane, capacity, width), BF16),
        back_out=pltpu.VMEM((experts, capacity, width), BF16),
        back_in=pltpu.VMEM((experts, capacity, width), BF16),
        out_grad=pltpu.VMEM((tokens, features), BF16),
        by_recur=per_token(F32),
        by_input=per_token(F32),
        by_conv=per_token(F32),
        by_gate=per_token(F32),
        gate=per_token(F32),
        mixed=per_token(BF16),
        first_decay=pltpu.VMEM((8, width), F32),
        reach=pltpu.VMEM((levels, tokens, width), F32),
        carry_weight=per_token(F32),
        d_mixed=per_token(F32),
        local_grad=per_token(F32),
        term=pltpu.VMEM((nz, ny, nc, lines, width), BF16),
        core_in=pltpu.VMEM((nz, ny, lines, width), BF16),
        core_out=pltpu.VMEM((nz, ny, lines, width), BF16),
        line_half=pltpu.VMEM((2, nx, lines, width), BF16),
        line_out=pltpu.VMEM((2, nz, lines, width), BF16),
        line_in=pltpu.VMEM((2, nz, lines, width), BF16),
        last_out=pltpu.VMEM((nz, lines, width), BF16),
        last_in=pltpu.VMEM((nz, lines, width), BF16),
        near_links=pltpu.VMEM((plane, 8, width), F32),
        far_links=pltpu.VMEM((nz, 8, width), F32),
        met=pltpu.SemaphoreType.REGULAR,
        load_sem=dma((len(held),)),
    )
    for name, shape in dict(
        a=(nz,),
        own=(2, nz),
        hand=(2, nz),
        half=(2, nz),
        unit=(2, nz),
        back=(1,),
        og=(4,),
        near=(1,),
        far=(1,),
        core=(nx,),
        line=(4, nx),
        last=(1,),
    ).items():
        for end in ("_send", "_recv"):
            shapes[name + end] = dma(shape)
    return shapes


SIZES = (8, 4, 2, 4)
SCRATCH_NAMES = tuple(
    scratch_of(SIZES, 128, 512, 256, {n: jax.ShapeDtypeStruct((8, 128), F32) for n in LOADED})
)


def layer(*loaded):
    sizes = tuple(lax.axis_size(a) for a in AXES)
    nz, ny, nc, nx = sizes
    named = dict(zip(LOADED, loaded, strict=True))
    tokens, width = loaded[3].shape
    hidden = named["w_gate"].shape[1]
    features = nx * width
    shapes = scratch_of(sizes, tokens, width, hidden, named)
    vmem = pl.BlockSpec(memory_space=pltpu.VMEM)
    left = pl.BlockSpec(memory_space=pltpu.HBM)
    return pl.pallas_call(
        functools.partial(layer_kernel, sizes),
        out_shape=tuple(
            pltpu.VMEM(shape, kind)
            for shape, kind in (
                ((features, hidden), BF16),
                ((features, hidden), BF16),
                ((hidden, features), BF16),
                ((features // (nz * ny * nc), width), F32),
                ((tokens, width), BF16),
                ((tokens, width), BF16),
            )
        ),
        in_specs=[left] * len(LOADED),
        out_specs=(vmem,) * len(OUT_NAMES),
        scratch_shapes=list(shapes.values()),
        compiler_params=pltpu.CompilerParams(
            collective_id=0, has_side_effects=True, vmem_limit_bytes=48 * 2**20
        ),
        name="layer",
    )(*(pltpu.with_memory_space_constraint(a, pltpu.HBM) for a in loaded))


def store_kernel(*refs):
    count = len(refs) // 2
    copies = [
        pltpu.make_async_copy(refs[k], refs[count + k], refs[-1].at[k]) for k in range(count)
    ]
    for copy in copies:
        copy.start()
    for copy in copies:
        copy.wait()


def stored(arrays):
    count = len(arrays)
    return pl.pallas_call(
        store_kernel,
        out_shape=tuple(jax.ShapeDtypeStruct(a.shape, a.dtype) for a in arrays),
        in_specs=[pl.BlockSpec(memory_space=pltpu.VMEM)] * count,
        out_specs=(pl.BlockSpec(memory_space=pl.ANY),) * count,
        scratch_shapes=[pltpu.SemaphoreType.DMA((count,))],
        name="store",
    )(*(pltpu.with_memory_space_constraint(a, pltpu.VMEM) for a in arrays))


def body(
    cotangent,
    mixer_out,
    route_ids,
    route_weights,
    conv_out,
    recur_gate,
    input_gate,
    gate_pre,
    states_before,
    decay_rate,
    out_proj,
    recur_map,
    input_map,
    expert_gate,
    expert_up,
    expert_down,
):
    grads = layer(
        route_ids.T,
        route_weights.T,
        mixer_out,
        cotangent,
        recur_gate,
        decay_rate[None, :],
        conv_out,
        input_gate,
        states_before,
        gate_pre,
        expert_gate[0],
        expert_up[0],
        expert_down[0],
        out_proj,
        recur_map,
        input_map,
    )
    grads = stored(grads)
    return (grads[0][None], grads[1][None], grads[2][None], *grads[3:])


def solution(mesh):
    torus = Mesh(mesh.devices.reshape(8, 4, 2, mesh.shape["tp"]), ("sp_0", "sp_1", "sp_2", "tp"))
    in_specs = (
        P(SP, "tp"),
        P(SP, "tp"),
        P(SP, None),
        P(SP, None),
        P(SP, "tp"),
        P(SP, "tp"),
        P(SP, "tp"),
        P(SP, "tp"),
        P(SP, "tp"),
        P("tp"),
        P(None, "tp"),
        P("tp", None, None),
        P("tp", None, None),
        P(SP, None, "tp"),
        P(SP, None, "tp"),
        P(SP, "tp", None),
    )
    out_specs = (
        P(SP, None, "tp"),
        P(SP, None, "tp"),
        P(SP, "tp", None),
        P(SP, "tp"),
        P(SP, "tp"),
        P(SP, "tp"),
    )
    return jax.shard_map(body, mesh=torus, in_specs=in_specs, out_specs=out_specs, check_vma=False)
```

```python
import functools
import types

import jax
import jax.numpy as jnp
from jax import lax
from jax.experimental import pallas as pl
from jax.experimental.pallas import tpu as pltpu
from jax.sharding import Mesh
from jax.sharding import PartitionSpec as P

SP = ("sp_0", "sp_1", "sp_2")
AXES = (*SP, "tp")
MESH_ID = pl.DeviceIdType.MESH
BF16 = jnp.bfloat16
F32 = jnp.float32


def near_first(count):
    return sorted(range(count), key=lambda k: (min(k, count - k), k))


def slot_hits(ids, experts, capacity):
    tokens = ids.shape[1]
    slots = experts * capacity
    first, second = ids[0:1, :], ids[1:2, :]
    expert = lax.broadcasted_iota(jnp.int32, (experts, tokens), 0)
    named = jnp.where((expert == first) | (expert == second), 1.0, 0.0).astype(jnp.bfloat16)
    at = lax.broadcasted_iota(jnp.int32, (tokens, tokens), 0)
    later = lax.broadcasted_iota(jnp.int32, (tokens, tokens), 1)
    earlier = jnp.where(at < later, 1.0, 0.0).astype(jnp.bfloat16)
    before = jnp.dot(named, earlier, preferred_element_type=jnp.float32)
    of_slot = lax.broadcasted_iota(jnp.int32, (slots, experts), 0)
    of_expert = lax.broadcasted_iota(jnp.int32, (slots, experts), 1)
    spread = jnp.where(of_slot // capacity == of_expert, 1.0, 0.0).astype(jnp.bfloat16)
    rank = jnp.dot(spread, before.astype(jnp.bfloat16), preferred_element_type=jnp.float32)
    slot = lax.broadcasted_iota(jnp.int32, (slots, tokens), 0)
    free = rank == (slot % capacity).astype(jnp.float32)
    return free & (slot // capacity == first), free & (slot // capacity == second)


def dot(left, right, at_left=1, at_right=0):
    return lax.dot_general(
        left, right, (((at_left,), (at_right,)), ((), ())), preferred_element_type=F32
    )


def expm1_of(v):
    series = jnp.ones_like(v)
    for n in range(11, 1, -1):
        series = 1.0 + v * series * (1.0 / n)
    return jnp.where(jnp.abs(v) < 0.5, v * series, jnp.exp(v) - 1.0)


def layer_kernel(sizes, *refs):
    names = IN_NAMES + OUT_NAMES + SCRATCH_NAMES
    r = types.SimpleNamespace(**dict(zip(names, refs, strict=True)))
    nz, ny, nc, nx = sizes
    plane = ny * nc
    experts = nz * plane
    z, y, c, x = (lax.axis_index(a) for a in AXES)
    tokens, width = r.mixed.shape
    capacity = r.sending.shape[2]
    me = (z * ny + y) * nc + c
    mine = y * nc + c
    right, left = lax.rem(x + 1, nx), lax.rem(x + nx - 1, nx)
    across = lax.rem(x + 2, nx)
    up, down = lax.rem(y + 1, ny), lax.rem(y + ny - 1, ny)
    over = lax.rem(y + 2, ny)
    twin = nc - 1 - c
    group = plane * capacity
    wide = [0, 1, nz - 1]
    ring = [dz for dz in near_first(nz) if dz not in wide]
    ring = ring[2:] + ring[:2]
    waits = []

    def columns(part):
        return pl.ds(pl.multiple_of(part * width, width), width)

    def partner(j, sign):
        dz, dy, dc = j // plane, (j // nc) % ny, j % nc
        return (
            lax.rem(z + sign * dz + nz, nz),
            lax.rem(y + sign * dy + ny, ny),
            lax.rem(c + sign * dc + nc, nc),
        )

    def remote(source, target, send, recv, device):
        return pltpu.make_async_remote_copy(
            src_ref=source,
            dst_ref=target,
            send_sem=send,
            recv_sem=recv,
            device_id=device,
            device_id_type=MESH_ID,
        )

    raw_own = [r.raw.at[k, :, columns(x)] for k in (0, 1)]
    places = [getattr(r, name + "_in", None) for name in LOADED]
    places[2:4] = raw_own
    loads = {
        name: pltpu.make_async_copy(getattr(r, name), places[k], r.load_sem.at[k])
        for k, name in enumerate(LOADED)
    }
    for name in LOADED:
        loads[name].start()

    barrier = pltpu.get_barrier_semaphore()

    def greet(sem, first, stop, step):
        def one(k, carry):
            pl.semaphore_signal(
                sem, inc=1, device_id=(*partner(k * step, 1), x), device_id_type=MESH_ID
            )
            return carry

        lax.fori_loop(first, stop, one, 0)

    greet(barrier, 1, nz, plane)
    greet(barrier, 1, plane, 1)
    for side in (left, right):
        pl.semaphore_signal(barrier, inc=1, device_id=(z, y, c, side), device_id_type=MESH_ID)

    for name in HELD:
        loads[name].wait()
    first, second = slot_hits(r.ids_in[...], experts, capacity)
    hits = jnp.where(first | second, 1.0, 0.0).astype(BF16)
    r.hits[...] = hits
    weights = r.weights_in[...]
    weight = jnp.sum(
        jnp.where(first, weights[0:1, :], 0.0) + jnp.where(second, weights[1:2, :], 0.0),
        axis=1,
        keepdims=True,
    )
    r.slot_weight[...] = jnp.broadcast_to(weight, r.slot_weight.shape)
    shape = (experts, capacity, width)
    r.sending[:, 0] = dot(hits, raw_own[0][...]).reshape(shape).astype(BF16)
    r.sending[:, 1] = (dot(hits, raw_own[1][...]) * weight).reshape(shape).astype(BF16)

    pl.semaphore_wait(barrier, nz - 1 + plane - 1 + 2)
    greet(r.met, 1, plane, 1)
    pl.semaphore_wait(r.met, plane - 1)

    def only_wait(like, sem):
        return remote(like, like, sem, sem, (z, y, twin, x))

    def sent(j):
        dz, dy, dc = partner(j, 1)
        return remote(
            r.sending.at[(dz * ny + dy) * nc + dc],
            r.pack.at[me, :, :, columns(x)],
            r.a_send.at[0],
            r.a_recv.at[j // plane],
            (dz, dy, dc, x),
        )

    sides = (left, right)
    others = (right, left)
    half_rows = tokens // 2

    def raw_sent(way, arrives):
        here = r.raw.at[:, :, columns(sides[way] if arrives else x)]
        return remote(
            here, here, r.raw_send.at[way], r.raw_recv.at[way],
            (z, y, c, sides[way] if arrives else others[way]),
        )

    def raw_passed(way, arrives):
        here = r.raw.at[
            :, pl.ds(way * half_rows, half_rows), columns(across if arrives else sides[way])
        ]
        return remote(
            here, here, r.raw_send.at[2 + way], r.raw_recv.at[2 + way],
            (z, y, c, sides[way] if arrives else others[way]),
        )

    for way in (0, 1):
        raw_sent(way, False).start()
    pltpu.make_async_copy(
        r.sending.at[me], r.pack.at[me, :, :, columns(x)], r.a_recv.at[0]
    ).start()
    for dz in (*ring, *wide):

        def send(j, carry):
            sent(j).start()
            return carry

        lax.fori_loop(max(dz * plane, 1), (dz + 1) * plane, send, 0)

    for name in RECURRENCE:
        loads[name].wait()
    recur = r.recur_gate_in[...].astype(F32)
    rate = r.decay_rate_in[...]
    log_decay = -8.0 * recur * rate
    decay = jnp.exp(log_decay)
    position = lax.broadcasted_iota(jnp.int32, (tokens, width), 0)
    at_start = (position + me * tokens) == 0
    norm = jnp.where(at_start, 1.0, jnp.sqrt(-expm1_of(2.0 * log_decay)))
    slope = jnp.where(at_start, 0.0, -jnp.exp(2.0 * log_decay) / norm)
    conv = r.conv_in[...].astype(F32)
    entry = r.input_gate_in[...].astype(F32)
    drive = entry * conv
    before = r.states_in[...].astype(F32)
    state = decay * before + norm * drive
    r.by_recur[...] = (
        (decay * before + slope * drive) * (-8.0 * rate) * recur * (1.0 - recur)
    )
    r.by_input[...] = norm * conv * entry * (1.0 - entry)
    r.by_conv[...] = norm * entry
    pre = r.gate_pre_in[...].astype(F32)
    root = 0.7978845608028654
    bent = jnp.tanh(root * (pre + 0.044715 * (pre * pre * pre)))
    cdf = 0.5 * (1.0 + bent)
    gate = pre * cdf
    gelu_slope = cdf + 0.5 * pre * (1.0 - bent * bent) * root * (1.0 + 3.0 * 0.044715 * (pre * pre))
    r.gate[...] = gate
    r.mixed[...] = (state * gate).astype(BF16)
    r.by_gate[...] = state * gelu_slope
    r.first_decay[...] = decay[0:8, :]
    following = pltpu.roll(decay, tokens - 1, 0)
    last = position == tokens - 1
    reach = jnp.where(last, 0.0, following)
    carry_weight = jnp.where(last, 1.0, following)
    step = 1
    level = 0
    while step < tokens:
        r.reach[level] = reach
        moved = pltpu.roll(reach, tokens - step, 0)
        reach = reach * moved
        moved = pltpu.roll(carry_weight, tokens - step, 0)
        carry_weight = carry_weight * jnp.where(position < tokens - step, moved, 1.0)
        step *= 2
        level += 1
    r.carry_weight[...] = carry_weight
    for name in LOADED:
        if name not in HELD + RECURRENCE:
            loads[name].wait()

    def send_wide(kind, part):
        cols = columns(part)
        for k, dz in enumerate(wide):
            to = lax.rem(z + dz, nz)
            slots = pl.ds(pl.multiple_of(to * group, group), group)
            picked = r.hits[slots, :]
            for side in (0, 1):
                value = dot(picked, r.raw[side, :, cols])
                if side:
                    value = value * r.slot_weight[slots, 0:1]
                r.wide[kind, k, :, side] = value.reshape(plane, capacity, width).astype(BF16)
            if dz == 0:
                pltpu.make_async_copy(
                    r.wide.at[kind, k, mine], r.pack.at[me, :, :, cols], r.wide_recv.at[kind, k]
                ).start()

            def give(j, carry):
                _, py, pc = partner(j, 1)
                remote(
                    r.wide.at[kind, k, py * nc + pc],
                    r.pack.at[me, :, :, cols],
                    r.wide_send.at[kind],
                    r.wide_recv.at[kind, k],
                    (to, py, pc, x),
                ).start()
                return carry

            lax.fori_loop(0 if dz else 1, plane, give, 0)

    def start_of(dz):
        return lax.rem(z - dz + nz, nz) * plane

    def ring_block(ref, dz, half, part):
        start, count = start_of(dz), plane
        if half is not None:
            count = plane // 2
            start = start + half * count
        return ref.at[pl.ds(start, count), ..., columns(part)]

    def own(dz, way, arrives):
        here = ring_block(r.pack, dz, None, sides[way] if arrives else x)
        return remote(
            here, here, r.own_send.at[way], r.own_recv.at[way, dz],
            (z, y, c, sides[way] if arrives else others[way]),
        )

    def passed(dz, way, arrives):
        here = ring_block(r.pack, dz, way, across if arrives else sides[way])
        return remote(
            here, here, r.hand_send.at[way], r.hand_recv.at[way, dz],
            (z, y, c, sides[way] if arrives else others[way]),
        )

    def hand_on(dz):
        for way in (0, 1):
            own(dz, way, True).wait_recv()
            passed(dz, way, False).start()

    def settle(dz):
        for way in (0, 1):
            passed(dz, way, True).wait_recv()

    def as_rows(kind, starts, cols):
        return jnp.concatenate(
            [r.pack[pl.ds(s, plane), kind, :, cols].reshape(group, -1) for s in starts], axis=0
        )

    def keep(ref, starts, cols, value):
        for k, s in enumerate(starts):
            part = value[k * group : (k + 1) * group]
            ref[pl.ds(s, plane), :, cols] = part.reshape(plane, capacity, -1).astype(BF16)

    def expert_rows(dzs):
        starts = [start_of(dz) for dz in dzs]
        size = pl.ds(0, len(dzs) * group)
        sums_of = [acc.at[size] for acc in (r.acc_gate, r.acc_up, r.acc_down)]
        for acc in sums_of:
            acc[...] = jnp.zeros(acc.shape, F32)

        def gather(t, carry):
            cols = columns(t)
            row_part = as_rows(0, starts, cols)
            sums_of[0][...] += dot(row_part, r.w_gate_in[cols, :])
            sums_of[1][...] += dot(row_part, r.w_up_in[cols, :])
            cot_part = as_rows(1, starts, cols)
            sums_of[2][...] += dot(cot_part, r.w_down_in[:, cols], 1, 1)
            return carry

        lax.fori_loop(0, nx, gather, 0, unroll=True)
        pre_gate, pre_up, d_active = (acc[...] for acc in sums_of)
        sig = jax.nn.sigmoid(pre_gate)
        silu = pre_gate * sig
        silu_slope = sig * (1.0 + pre_gate * (1.0 - sig))
        d_gate = d_active * pre_up * silu_slope
        d_up = d_active * silu
        whole = slice(None)
        keep(r.active, starts, whole, silu * pre_up)
        keep(r.d_gate, starts, whole, d_gate)
        keep(r.d_up, starts, whole, d_up)
        d_gate, d_up = d_gate.astype(BF16), d_up.astype(BF16)

        def spread(t, carry):
            cols = columns(t)
            value = dot(d_gate, r.w_gate_in[cols, :], 1, 1)
            value += dot(d_up, r.w_up_in[cols, :], 1, 1)
            keep(r.partial, starts, cols, value)
            return carry

        lax.fori_loop(0, nx, spread, 0, unroll=True)

    def half_sum(dz, way, arrives):
        return remote(
            ring_block(r.partial, dz, way, across),
            r.half_in.at[way, dz],
            r.half_send.at[way],
            r.half_recv.at[way, dz],
            (z, y, c, sides[way] if arrives else others[way]),
        )

    def unit_sum(dz, way, arrives):
        return remote(
            r.unit_out.at[way, dz],
            r.unit_in.at[way, dz],
            r.unit_send.at[way],
            r.unit_recv.at[way, dz],
            (z, y, c, sides[way] if arrives else others[way]),
        )

    def sum_one(dz):
        for way in (0, 1):
            half_sum(dz, way, False).start()

    def sum_two(dz):
        start = start_of(dz)
        for way in (0, 1):
            half_sum(dz, way, True).wait_recv()
            value = r.partial[pl.ds(start, plane), :, columns(others[way])].astype(F32)
            more = r.half_in[way, dz].astype(F32)
            half = plane // 2
            parts = [value[:half], value[half:]]
            parts[way] = parts[way] + more
            r.unit_out[way, dz] = jnp.concatenate(parts, axis=0).astype(BF16)
            unit_sum(dz, way, False).start()

    def returned(j):
        dz, dy, dc = partner(j, -1)
        return remote(
            r.back_out.at[(dz * ny + dy) * nc + dc],
            r.back_in.at[me],
            r.back_send.at[0],
            r.back_recv.at[0],
            (dz, dy, dc, x),
        )

    def back_local():
        return pltpu.make_async_copy(
            r.back_out.at[me], r.back_in.at[me], r.back_recv.at[0]
        )

    def sum_three(dz):
        start = start_of(dz)
        value = r.partial[pl.ds(start, plane), :, columns(x)].astype(F32)
        for way in (0, 1):
            unit_sum(dz, way, True).wait_recv()
            value = value + r.unit_in[way, dz].astype(F32)
        r.back_out[pl.ds(start, plane)] = value.astype(BF16)

        def give(j, carry):
            returned(j).start()
            return carry

        lax.fori_loop(max(dz * plane, 1), (dz + 1) * plane, give, 0)
        if dz == 0:
            back_local().start()

    chunks = [wide[:1], ring[0:2], wide[1:], ring[2:4], ring[4:]]

    def sums(stage, k):
        for dz in chunks[k] if k >= 0 else ():
            stage(dz)

    def rows_of(ref):
        return ref[...].reshape(experts * capacity, -1)

    def packed(kind, cols):
        return r.pack[:, kind, :, cols].reshape(experts * capacity, -1)

    def grad_in(slope_ref, grad_ref, begin, end):
        def part(t, carry):
            cols = columns(t)
            grad_ref[cols, :] = dot(packed(0, cols), rows_of(slope_ref), 0, 0).astype(BF16)
            return carry

        lax.fori_loop(begin, end, part, 0)

    def grad_down(begin, end):
        def part(t, carry):
            cols = columns(t)
            r.grad_down[:, cols] = dot(rows_of(r.active), packed(1, cols), 0, 0).astype(BF16)
            return carry

        lax.fori_loop(begin, end, part, 0)

    def arrived(dz):
        only_wait(ring_block(r.pack, dz, None, x), r.a_recv.at[dz]).wait_recv()
        if dz in wide:
            for kind, part in enumerate((left, right, across)):
                only_wait(ring_block(r.pack, dz, None, part), r.wide_recv.at[kind, wide.index(dz)]).wait_recv()
        else:
            for way in (0, 1):
                own(dz, way, False).start()

    def work(k):
        expert_rows(chunks[k])
        sums(sum_one, k)

    for way in (0, 1):
        raw_sent(way, True).wait_recv()
        raw_passed(way, False).start()
    for way in (0, 1):
        send_wide(way, sides[way])
    arrived(ring[0])
    for way in (0, 1):
        raw_passed(way, True).wait_recv()
    send_wide(2, across)
    arrived(ring[1])
    hand_on(ring[0])
    arrived(wide[0])
    work(0)
    arrived(ring[2])
    hand_on(ring[1])
    settle(ring[0])
    arrived(ring[3])
    hand_on(ring[2])
    settle(ring[1])
    sums(sum_two, 0)
    work(1)
    arrived(ring[4])
    hand_on(ring[3])
    settle(ring[2])
    sums(sum_two, 1)
    sums(sum_three, 0)
    hand_on(ring[4])
    for dz in wide[1:]:
        arrived(dz)
    work(2)
    settle(ring[3])
    sums(sum_three, 1)
    work(3)
    sums(sum_two, 2)
    settle(ring[4])
    work(4)
    k = 3
    sums(sum_two, k)
    sums(sum_three, 2)
    grad_in(r.d_gate, r.grad_gate, 0, 2)
    sums(sum_two, k + 1)
    sums(sum_three, k)
    grad_in(r.d_gate, r.grad_gate, 2, nx)
    sums(sum_three, k + 1)
    grad_in(r.d_up, r.grad_up, 0, nx)

    only_wait(r.back_in, r.back_recv.at[0]).wait_recv()
    routed = dot(r.hits[...], r.back_in[...].reshape(experts * capacity, width), 0, 0)
    r.out_grad[:, columns(x)] = (raw_own[1][...].astype(F32) + routed).astype(BF16)

    def grad_own(way, arrives):
        here = r.out_grad.at[:, columns(sides[way] if arrives else x)]
        return remote(
            here, here, r.og_send.at[way], r.og_recv.at[way],
            (z, y, c, sides[way] if arrives else others[way]),
        )

    def grad_passed(way, arrives):
        here = r.out_grad.at[
            pl.ds(way * half_rows, half_rows), columns(across if arrives else sides[way])
        ]
        return remote(
            here, here, r.og_send.at[2 + way], r.og_recv.at[2 + way],
            (z, y, c, sides[way] if arrives else others[way]),
        )

    for way in (0, 1):
        grad_own(way, False).start()

    lines = r.proj_out.shape[0]
    pair = nz // nx

    def planes(t):
        return pl.ds(t * pair, pair)

    def core_sum(t):
        return remote(
            r.term.at[planes(t), :, twin],
            r.core_in.at[planes(t)],
            r.core_send.at[t],
            r.core_recv.at[t],
            (z, y, twin, x),
        )

    def line_half(t, way, arrives):
        return remote(
            r.core_out.at[t * pair + way, over],
            r.line_half.at[way, t],
            r.line_send.at[way, t],
            r.line_recv.at[way, t],
            (z, (down, up)[way] if arrives else (up, down)[way], c, x),
        )

    def line_unit(t, way, arrives):
        return remote(
            r.line_out.at[way, planes(t)],
            r.line_in.at[way, planes(t)],
            r.line_send.at[2 + way, t],
            r.line_recv.at[2 + way, t],
            (z, (down, up)[way] if arrives else (up, down)[way], c, x),
        )

    def start_term(t):
        value = dot(r.out_grad[:, columns(t)], r.mixed[...], 0, 0)
        r.term[planes(t)] = value.reshape(pair, ny, nc, lines, width).astype(BF16)
        core_sum(t).start()

    def add_core(t):
        core_sum(t).wait_recv()
        for k in range(pair):
            row = t * pair + k
            value = r.term[row, :, pl.ds(c, 1)].reshape(ny, lines, width).astype(F32)
            r.core_out[row] = (value + r.core_in[row].astype(F32)).astype(BF16)
        for way in (0, 1):
            line_half(t, way, False).start()

    def add_half(t):
        for way in (0, 1):
            line_half(t, way, True).wait_recv()
            target = (up, down)[way]
            for k in range(pair):
                row = t * pair + k
                value = r.core_out[row, target].astype(F32)
                if k == way:
                    value = value + r.line_half[way, t].astype(F32)
                r.line_out[way, row] = value.astype(BF16)
            line_unit(t, way, False).start()

    def add_line(t):
        for way in (0, 1):
            line_unit(t, way, True).wait_recv()
        for k in range(pair):
            row = t * pair + k
            value = r.core_out[row, y].astype(F32)
            for way in (0, 1):
                value = value + r.line_in[way, row].astype(F32)
            r.last_out[row] = value.astype(BF16)

            @pl.when(row != z)
            def _():
                remote(
                    r.last_out.at[row],
                    r.last_in.at[z],
                    r.last_send.at[0],
                    r.last_recv.at[0],
                    (row, y, c, x),
                ).start()

    start_term(x)
    grad_down(0, 2)
    add_core(x)
    for way in (0, 1):
        grad_own(way, True).wait_recv()
        grad_passed(way, False).start()
    start_term(left)
    start_term(right)
    add_half(x)
    add_core(left)
    add_core(right)
    for way in (0, 1):
        grad_passed(way, True).wait_recv()
    start_term(across)

    r.d_mixed[...] = jnp.zeros_like(r.d_mixed)

    def mix(t, carry):
        cols = columns(t)
        r.d_mixed[...] += dot(r.out_grad[:, cols], r.out_proj_in[cols, :])
        return carry

    lax.fori_loop(0, nx, mix, 0)
    d_mixed = r.d_mixed[...]
    r.gate_grad[...] = (d_mixed * r.by_gate[...]).astype(BF16)
    local_grad = d_mixed * r.gate[...]
    step, level = 1, 0
    while step < tokens:
        local_grad = local_grad + r.reach[level] * pltpu.roll(local_grad, tokens - step, 0)
        step *= 2
        level += 1
    r.local_grad[...] = local_grad
    head = r.first_decay[0:1, :]
    link = jnp.concatenate(
        [
            head * r.carry_weight[0:1, :],
            head * local_grad[0:1, :],
            jnp.zeros((6, width), F32),
        ],
        axis=0,
    )
    r.near_links[mine] = link

    def near_link(j):
        _, py, pc = partner(j, 1)
        here = r.near_links.at[mine]
        return remote(here, here, r.near_send.at[0], r.near_recv.at[0], (z, py, pc, x))

    for j in range(1, plane):
        near_link(j).start()
    add_core(across)
    add_half(left)
    add_half(right)
    add_line(x)
    add_half(across)

    only_wait(r.near_links.at[pl.ds(0, plane - 1)], r.near_recv.at[0]).wait_recv()
    one, zero = jnp.ones((1, width), F32), jnp.zeros((1, width), F32)
    all_weight, all_start, near_weight, near_start = one, zero, one, zero
    for q in range(plane - 1, -1, -1):
        a, b = r.near_links[q, 0:1, :], r.near_links[q, 1:2, :]
        all_weight, all_start = a * all_weight, b + a * all_start
        later = q > mine
        near_start = jnp.where(later, b + a * near_start, near_start)
        near_weight = jnp.where(later, a * near_weight, near_weight)
    r.far_links[z] = jnp.concatenate(
        [all_weight, all_start, jnp.zeros((6, width), F32)], axis=0
    )

    def far_link(dz):
        pz, _, _ = partner(dz * plane, 1)
        here = r.far_links.at[z]
        return remote(here, here, r.far_send.at[0], r.far_recv.at[0], (pz, y, c, x))

    for dz in range(1, nz):
        far_link(dz).start()
    add_line(left)
    add_line(right)
    grad_down(2, nx)
    add_line(across)

    ahead = pl.ds(0, experts // 2)
    ringed = len(ring) * plane
    only_wait(r.sending.at[pl.ds(0, experts - 1)], r.a_send.at[0]).wait_send()
    only_wait(r.back_out.at[pl.ds(0, experts - 1)], r.back_send.at[0]).wait_send()
    for way in (0, 1):
        only_wait(r.pack.at[pl.ds(0, ringed), :, :, columns(x)], r.own_send.at[way]).wait_send()
        only_wait(r.pack.at[pl.ds(0, ringed // 2), :, :, columns(x)], r.hand_send.at[way]).wait_send()
        only_wait(r.partial.at[ahead, :, columns(x)], r.half_send.at[way]).wait_send()
        only_wait(r.unit_out.at[way], r.unit_send.at[way]).wait_send()
        raw_sent(way, False).wait_send()
        raw_passed(way, False).wait_send()
        grad_own(way, False).wait_send()
        grad_passed(way, False).wait_send()
    far = pl.ds(0, len(wide) * plane - 1)
    for kind in range(3):
        only_wait(r.pack.at[far, :, :, columns(x)], r.wide_send.at[kind]).wait_send()
    only_wait(r.near_links.at[pl.ds(0, plane - 1)], r.near_send.at[0]).wait_send()
    for t in range(nx):
        core_sum(t).wait_send()
        for way in (0, 1):
            line_half(t, way, False).wait_send()
            line_unit(t, way, False).wait_send()
    only_wait(r.far_links.at[pl.ds(0, nz - 1)], r.far_recv.at[0]).wait_recv()
    far_start = zero
    for q in range(nz - 1, -1, -1):
        a, b = r.far_links[q, 0:1, :], r.far_links[q, 1:2, :]
        far_start = jnp.where(q > z, b + a * far_start, far_start)
    incoming = near_start + near_weight * far_start
    state_grad = r.local_grad[...] + r.carry_weight[...] * incoming
    d_recur = (state_grad * r.by_recur[...]).astype(BF16)
    d_input = (state_grad * r.by_input[...]).astype(BF16)
    through = dot(d_recur, r.recur_map_in[0], 1, 1) + dot(d_input, r.input_map_in[0], 1, 1)
    r.conv_grad[...] = (state_grad * r.by_conv[...] + through).astype(BF16)

    only_wait(r.last_in.at[pl.ds(0, nz - 1)], r.last_recv.at[0]).wait_recv()
    total = r.last_out[z].astype(F32)
    for dz in range(1, nz):
        total = total + r.last_in[lax.rem(z + dz, nz)].astype(F32)
    r.proj_out[...] = total

    only_wait(r.far_links.at[pl.ds(0, nz - 1)], r.far_send.at[0]).wait_send()
    only_wait(r.last_out.at[pl.ds(0, nz - 1)], r.last_send.at[0]).wait_send()


HELD = ("ids", "weights", "mixer", "cot")
RECURRENCE = (
    "recur_gate", "decay_rate", "conv", "input_gate", "states", "gate_pre",
)
LOADED = (*HELD, *RECURRENCE, "w_gate", "w_up", "w_down", "out_proj", "recur_map", "input_map")
IN_NAMES = LOADED
OUT_NAMES = ("grad_gate", "grad_up", "grad_down", "proj_out", "conv_grad", "gate_grad")


def scratch_of(sizes, tokens, width, hidden, held):
    nz, ny, nc, nx = sizes
    plane = ny * nc
    experts = nz * plane
    capacity = 4 * tokens // experts
    features = nx * width
    lines = features // experts
    group = plane * capacity
    levels = tokens.bit_length() - 1
    dma = pltpu.SemaphoreType.DMA
    per_token = lambda kind: pltpu.VMEM((tokens, width), kind)
    shapes = {
        name + "_in": pltpu.VMEM(a.shape, a.dtype)
        for name, a in held.items()
        if name not in HELD[2:]
    }
    shapes |= dict(
        pack=pltpu.VMEM((experts, 2, capacity, features), BF16),
        raw=pltpu.VMEM((2, tokens, features), BF16),
        slot_weight=pltpu.VMEM((experts * capacity, 128), F32),
        wide=pltpu.VMEM((3, 3, plane, 2, capacity, width), BF16),
        sending=pltpu.VMEM((experts, 2, capacity, width), BF16),
        hits=pltpu.VMEM((experts * capacity, tokens), BF16),
        acc_gate=pltpu.VMEM((2 * group, hidden), F32),
        acc_up=pltpu.VMEM((2 * group, hidden), F32),
        acc_down=pltpu.VMEM((2 * group, hidden), F32),
        active=pltpu.VMEM((experts, capacity, hidden), BF16),
        d_gate=pltpu.VMEM((experts, capacity, hidden), BF16),
        d_up=pltpu.VMEM((experts, capacity, hidden), BF16),
        partial=pltpu.VMEM((experts, capacity, features), BF16),
        half_in=pltpu.VMEM((2, nz, plane // 2, capacity, width), BF16),
        unit_out=pltpu.VMEM((2, nz, plane, capacity, width), BF16),
        unit_in=pltpu.VMEM((2, nz, plane, capacity, width), BF16),
        back_out=pltpu.VMEM((experts, capacity, width), BF16),
        back_in=pltpu.VMEM((experts, capacity, width), BF16),
        out_grad=pltpu.VMEM((tokens, features), BF16),
        by_recur=per_token(F32),
        by_input=per_token(F32),
        by_conv=per_token(F32),
        by_gate=per_token(F32),
        gate=per_token(F32),
        mixed=per_token(BF16),
        first_decay=pltpu.VMEM((8, width), F32),
        reach=pltpu.VMEM((levels, tokens, width), F32),
        carry_weight=per_token(F32),
        d_mixed=per_token(F32),
        local_grad=per_token(F32),
        term=pltpu.VMEM((nz, ny, nc, lines, width), BF16),
        core_in=pltpu.VMEM((nz, ny, lines, width), BF16),
        core_out=pltpu.VMEM((nz, ny, lines, width), BF16),
        line_half=pltpu.VMEM((2, nx, lines, width), BF16),
        line_out=pltpu.VMEM((2, nz, lines, width), BF16),
        line_in=pltpu.VMEM((2, nz, lines, width), BF16),
        last_out=pltpu.VMEM((nz, lines, width), BF16),
        last_in=pltpu.VMEM((nz, lines, width), BF16),
        near_links=pltpu.VMEM((plane, 8, width), F32),
        far_links=pltpu.VMEM((nz, 8, width), F32),
        met=pltpu.SemaphoreType.REGULAR,
        load_sem=dma((len(held),)),
    )
    for name, (send, recv) in dict(
        a=((1,), (nz,)),
        own=((2,), (2, nz)),
        hand=((2,), (2, nz)),
        half=((2,), (2, nz)),
        unit=((2,), (2, nz)),
        back=((1,), (1,)),
        raw=((4,), (4,)),
        wide=((3,), (3, 3)),
        og=((4,), (4,)),
        near=((1,), (1,)),
        far=((1,), (1,)),
        core=((nx,), (nx,)),
        line=((4, nx), (4, nx)),
        last=((1,), (1,)),
    ).items():
        shapes[name + "_send"] = dma(send)
        shapes[name + "_recv"] = dma(recv)
    return shapes


SIZES = (8, 4, 2, 4)
SCRATCH_NAMES = tuple(
    scratch_of(SIZES, 128, 512, 256, {n: jax.ShapeDtypeStruct((8, 128), F32) for n in LOADED})
)


def layer(*loaded):
    sizes = tuple(lax.axis_size(a) for a in AXES)
    nz, ny, nc, nx = sizes
    named = dict(zip(LOADED, loaded, strict=True))
    tokens, width = loaded[3].shape
    hidden = named["w_gate"].shape[1]
    features = nx * width
    shapes = scratch_of(sizes, tokens, width, hidden, named)
    vmem = pl.BlockSpec(memory_space=pltpu.VMEM)
    left = pl.BlockSpec(memory_space=pltpu.HBM)
    return pl.pallas_call(
        functools.partial(layer_kernel, sizes),
        out_shape=tuple(
            pltpu.VMEM(shape, kind)
            for shape, kind in (
                ((features, hidden), BF16),
                ((features, hidden), BF16),
                ((hidden, features), BF16),
                ((features // (nz * ny * nc), width), F32),
                ((tokens, width), BF16),
                ((tokens, width), BF16),
            )
        ),
        in_specs=[left] * len(LOADED),
        out_specs=(vmem,) * len(OUT_NAMES),
        scratch_shapes=list(shapes.values()),
        compiler_params=pltpu.CompilerParams(
            collective_id=0, has_side_effects=True, vmem_limit_bytes=48 * 2**20
        ),
        name="layer",
    )(*(pltpu.with_memory_space_constraint(a, pltpu.HBM) for a in loaded))


def store_kernel(*refs):
    count = len(refs) // 2
    copies = [
        pltpu.make_async_copy(refs[k], refs[count + k], refs[-1].at[k]) for k in range(count)
    ]
    for copy in copies:
        copy.start()
    for copy in copies:
        copy.wait()


def stored(arrays):
    count = len(arrays)
    return pl.pallas_call(
        store_kernel,
        out_shape=tuple(jax.ShapeDtypeStruct(a.shape, a.dtype) for a in arrays),
        in_specs=[pl.BlockSpec(memory_space=pltpu.VMEM)] * count,
        out_specs=(pl.BlockSpec(memory_space=pl.ANY),) * count,
        scratch_shapes=[pltpu.SemaphoreType.DMA((count,))],
        name="store",
    )(*(pltpu.with_memory_space_constraint(a, pltpu.VMEM) for a in arrays))


def body(
    cotangent,
    mixer_out,
    route_ids,
    route_weights,
    conv_out,
    recur_gate,
    input_gate,
    gate_pre,
    states_before,
    decay_rate,
    out_proj,
    recur_map,
    input_map,
    expert_gate,
    expert_up,
    expert_down,
):
    grads = layer(
        route_ids.T,
        route_weights.T,
        mixer_out,
        cotangent,
        recur_gate,
        decay_rate[None, :],
        conv_out,
        input_gate,
        states_before,
        gate_pre,
        expert_gate[0],
        expert_up[0],
        expert_down[0],
        out_proj,
        recur_map,
        input_map,
    )
    grads = stored(grads)
    return (grads[0][None], grads[1][None], grads[2][None], *grads[3:])


def solution(mesh):
    torus = Mesh(mesh.devices.reshape(8, 4, 2, mesh.shape["tp"]), ("sp_0", "sp_1", "sp_2", "tp"))
    in_specs = (
        P(SP, "tp"),
        P(SP, "tp"),
        P(SP, None),
        P(SP, None),
        P(SP, "tp"),
        P(SP, "tp"),
        P(SP, "tp"),
        P(SP, "tp"),
        P(SP, "tp"),
        P("tp"),
        P(None, "tp"),
        P("tp", None, None),
        P("tp", None, None),
        P(SP, None, "tp"),
        P(SP, None, "tp"),
        P(SP, "tp", None),
    )
    out_specs = (
        P(SP, None, "tp"),
        P(SP, None, "tp"),
        P(SP, "tp", None),
        P(SP, "tp"),
        P(SP, "tp"),
        P(SP, "tp"),
    )
    return jax.shard_map(body, mesh=torus, in_specs=in_specs, out_specs=out_specs, check_vma=False)
```

```python
import functools
import types

import jax
import jax.numpy as jnp
from jax import lax
from jax.experimental import pallas as pl
from jax.experimental.pallas import tpu as pltpu
from jax.sharding import Mesh
from jax.sharding import PartitionSpec as P

SP = ("sp_0", "sp_1", "sp_2")
AXES = (*SP, "tp")
MESH_ID = pl.DeviceIdType.MESH
BF16 = jnp.bfloat16
F32 = jnp.float32


def near_first(count):
    return sorted(range(count), key=lambda k: (min(k, count - k), k))


def slot_hits(ids, experts, capacity):
    tokens = ids.shape[1]
    slots = experts * capacity
    first, second = ids[0:1, :], ids[1:2, :]
    expert = lax.broadcasted_iota(jnp.int32, (experts, tokens), 0)
    named = jnp.where((expert == first) | (expert == second), 1.0, 0.0).astype(jnp.bfloat16)
    at = lax.broadcasted_iota(jnp.int32, (tokens, tokens), 0)
    later = lax.broadcasted_iota(jnp.int32, (tokens, tokens), 1)
    earlier = jnp.where(at < later, 1.0, 0.0).astype(jnp.bfloat16)
    before = jnp.dot(named, earlier, preferred_element_type=jnp.float32)
    of_slot = lax.broadcasted_iota(jnp.int32, (slots, experts), 0)
    of_expert = lax.broadcasted_iota(jnp.int32, (slots, experts), 1)
    spread = jnp.where(of_slot // capacity == of_expert, 1.0, 0.0).astype(jnp.bfloat16)
    rank = jnp.dot(spread, before.astype(jnp.bfloat16), preferred_element_type=jnp.float32)
    slot = lax.broadcasted_iota(jnp.int32, (slots, tokens), 0)
    free = rank == (slot % capacity).astype(jnp.float32)
    return free & (slot // capacity == first), free & (slot // capacity == second)


def dot(left, right, at_left=1, at_right=0):
    return lax.dot_general(
        left, right, (((at_left,), (at_right,)), ((), ())), preferred_element_type=F32
    )


def expm1_of(v):
    series = jnp.ones_like(v)
    for n in range(11, 1, -1):
        series = 1.0 + v * series * (1.0 / n)
    return jnp.where(jnp.abs(v) < 0.5, v * series, jnp.exp(v) - 1.0)


def layer_kernel(sizes, *refs):
    names = IN_NAMES + OUT_NAMES + SCRATCH_NAMES
    r = types.SimpleNamespace(**dict(zip(names, refs, strict=True)))
    nz, ny, nc, nx = sizes
    plane = ny * nc
    experts = nz * plane
    z, y, c, x = (lax.axis_index(a) for a in AXES)
    tokens, width = r.mixed.shape
    capacity = r.sending.shape[2]
    me = (z * ny + y) * nc + c
    mine = y * nc + c
    right, left = lax.rem(x + 1, nx), lax.rem(x + nx - 1, nx)
    across = lax.rem(x + 2, nx)
    up, down = lax.rem(y + 1, ny), lax.rem(y + ny - 1, ny)
    over = lax.rem(y + 2, ny)
    twin = nc - 1 - c
    group = plane * capacity
    wide = [0, 1, nz - 1]
    ring = [dz for dz in near_first(nz) if dz not in wide]
    ring = ring[2:] + ring[:2]
    waits = []

    def columns(part):
        return pl.ds(pl.multiple_of(part * width, width), width)

    def partner(j, sign):
        dz, dy, dc = j // plane, (j // nc) % ny, j % nc
        return (
            lax.rem(z + sign * dz + nz, nz),
            lax.rem(y + sign * dy + ny, ny),
            lax.rem(c + sign * dc + nc, nc),
        )

    def remote(source, target, send, recv, device):
        return pltpu.make_async_remote_copy(
            src_ref=source,
            dst_ref=target,
            send_sem=send,
            recv_sem=recv,
            device_id=device,
            device_id_type=MESH_ID,
        )

    raw_own = [r.raw.at[k, :, columns(x)] for k in (0, 1)]
    places = [getattr(r, name + "_in", None) for name in LOADED]
    places[2:4] = raw_own
    loads = {
        name: pltpu.make_async_copy(getattr(r, name), places[k], r.load_sem.at[k])
        for k, name in enumerate(LOADED)
    }
    for name in LOADED:
        loads[name].start()

    barrier = pltpu.get_barrier_semaphore()

    def greet(sem, first, stop, step):
        def one(k, carry):
            pl.semaphore_signal(
                sem, inc=1, device_id=(*partner(k * step, 1), x), device_id_type=MESH_ID
            )
            return carry

        lax.fori_loop(first, stop, one, 0)

    greet(barrier, 1, nz, plane)
    greet(barrier, 1, plane, 1)
    for side in (left, right):
        pl.semaphore_signal(barrier, inc=1, device_id=(z, y, c, side), device_id_type=MESH_ID)

    for name in HELD:
        loads[name].wait()
    first, second = slot_hits(r.ids_in[...], experts, capacity)
    hits = jnp.where(first | second, 1.0, 0.0).astype(BF16)
    r.hits[...] = hits
    weights = r.weights_in[...]
    weight = jnp.sum(
        jnp.where(first, weights[0:1, :], 0.0) + jnp.where(second, weights[1:2, :], 0.0),
        axis=1,
        keepdims=True,
    )
    r.slot_weight[...] = jnp.broadcast_to(weight, r.slot_weight.shape)
    shape = (experts, capacity, width)
    r.sending[:, 0] = dot(hits, raw_own[0][...]).reshape(shape).astype(BF16)
    r.sending[:, 1] = (dot(hits, raw_own[1][...]) * weight).reshape(shape).astype(BF16)

    pl.semaphore_wait(barrier, nz - 1 + plane - 1 + 2)
    greet(r.met, 1, plane, 1)
    pl.semaphore_wait(r.met, plane - 1)

    def only_wait(like, sem):
        return remote(like, like, sem, sem, (z, y, twin, x))

    def sent(j):
        dz, dy, dc = partner(j, 1)
        return remote(
            r.sending.at[(dz * ny + dy) * nc + dc],
            r.pack.at[me, :, :, columns(x)],
            r.a_send.at[0],
            r.a_recv.at[j // plane],
            (dz, dy, dc, x),
        )

    sides = (left, right)
    others = (right, left)
    half_rows = tokens // 2

    def ring_gather(view, send, recv):
        def step(kind, way, arrives):
            half = 1 - way if kind == 1 else way
            if kind == 2:
                part = across if arrives else sides[way]
            else:
                part = sides[way] if arrives else x
            here = view(pl.ds(half * half_rows, half_rows), columns(part))
            return remote(
                here, here, send.at[kind, way], recv.at[kind, way],
                (z, y, c, sides[way] if arrives else others[way]),
            )

        return step

    raw_step = ring_gather(lambda rows, cols: r.raw.at[:, rows, cols], r.raw_send, r.raw_recv)
    for kind in (0, 1):
        for way in (0, 1):
            raw_step(kind, way, False).start()
    pltpu.make_async_copy(
        r.sending.at[me], r.pack.at[me, :, :, columns(x)], r.a_recv.at[0]
    ).start()
    for dz in (*ring, *wide):

        def send(j, carry):
            sent(j).start()
            return carry

        lax.fori_loop(max(dz * plane, 1), (dz + 1) * plane, send, 0)

    for name in RECURRENCE:
        loads[name].wait()
    recur = r.recur_gate_in[...].astype(F32)
    rate = r.decay_rate_in[...]
    log_decay = -8.0 * recur * rate
    decay = jnp.exp(log_decay)
    position = lax.broadcasted_iota(jnp.int32, (tokens, width), 0)
    at_start = (position + me * tokens) == 0
    norm = jnp.where(at_start, 1.0, jnp.sqrt(-expm1_of(2.0 * log_decay)))
    slope = jnp.where(at_start, 0.0, -jnp.exp(2.0 * log_decay) / norm)
    conv = r.conv_in[...].astype(F32)
    entry = r.input_gate_in[...].astype(F32)
    drive = entry * conv
    before = r.states_in[...].astype(F32)
    state = decay * before + norm * drive
    r.by_recur[...] = (
        (decay * before + slope * drive) * (-8.0 * rate) * recur * (1.0 - recur)
    )
    r.by_input[...] = norm * conv * entry * (1.0 - entry)
    r.by_conv[...] = norm * entry
    pre = r.gate_pre_in[...].astype(F32)
    root = 0.7978845608028654
    bent = jnp.tanh(root * (pre + 0.044715 * (pre * pre * pre)))
    cdf = 0.5 * (1.0 + bent)
    gate = pre * cdf
    gelu_slope = cdf + 0.5 * pre * (1.0 - bent * bent) * root * (1.0 + 3.0 * 0.044715 * (pre * pre))
    r.gate[...] = gate
    r.mixed[...] = (state * gate).astype(BF16)
    r.by_gate[...] = state * gelu_slope
    r.first_decay[...] = decay[0:8, :]
    following = pltpu.roll(decay, tokens - 1, 0)
    last = position == tokens - 1
    reach = jnp.where(last, 0.0, following)
    carry_weight = jnp.where(last, 1.0, following)
    step = 1
    level = 0
    while step < tokens:
        r.reach[level] = reach
        moved = pltpu.roll(reach, tokens - step, 0)
        reach = reach * moved
        moved = pltpu.roll(carry_weight, tokens - step, 0)
        carry_weight = carry_weight * jnp.where(position < tokens - step, moved, 1.0)
        step *= 2
        level += 1
    r.carry_weight[...] = carry_weight
    for name in LOADED:
        if name not in HELD + RECURRENCE:
            loads[name].wait()

    def send_wide(kind, part):
        cols = columns(part)
        for k, dz in enumerate(wide):
            to = lax.rem(z + dz, nz)
            slots = pl.ds(pl.multiple_of(to * group, group), group)
            picked = r.hits[slots, :]
            for side in (0, 1):
                value = dot(picked, r.raw[side, :, cols])
                if side:
                    value = value * r.slot_weight[slots, 0:1]
                r.wide[kind, k, :, side] = value.reshape(plane, capacity, width).astype(BF16)
            if dz == 0:
                pltpu.make_async_copy(
                    r.wide.at[kind, k, mine], r.pack.at[me, :, :, cols], r.wide_recv.at[kind, k]
                ).start()

            def give(j, carry):
                _, py, pc = partner(j, 1)
                remote(
                    r.wide.at[kind, k, py * nc + pc],
                    r.pack.at[me, :, :, cols],
                    r.wide_send.at[kind],
                    r.wide_recv.at[kind, k],
                    (to, py, pc, x),
                ).start()
                return carry

            lax.fori_loop(0 if dz else 1, plane, give, 0)

    def start_of(dz):
        return lax.rem(z - dz + nz, nz) * plane

    def ring_block(ref, dz, half, part):
        start, count = start_of(dz), plane
        if half is not None:
            count = plane // 2
            start = start + half * count
        return ref.at[pl.ds(start, count), ..., columns(part)]

    def own(dz, way, arrives):
        here = ring_block(r.pack, dz, None, sides[way] if arrives else x)
        return remote(
            here, here, r.own_send.at[way], r.own_recv.at[way, dz],
            (z, y, c, sides[way] if arrives else others[way]),
        )

    def passed(dz, way, arrives):
        here = ring_block(r.pack, dz, way, across if arrives else sides[way])
        return remote(
            here, here, r.hand_send.at[way], r.hand_recv.at[way, dz],
            (z, y, c, sides[way] if arrives else others[way]),
        )

    def hand_on(dz):
        for way in (0, 1):
            own(dz, way, True).wait_recv()
            passed(dz, way, False).start()

    def settle(dz):
        for way in (0, 1):
            passed(dz, way, True).wait_recv()

    def as_rows(kind, starts, cols):
        return jnp.concatenate(
            [r.pack[pl.ds(s, plane), kind, :, cols].reshape(group, -1) for s in starts], axis=0
        )

    def keep(ref, starts, cols, value):
        for k, s in enumerate(starts):
            part = value[k * group : (k + 1) * group]
            ref[pl.ds(s, plane), :, cols] = part.reshape(plane, capacity, -1).astype(BF16)

    def expert_rows(dzs):
        starts = [start_of(dz) for dz in dzs]
        size = pl.ds(0, len(dzs) * group)
        sums_of = [acc.at[size] for acc in (r.acc_gate, r.acc_up, r.acc_down)]
        for acc in sums_of:
            acc[...] = jnp.zeros(acc.shape, F32)

        def gather(t, carry):
            cols = columns(t)
            row_part = as_rows(0, starts, cols)
            sums_of[0][...] += dot(row_part, r.w_gate_in[cols, :])
            sums_of[1][...] += dot(row_part, r.w_up_in[cols, :])
            cot_part = as_rows(1, starts, cols)
            sums_of[2][...] += dot(cot_part, r.w_down_in[:, cols], 1, 1)
            return carry

        lax.fori_loop(0, nx, gather, 0, unroll=True)
        pre_gate, pre_up, d_active = (acc[...] for acc in sums_of)
        sig = jax.nn.sigmoid(pre_gate)
        silu = pre_gate * sig
        silu_slope = sig * (1.0 + pre_gate * (1.0 - sig))
        d_gate = d_active * pre_up * silu_slope
        d_up = d_active * silu
        whole = slice(None)
        keep(r.active, starts, whole, silu * pre_up)
        keep(r.d_gate, starts, whole, d_gate)
        keep(r.d_up, starts, whole, d_up)
        d_gate, d_up = d_gate.astype(BF16), d_up.astype(BF16)

        def spread(t, carry):
            cols = columns(t)
            value = dot(d_gate, r.w_gate_in[cols, :], 1, 1)
            value += dot(d_up, r.w_up_in[cols, :], 1, 1)
            keep(r.partial, starts, cols, value)
            return carry

        lax.fori_loop(0, nx, spread, 0, unroll=True)

    def half_sum(dz, way, arrives):
        return remote(
            ring_block(r.partial, dz, way, across),
            r.half_in.at[way, dz],
            r.half_send.at[way],
            r.half_recv.at[way, dz],
            (z, y, c, sides[way] if arrives else others[way]),
        )

    def unit_sum(dz, way, arrives):
        return remote(
            r.unit_out.at[way, dz],
            r.unit_in.at[way, dz],
            r.unit_send.at[way],
            r.unit_recv.at[way, dz],
            (z, y, c, sides[way] if arrives else others[way]),
        )

    def sum_one(dz):
        for way in (0, 1):
            half_sum(dz, way, False).start()

    def sum_two(dz):
        start = start_of(dz)
        for way in (0, 1):
            half_sum(dz, way, True).wait_recv()
            value = r.partial[pl.ds(start, plane), :, columns(others[way])].astype(F32)
            more = r.half_in[way, dz].astype(F32)
            half = plane // 2
            parts = [value[:half], value[half:]]
            parts[way] = parts[way] + more
            r.unit_out[way, dz] = jnp.concatenate(parts, axis=0).astype(BF16)
            unit_sum(dz, way, False).start()

    def returned(j):
        dz, dy, dc = partner(j, -1)
        return remote(
            r.back_out.at[(dz * ny + dy) * nc + dc],
            r.back_in.at[me],
            r.back_send.at[0],
            r.back_recv.at[0],
            (dz, dy, dc, x),
        )

    def back_local():
        return pltpu.make_async_copy(
            r.back_out.at[me], r.back_in.at[me], r.back_recv.at[0]
        )

    def sum_three(dz):
        start = start_of(dz)
        value = r.partial[pl.ds(start, plane), :, columns(x)].astype(F32)
        for way in (0, 1):
            unit_sum(dz, way, True).wait_recv()
            value = value + r.unit_in[way, dz].astype(F32)
        r.back_out[pl.ds(start, plane)] = value.astype(BF16)

        def give(j, carry):
            returned(j).start()
            return carry

        lax.fori_loop(max(dz * plane, 1), (dz + 1) * plane, give, 0)
        if dz == 0:
            back_local().start()

    chunks = [wide[:1], ring[0:2], ring[2:3], wide[1:], ring[3:]]

    def sums(stage, k):
        for dz in chunks[k] if k >= 0 else ():
            stage(dz)

    def rows_of(ref):
        return ref[...].reshape(experts * capacity, -1)

    def packed(kind, cols):
        return r.pack[:, kind, :, cols].reshape(experts * capacity, -1)

    def grad_in(slope_ref, grad_ref, begin, end):
        def part(t, carry):
            cols = columns(t)
            grad_ref[cols, :] = dot(packed(0, cols), rows_of(slope_ref), 0, 0).astype(BF16)
            return carry

        lax.fori_loop(begin, end, part, 0)

    def grad_down(begin, end):
        def part(t, carry):
            cols = columns(t)
            r.grad_down[:, cols] = dot(rows_of(r.active), packed(1, cols), 0, 0).astype(BF16)
            return carry

        lax.fori_loop(begin, end, part, 0)

    def arrived(dz):
        only_wait(ring_block(r.pack, dz, None, x), r.a_recv.at[dz]).wait_recv()
        if dz in wide:
            for kind, part in enumerate((left, right, across)):
                only_wait(ring_block(r.pack, dz, None, part), r.wide_recv.at[kind, wide.index(dz)]).wait_recv()
        else:
            for way in (0, 1):
                own(dz, way, False).start()

    def work(k):
        expert_rows(chunks[k])
        sums(sum_one, k)

    for way in (0, 1):
        raw_step(0, way, True).wait_recv()
        raw_step(2, way, False).start()
    for way in (0, 1):
        raw_step(1, way, True).wait_recv()
        send_wide(way, sides[way])
    arrived(ring[0])
    for way in (0, 1):
        raw_step(2, way, True).wait_recv()
    send_wide(2, across)
    arrived(ring[1])
    hand_on(ring[0])
    arrived(wide[0])
    work(0)
    arrived(ring[2])
    hand_on(ring[1])
    settle(ring[0])
    arrived(ring[3])
    hand_on(ring[2])
    settle(ring[1])
    arrived(ring[4])
    sums(sum_two, 0)
    expert_rows(chunks[1])
    hand_on(ring[3])
    sums(sum_one, 1)
    settle(ring[2])
    hand_on(ring[4])
    expert_rows(chunks[2])
    sums(sum_two, 1)
    sums(sum_one, 2)
    sums(sum_three, 0)
    for dz in wide[1:]:
        arrived(dz)
    work(3)
    settle(ring[3])
    settle(ring[4])
    work(4)
    sums(sum_three, 1)
    sums(sum_two, 2)
    sums(sum_two, 3)
    grad_in(r.d_gate, r.grad_gate, 0, 2)
    sums(sum_two, 4)
    sums(sum_three, 2)
    sums(sum_three, 3)
    grad_in(r.d_gate, r.grad_gate, 2, nx)
    sums(sum_three, 4)
    grad_in(r.d_up, r.grad_up, 0, nx)

    only_wait(r.back_in, r.back_recv.at[0]).wait_recv()
    routed = dot(r.hits[...], r.back_in[...].reshape(experts * capacity, width), 0, 0)
    r.out_grad[:, columns(x)] = (raw_own[1][...].astype(F32) + routed).astype(BF16)

    grad_step = ring_gather(lambda rows, cols: r.out_grad.at[rows, cols], r.og_send, r.og_recv)
    for kind in (0, 1):
        for way in (0, 1):
            grad_step(kind, way, False).start()

    lines = r.proj_out.shape[0]
    pair = nz // nx

    def planes(t):
        return pl.ds(t * pair, pair)

    def core_sum(t):
        return remote(
            r.term.at[planes(t), :, twin],
            r.core_in.at[planes(t)],
            r.core_send.at[t],
            r.core_recv.at[t],
            (z, y, twin, x),
        )

    def line_half(t, way, arrives):
        return remote(
            r.core_out.at[t * pair + way, over],
            r.line_half.at[way, t],
            r.line_send.at[way, t],
            r.line_recv.at[way, t],
            (z, (down, up)[way] if arrives else (up, down)[way], c, x),
        )

    def line_unit(t, way, arrives):
        return remote(
            r.line_out.at[way, planes(t)],
            r.line_in.at[way, planes(t)],
            r.line_send.at[2 + way, t],
            r.line_recv.at[2 + way, t],
            (z, (down, up)[way] if arrives else (up, down)[way], c, x),
        )

    def start_term(t):
        value = dot(r.out_grad[:, columns(t)], r.mixed[...], 0, 0)
        r.term[planes(t)] = value.reshape(pair, ny, nc, lines, width).astype(BF16)
        core_sum(t).start()

    def add_core(t):
        core_sum(t).wait_recv()
        for k in range(pair):
            row = t * pair + k
            value = r.term[row, :, pl.ds(c, 1)].reshape(ny, lines, width).astype(F32)
            r.core_out[row] = (value + r.core_in[row].astype(F32)).astype(BF16)
        for way in (0, 1):
            line_half(t, way, False).start()

    def add_half(t):
        for way in (0, 1):
            line_half(t, way, True).wait_recv()
            target = (up, down)[way]
            for k in range(pair):
                row = t * pair + k
                value = r.core_out[row, target].astype(F32)
                if k == way:
                    value = value + r.line_half[way, t].astype(F32)
                r.line_out[way, row] = value.astype(BF16)
            line_unit(t, way, False).start()

    def add_line(t):
        for way in (0, 1):
            line_unit(t, way, True).wait_recv()
        for k in range(pair):
            row = t * pair + k
            value = r.core_out[row, y].astype(F32)
            for way in (0, 1):
                value = value + r.line_in[way, row].astype(F32)
            r.last_out[row] = value.astype(BF16)

            @pl.when(row != z)
            def _():
                remote(
                    r.last_out.at[row],
                    r.last_in.at[z],
                    r.last_send.at[0],
                    r.last_recv.at[0],
                    (row, y, c, x),
                ).start()

    start_term(x)
    grad_down(0, 2)
    add_core(x)
    for way in (0, 1):
        grad_step(0, way, True).wait_recv()
        grad_step(2, way, False).start()
    add_half(x)
    for way in (0, 1):
        grad_step(1, way, True).wait_recv()
        start_term(sides[way])
    add_core(left)
    add_core(right)
    for way in (0, 1):
        grad_step(2, way, True).wait_recv()
    start_term(across)

    r.d_mixed[...] = jnp.zeros_like(r.d_mixed)

    def mix(t, carry):
        cols = columns(t)
        r.d_mixed[...] += dot(r.out_grad[:, cols], r.out_proj_in[cols, :])
        return carry

    lax.fori_loop(0, nx, mix, 0)
    d_mixed = r.d_mixed[...]
    r.gate_grad[...] = (d_mixed * r.by_gate[...]).astype(BF16)
    local_grad = d_mixed * r.gate[...]
    step, level = 1, 0
    while step < tokens:
        local_grad = local_grad + r.reach[level] * pltpu.roll(local_grad, tokens - step, 0)
        step *= 2
        level += 1
    r.local_grad[...] = local_grad
    head = r.first_decay[0:1, :]
    link = jnp.concatenate(
        [
            head * r.carry_weight[0:1, :],
            head * local_grad[0:1, :],
            jnp.zeros((6, width), F32),
        ],
        axis=0,
    )
    r.near_links[mine] = link

    def near_link(j):
        _, py, pc = partner(j, 1)
        here = r.near_links.at[mine]
        return remote(here, here, r.near_send.at[0], r.near_recv.at[0], (z, py, pc, x))

    for j in range(1, plane):
        near_link(j).start()
    add_core(across)
    add_half(left)
    add_half(right)
    add_half(across)

    only_wait(r.near_links.at[pl.ds(0, plane - 1)], r.near_recv.at[0]).wait_recv()
    one, zero = jnp.ones((1, width), F32), jnp.zeros((1, width), F32)
    all_weight, all_start, near_weight, near_start = one, zero, one, zero
    for q in range(plane - 1, -1, -1):
        a, b = r.near_links[q, 0:1, :], r.near_links[q, 1:2, :]
        all_weight, all_start = a * all_weight, b + a * all_start
        later = q > mine
        near_start = jnp.where(later, b + a * near_start, near_start)
        near_weight = jnp.where(later, a * near_weight, near_weight)
    r.far_links[z] = jnp.concatenate(
        [all_weight, all_start, jnp.zeros((6, width), F32)], axis=0
    )

    def far_link(dz):
        pz, _, _ = partner(dz * plane, 1)
        here = r.far_links.at[z]
        return remote(here, here, r.far_send.at[0], r.far_recv.at[0], (pz, y, c, x))

    for dz in range(1, nz):
        far_link(dz).start()
    add_line(x)
    add_line(left)
    add_line(right)
    grad_down(2, nx)
    add_line(across)

    ahead = pl.ds(0, experts // 2)
    ringed = len(ring) * plane
    only_wait(r.sending.at[pl.ds(0, experts - 1)], r.a_send.at[0]).wait_send()
    only_wait(r.back_out.at[pl.ds(0, experts - 1)], r.back_send.at[0]).wait_send()
    for way in (0, 1):
        only_wait(r.pack.at[pl.ds(0, ringed), :, :, columns(x)], r.own_send.at[way]).wait_send()
        only_wait(r.pack.at[pl.ds(0, ringed // 2), :, :, columns(x)], r.hand_send.at[way]).wait_send()
        only_wait(r.partial.at[ahead, :, columns(x)], r.half_send.at[way]).wait_send()
        only_wait(r.unit_out.at[way], r.unit_send.at[way]).wait_send()
        for kind in range(3):
            raw_step(kind, way, False).wait_send()
            grad_step(kind, way, False).wait_send()
    far = pl.ds(0, len(wide) * plane - 1)
    for kind in range(3):
        only_wait(r.pack.at[far, :, :, columns(x)], r.wide_send.at[kind]).wait_send()
    only_wait(r.near_links.at[pl.ds(0, plane - 1)], r.near_send.at[0]).wait_send()
    for t in range(nx):
        core_sum(t).wait_send()
        for way in (0, 1):
            line_half(t, way, False).wait_send()
            line_unit(t, way, False).wait_send()
    only_wait(r.far_links.at[pl.ds(0, nz - 1)], r.far_recv.at[0]).wait_recv()
    far_start = zero
    for q in range(nz - 1, -1, -1):
        a, b = r.far_links[q, 0:1, :], r.far_links[q, 1:2, :]
        far_start = jnp.where(q > z, b + a * far_start, far_start)
    incoming = near_start + near_weight * far_start
    state_grad = r.local_grad[...] + r.carry_weight[...] * incoming
    d_recur = (state_grad * r.by_recur[...]).astype(BF16)
    d_input = (state_grad * r.by_input[...]).astype(BF16)
    through = dot(d_recur, r.recur_map_in[0], 1, 1) + dot(d_input, r.input_map_in[0], 1, 1)
    r.conv_grad[...] = (state_grad * r.by_conv[...] + through).astype(BF16)

    only_wait(r.last_in.at[pl.ds(0, nz - 1)], r.last_recv.at[0]).wait_recv()
    total = r.last_out[z].astype(F32)
    for dz in range(1, nz):
        total = total + r.last_in[lax.rem(z + dz, nz)].astype(F32)
    r.proj_out[...] = total

    only_wait(r.far_links.at[pl.ds(0, nz - 1)], r.far_send.at[0]).wait_send()
    only_wait(r.last_out.at[pl.ds(0, nz - 1)], r.last_send.at[0]).wait_send()


HELD = ("ids", "weights", "mixer", "cot")
RECURRENCE = (
    "recur_gate", "decay_rate", "conv", "input_gate", "states", "gate_pre",
)
LOADED = (*HELD, *RECURRENCE, "w_gate", "w_up", "w_down", "out_proj", "recur_map", "input_map")
IN_NAMES = LOADED
OUT_NAMES = ("grad_gate", "grad_up", "grad_down", "proj_out", "conv_grad", "gate_grad")


def scratch_of(sizes, tokens, width, hidden, held):
    nz, ny, nc, nx = sizes
    plane = ny * nc
    experts = nz * plane
    capacity = 4 * tokens // experts
    features = nx * width
    lines = features // experts
    group = plane * capacity
    levels = tokens.bit_length() - 1
    dma = pltpu.SemaphoreType.DMA
    per_token = lambda kind: pltpu.VMEM((tokens, width), kind)
    shapes = {
        name + "_in": pltpu.VMEM(a.shape, a.dtype)
        for name, a in held.items()
        if name not in HELD[2:]
    }
    shapes |= dict(
        pack=pltpu.VMEM((experts, 2, capacity, features), BF16),
        raw=pltpu.VMEM((2, tokens, features), BF16),
        slot_weight=pltpu.VMEM((experts * capacity, 128), F32),
        wide=pltpu.VMEM((3, 3, plane, 2, capacity, width), BF16),
        sending=pltpu.VMEM((experts, 2, capacity, width), BF16),
        hits=pltpu.VMEM((experts * capacity, tokens), BF16),
        acc_gate=pltpu.VMEM((2 * group, hidden), F32),
        acc_up=pltpu.VMEM((2 * group, hidden), F32),
        acc_down=pltpu.VMEM((2 * group, hidden), F32),
        active=pltpu.VMEM((experts, capacity, hidden), BF16),
        d_gate=pltpu.VMEM((experts, capacity, hidden), BF16),
        d_up=pltpu.VMEM((experts, capacity, hidden), BF16),
        partial=pltpu.VMEM((experts, capacity, features), BF16),
        half_in=pltpu.VMEM((2, nz, plane // 2, capacity, width), BF16),
        unit_out=pltpu.VMEM((2, nz, plane, capacity, width), BF16),
        unit_in=pltpu.VMEM((2, nz, plane, capacity, width), BF16),
        back_out=pltpu.VMEM((experts, capacity, width), BF16),
        back_in=pltpu.VMEM((experts, capacity, width), BF16),
        out_grad=pltpu.VMEM((tokens, features), BF16),
        by_recur=per_token(F32),
        by_input=per_token(F32),
        by_conv=per_token(F32),
        by_gate=per_token(F32),
        gate=per_token(F32),
        mixed=per_token(BF16),
        first_decay=pltpu.VMEM((8, width), F32),
        reach=pltpu.VMEM((levels, tokens, width), F32),
        carry_weight=per_token(F32),
        d_mixed=per_token(F32),
        local_grad=per_token(F32),
        term=pltpu.VMEM((nz, ny, nc, lines, width), BF16),
        core_in=pltpu.VMEM((nz, ny, lines, width), BF16),
        core_out=pltpu.VMEM((nz, ny, lines, width), BF16),
        line_half=pltpu.VMEM((2, nx, lines, width), BF16),
        line_out=pltpu.VMEM((2, nz, lines, width), BF16),
        line_in=pltpu.VMEM((2, nz, lines, width), BF16),
        last_out=pltpu.VMEM((nz, lines, width), BF16),
        last_in=pltpu.VMEM((nz, lines, width), BF16),
        near_links=pltpu.VMEM((plane, 8, width), F32),
        far_links=pltpu.VMEM((nz, 8, width), F32),
        met=pltpu.SemaphoreType.REGULAR,
        load_sem=dma((len(held),)),
    )
    for name, (send, recv) in dict(
        a=((1,), (nz,)),
        own=((2,), (2, nz)),
        hand=((2,), (2, nz)),
        half=((2,), (2, nz)),
        unit=((2,), (2, nz)),
        back=((1,), (1,)),
        raw=((3, 2), (3, 2)),
        wide=((3,), (3, 3)),
        og=((3, 2), (3, 2)),
        near=((1,), (1,)),
        far=((1,), (1,)),
        core=((nx,), (nx,)),
        line=((4, nx), (4, nx)),
        last=((1,), (1,)),
    ).items():
        shapes[name + "_send"] = dma(send)
        shapes[name + "_recv"] = dma(recv)
    return shapes


SIZES = (8, 4, 2, 4)
SCRATCH_NAMES = tuple(
    scratch_of(SIZES, 128, 512, 256, {n: jax.ShapeDtypeStruct((8, 128), F32) for n in LOADED})
)


def layer(*loaded):
    sizes = tuple(lax.axis_size(a) for a in AXES)
    nz, ny, nc, nx = sizes
    named = dict(zip(LOADED, loaded, strict=True))
    tokens, width = loaded[3].shape
    hidden = named["w_gate"].shape[1]
    features = nx * width
    shapes = scratch_of(sizes, tokens, width, hidden, named)
    vmem = pl.BlockSpec(memory_space=pltpu.VMEM)
    left = pl.BlockSpec(memory_space=pltpu.HBM)
    return pl.pallas_call(
        functools.partial(layer_kernel, sizes),
        out_shape=tuple(
            pltpu.VMEM(shape, kind)
            for shape, kind in (
                ((features, hidden), BF16),
                ((features, hidden), BF16),
                ((hidden, features), BF16),
                ((features // (nz * ny * nc), width), F32),
                ((tokens, width), BF16),
                ((tokens, width), BF16),
            )
        ),
        in_specs=[left] * len(LOADED),
        out_specs=(vmem,) * len(OUT_NAMES),
        scratch_shapes=list(shapes.values()),
        compiler_params=pltpu.CompilerParams(
            collective_id=0, has_side_effects=True, vmem_limit_bytes=48 * 2**20
        ),
        name="layer",
    )(*(pltpu.with_memory_space_constraint(a, pltpu.HBM) for a in loaded))


def store_kernel(*refs):
    count = len(refs) // 2
    copies = [
        pltpu.make_async_copy(refs[k], refs[count + k], refs[-1].at[k]) for k in range(count)
    ]
    for copy in copies:
        copy.start()
    for copy in copies:
        copy.wait()


def stored(arrays):
    count = len(arrays)
    return pl.pallas_call(
        store_kernel,
        out_shape=tuple(jax.ShapeDtypeStruct(a.shape, a.dtype) for a in arrays),
        in_specs=[pl.BlockSpec(memory_space=pltpu.VMEM)] * count,
        out_specs=(pl.BlockSpec(memory_space=pl.ANY),) * count,
        scratch_shapes=[pltpu.SemaphoreType.DMA((count,))],
        name="store",
    )(*(pltpu.with_memory_space_constraint(a, pltpu.VMEM) for a in arrays))


def body(
    cotangent,
    mixer_out,
    route_ids,
    route_weights,
    conv_out,
    recur_gate,
    input_gate,
    gate_pre,
    states_before,
    decay_rate,
    out_proj,
    recur_map,
    input_map,
    expert_gate,
    expert_up,
    expert_down,
):
    grads = layer(
        route_ids.T,
        route_weights.T,
        mixer_out,
        cotangent,
        recur_gate,
        decay_rate[None, :],
        conv_out,
        input_gate,
        states_before,
        gate_pre,
        expert_gate[0],
        expert_up[0],
        expert_down[0],
        out_proj,
        recur_map,
        input_map,
    )
    grads = stored(grads)
    return (grads[0][None], grads[1][None], grads[2][None], *grads[3:])


def solution(mesh):
    torus = Mesh(mesh.devices.reshape(8, 4, 2, mesh.shape["tp"]), ("sp_0", "sp_1", "sp_2", "tp"))
    in_specs = (
        P(SP, "tp"),
        P(SP, "tp"),
        P(SP, None),
        P(SP, None),
        P(SP, "tp"),
        P(SP, "tp"),
        P(SP, "tp"),
        P(SP, "tp"),
        P(SP, "tp"),
        P("tp"),
        P(None, "tp"),
        P("tp", None, None),
        P("tp", None, None),
        P(SP, None, "tp"),
        P(SP, None, "tp"),
        P(SP, "tp", None),
    )
    out_specs = (
        P(SP, None, "tp"),
        P(SP, None, "tp"),
        P(SP, "tp", None),
        P(SP, "tp"),
        P(SP, "tp"),
        P(SP, "tp"),
    )
    return jax.shard_map(body, mesh=torus, in_specs=in_specs, out_specs=out_specs, check_vma=False)
```

```python
import functools
import types

import jax
import jax.numpy as jnp
from jax import lax
from jax.experimental import pallas as pl
from jax.experimental.pallas import tpu as pltpu
from jax.sharding import Mesh
from jax.sharding import PartitionSpec as P

SP = ("sp_0", "sp_1", "sp_2")
AXES = (*SP, "tp")
MESH_ID = pl.DeviceIdType.MESH
BF16 = jnp.bfloat16
F32 = jnp.float32


def near_first(count):
    return sorted(range(count), key=lambda k: (min(k, count - k), k))


def slot_hits(ids, experts, capacity):
    tokens = ids.shape[1]
    slots = experts * capacity
    first, second = ids[0:1, :], ids[1:2, :]
    expert = lax.broadcasted_iota(jnp.int32, (experts, tokens), 0)
    named = jnp.where((expert == first) | (expert == second), 1.0, 0.0).astype(jnp.bfloat16)
    at = lax.broadcasted_iota(jnp.int32, (tokens, tokens), 0)
    later = lax.broadcasted_iota(jnp.int32, (tokens, tokens), 1)
    earlier = jnp.where(at < later, 1.0, 0.0).astype(jnp.bfloat16)
    before = jnp.dot(named, earlier, preferred_element_type=jnp.float32)
    of_slot = lax.broadcasted_iota(jnp.int32, (slots, experts), 0)
    of_expert = lax.broadcasted_iota(jnp.int32, (slots, experts), 1)
    spread = jnp.where(of_slot // capacity == of_expert, 1.0, 0.0).astype(jnp.bfloat16)
    rank = jnp.dot(spread, before.astype(jnp.bfloat16), preferred_element_type=jnp.float32)
    slot = lax.broadcasted_iota(jnp.int32, (slots, tokens), 0)
    free = rank == (slot % capacity).astype(jnp.float32)
    return free & (slot // capacity == first), free & (slot // capacity == second)


def dot(left, right, at_left=1, at_right=0):
    return lax.dot_general(
        left, right, (((at_left,), (at_right,)), ((), ())), preferred_element_type=F32
    )


def expm1_of(v):
    series = jnp.ones_like(v)
    for n in range(11, 1, -1):
        series = 1.0 + v * series * (1.0 / n)
    return jnp.where(jnp.abs(v) < 0.5, v * series, jnp.exp(v) - 1.0)


def layer_kernel(sizes, *refs):
    names = IN_NAMES + OUT_NAMES + SCRATCH_NAMES
    r = types.SimpleNamespace(**dict(zip(names, refs, strict=True)))
    nz, ny, nc, nx = sizes
    plane = ny * nc
    experts = nz * plane
    z, y, c, x = (lax.axis_index(a) for a in AXES)
    tokens, width = r.mixed.shape
    capacity = r.sending.shape[2]
    me = (z * ny + y) * nc + c
    mine = y * nc + c
    right, left = lax.rem(x + 1, nx), lax.rem(x + nx - 1, nx)
    across = lax.rem(x + 2, nx)
    up, down = lax.rem(y + 1, ny), lax.rem(y + ny - 1, ny)
    over = lax.rem(y + 2, ny)
    twin = nc - 1 - c
    group = plane * capacity
    wide = [0, 1, nz - 1]
    ring = [dz for dz in near_first(nz) if dz not in wide]
    ring = ring[2:] + ring[:2]
    waits = []

    def columns(part):
        return pl.ds(pl.multiple_of(part * width, width), width)

    def partner(j, sign):
        dz, dy, dc = j // plane, (j // nc) % ny, j % nc
        return (
            lax.rem(z + sign * dz + nz, nz),
            lax.rem(y + sign * dy + ny, ny),
            lax.rem(c + sign * dc + nc, nc),
        )

    def remote(source, target, send, recv, device):
        return pltpu.make_async_remote_copy(
            src_ref=source,
            dst_ref=target,
            send_sem=send,
            recv_sem=recv,
            device_id=device,
            device_id_type=MESH_ID,
        )

    raw_own = [r.raw.at[k, :, columns(x)] for k in (0, 1)]
    places = [getattr(r, name + "_in", None) for name in LOADED]
    places[2:4] = raw_own
    loads = {
        name: pltpu.make_async_copy(getattr(r, name), places[k], r.load_sem.at[k])
        for k, name in enumerate(LOADED)
    }
    for name in LOADED:
        loads[name].start()

    barrier = pltpu.get_barrier_semaphore()

    def greet(sem, first, stop, step):
        def one(k, carry):
            pl.semaphore_signal(
                sem, inc=1, device_id=(*partner(k * step, 1), x), device_id_type=MESH_ID
            )
            return carry

        lax.fori_loop(first, stop, one, 0)

    greet(barrier, 1, nz, plane)
    greet(barrier, 1, plane, 1)
    for side in (left, right):
        pl.semaphore_signal(barrier, inc=1, device_id=(z, y, c, side), device_id_type=MESH_ID)

    for name in HELD:
        loads[name].wait()
    first, second = slot_hits(r.ids_in[...], experts, capacity)
    hits = jnp.where(first | second, 1.0, 0.0).astype(BF16)
    r.hits[...] = hits
    weights = r.weights_in[...]
    weight = jnp.sum(
        jnp.where(first, weights[0:1, :], 0.0) + jnp.where(second, weights[1:2, :], 0.0),
        axis=1,
        keepdims=True,
    )
    r.slot_weight[...] = jnp.broadcast_to(weight, r.slot_weight.shape)
    shape = (experts, capacity, width)
    r.sending[:, 0] = dot(hits, raw_own[0][...]).reshape(shape).astype(BF16)
    r.sending[:, 1] = (dot(hits, raw_own[1][...]) * weight).reshape(shape).astype(BF16)

    pl.semaphore_wait(barrier, nz - 1 + plane - 1 + 2)
    greet(r.met, 1, plane, 1)
    pl.semaphore_wait(r.met, plane - 1)

    def only_wait(like, sem):
        return remote(like, like, sem, sem, (z, y, twin, x))

    def sent(j):
        dz, dy, dc = partner(j, 1)
        return remote(
            r.sending.at[(dz * ny + dy) * nc + dc],
            r.pack.at[me, :, :, columns(x)],
            r.a_send.at[0],
            r.a_recv.at[j // plane],
            (dz, dy, dc, x),
        )

    sides = (left, right)
    others = (right, left)
    half_rows = tokens // 2

    def ring_gather(view, send, recv):
        def step(kind, way, arrives):
            half = 1 - way if kind == 1 else way
            if kind == 2:
                part = across if arrives else sides[way]
            else:
                part = sides[way] if arrives else x
            here = view(pl.ds(half * half_rows, half_rows), columns(part))
            return remote(
                here, here, send.at[kind, way], recv.at[kind, way],
                (z, y, c, sides[way] if arrives else others[way]),
            )

        return step

    raw_step = ring_gather(lambda rows, cols: r.raw.at[:, rows, cols], r.raw_send, r.raw_recv)
    for kind in (0, 1):
        for way in (0, 1):
            raw_step(kind, way, False).start()
    pltpu.make_async_copy(
        r.sending.at[me], r.pack.at[me, :, :, columns(x)], r.a_recv.at[0]
    ).start()
    for dz in (*ring, *wide):

        def send(j, carry):
            sent(j).start()
            return carry

        lax.fori_loop(max(dz * plane, 1), (dz + 1) * plane, send, 0)

    for name in RECURRENCE:
        loads[name].wait()
    recur = r.recur_gate_in[...].astype(F32)
    rate = r.decay_rate_in[...]
    log_decay = -8.0 * recur * rate
    decay = jnp.exp(log_decay)
    position = lax.broadcasted_iota(jnp.int32, (tokens, width), 0)
    at_start = (position + me * tokens) == 0
    norm = jnp.where(at_start, 1.0, jnp.sqrt(-expm1_of(2.0 * log_decay)))
    slope = jnp.where(at_start, 0.0, -jnp.exp(2.0 * log_decay) / norm)
    conv = r.conv_in[...].astype(F32)
    entry = r.input_gate_in[...].astype(F32)
    drive = entry * conv
    before = r.states_in[...].astype(F32)
    state = decay * before + norm * drive
    r.by_recur[...] = (
        (decay * before + slope * drive) * (-8.0 * rate) * recur * (1.0 - recur)
    )
    r.by_input[...] = norm * conv * entry * (1.0 - entry)
    r.by_conv[...] = norm * entry
    pre = r.gate_pre_in[...].astype(F32)
    root = 0.7978845608028654
    bent = jnp.tanh(root * (pre + 0.044715 * (pre * pre * pre)))
    cdf = 0.5 * (1.0 + bent)
    gate = pre * cdf
    gelu_slope = cdf + 0.5 * pre * (1.0 - bent * bent) * root * (1.0 + 3.0 * 0.044715 * (pre * pre))
    r.gate[...] = gate
    r.mixed[...] = (state * gate).astype(BF16)
    r.by_gate[...] = state * gelu_slope
    r.first_decay[...] = decay[0:8, :]
    following = pltpu.roll(decay, tokens - 1, 0)
    last = position == tokens - 1
    reach = jnp.where(last, 0.0, following)
    carry_weight = jnp.where(last, 1.0, following)
    step = 1
    level = 0
    while step < tokens:
        r.reach[level] = reach
        moved = pltpu.roll(reach, tokens - step, 0)
        reach = reach * moved
        moved = pltpu.roll(carry_weight, tokens - step, 0)
        carry_weight = carry_weight * jnp.where(position < tokens - step, moved, 1.0)
        step *= 2
        level += 1
    r.carry_weight[...] = carry_weight
    for name in LOADED:
        if name not in HELD + RECURRENCE:
            loads[name].wait()

    def send_wide(kind, part):
        cols = columns(part)
        for k, dz in enumerate(wide):
            to = lax.rem(z + dz, nz)
            slots = pl.ds(pl.multiple_of(to * group, group), group)
            picked = r.hits[slots, :]
            for side in (0, 1):
                value = dot(picked, r.raw[side, :, cols])
                if side:
                    value = value * r.slot_weight[slots, 0:1]
                r.wide[kind, k, :, side] = value.reshape(plane, capacity, width).astype(BF16)
            if dz == 0:
                pltpu.make_async_copy(
                    r.wide.at[kind, k, mine], r.pack.at[me, :, :, cols], r.wide_recv.at[kind, k]
                ).start()

            def give(j, carry):
                _, py, pc = partner(j, 1)
                remote(
                    r.wide.at[kind, k, py * nc + pc],
                    r.pack.at[me, :, :, cols],
                    r.wide_send.at[kind],
                    r.wide_recv.at[kind, k],
                    (to, py, pc, x),
                ).start()
                return carry

            lax.fori_loop(0 if dz else 1, plane, give, 0)

    def start_of(dz):
        return lax.rem(z - dz + nz, nz) * plane

    def ring_block(ref, dz, half, part):
        start, count = start_of(dz), plane
        if half is not None:
            count = plane // 2
            start = start + half * count
        return ref.at[pl.ds(start, count), ..., columns(part)]

    def own(dz, way, arrives):
        here = ring_block(r.pack, dz, None, sides[way] if arrives else x)
        return remote(
            here, here, r.own_send.at[way], r.own_recv.at[way, dz],
            (z, y, c, sides[way] if arrives else others[way]),
        )

    def passed(dz, way, arrives):
        here = ring_block(r.pack, dz, way, across if arrives else sides[way])
        return remote(
            here, here, r.hand_send.at[way], r.hand_recv.at[way, dz],
            (z, y, c, sides[way] if arrives else others[way]),
        )

    def hand_on(dz):
        for way in (0, 1):
            own(dz, way, True).wait_recv()
            passed(dz, way, False).start()

    def settle(dz):
        for way in (0, 1):
            passed(dz, way, True).wait_recv()

    def as_rows(kind, starts, cols):
        return jnp.concatenate(
            [r.pack[pl.ds(s, plane), kind, :, cols].reshape(group, -1) for s in starts], axis=0
        )

    def keep(ref, starts, cols, value):
        for k, s in enumerate(starts):
            part = value[k * group : (k + 1) * group]
            ref[pl.ds(s, plane), :, cols] = part.reshape(plane, capacity, -1).astype(BF16)

    def expert_rows(dzs):
        starts = [start_of(dz) for dz in dzs]
        size = pl.ds(0, len(dzs) * group)
        sums_of = [acc.at[size] for acc in (r.acc_gate, r.acc_up, r.acc_down)]
        for acc in sums_of:
            acc[...] = jnp.zeros(acc.shape, F32)

        def gather(t, carry):
            cols = columns(t)
            row_part = as_rows(0, starts, cols)
            sums_of[0][...] += dot(row_part, r.w_gate_in[cols, :])
            sums_of[1][...] += dot(row_part, r.w_up_in[cols, :])
            cot_part = as_rows(1, starts, cols)
            sums_of[2][...] += dot(cot_part, r.w_down_in[:, cols], 1, 1)
            return carry

        lax.fori_loop(0, nx, gather, 0, unroll=True)
        pre_gate, pre_up, d_active = (acc[...] for acc in sums_of)
        sig = jax.nn.sigmoid(pre_gate)
        silu = pre_gate * sig
        silu_slope = sig * (1.0 + pre_gate * (1.0 - sig))
        d_gate = d_active * pre_up * silu_slope
        d_up = d_active * silu
        whole = slice(None)
        keep(r.active, starts, whole, silu * pre_up)
        keep(r.d_gate, starts, whole, d_gate)
        keep(r.d_up, starts, whole, d_up)
        d_gate, d_up = d_gate.astype(BF16), d_up.astype(BF16)

        def spread(t, carry):
            cols = columns(t)
            value = dot(d_gate, r.w_gate_in[cols, :], 1, 1)
            value += dot(d_up, r.w_up_in[cols, :], 1, 1)
            keep(r.partial, starts, cols, value)
            return carry

        lax.fori_loop(0, nx, spread, 0, unroll=True)

    def half_sum(dz, way, arrives):
        return remote(
            ring_block(r.partial, dz, way, across),
            r.half_in.at[way, dz],
            r.half_send.at[way],
            r.half_recv.at[way, dz],
            (z, y, c, sides[way] if arrives else others[way]),
        )

    def unit_sum(dz, way, arrives):
        return remote(
            r.unit_out.at[way, dz],
            r.unit_in.at[way, dz],
            r.unit_send.at[way],
            r.unit_recv.at[way, dz],
            (z, y, c, sides[way] if arrives else others[way]),
        )

    def sum_one(dz):
        for way in (0, 1):
            half_sum(dz, way, False).start()

    def sum_two(dz):
        start = start_of(dz)
        for way in (0, 1):
            half_sum(dz, way, True).wait_recv()
            value = r.partial[pl.ds(start, plane), :, columns(others[way])].astype(F32)
            more = r.half_in[way, dz].astype(F32)
            half = plane // 2
            parts = [value[:half], value[half:]]
            parts[way] = parts[way] + more
            r.unit_out[way, dz] = jnp.concatenate(parts, axis=0).astype(BF16)
            unit_sum(dz, way, False).start()

    def returned(j):
        dz, dy, dc = partner(j, -1)
        return remote(
            r.back_out.at[(dz * ny + dy) * nc + dc],
            r.back_in.at[me],
            r.back_send.at[0],
            r.back_recv.at[0],
            (dz, dy, dc, x),
        )

    def back_local():
        return pltpu.make_async_copy(
            r.back_out.at[me], r.back_in.at[me], r.back_recv.at[0]
        )

    def sum_three(dz):
        start = start_of(dz)
        value = r.partial[pl.ds(start, plane), :, columns(x)].astype(F32)
        for way in (0, 1):
            unit_sum(dz, way, True).wait_recv()
            value = value + r.unit_in[way, dz].astype(F32)
        r.back_out[pl.ds(start, plane)] = value.astype(BF16)

        def give(j, carry):
            returned(j).start()
            return carry

        lax.fori_loop(max(dz * plane, 1), (dz + 1) * plane, give, 0)
        if dz == 0:
            back_local().start()

    chunks = [wide[:1], ring[0:2], ring[2:3], wide[1:], ring[3:]]

    def sums(stage, k):
        for dz in chunks[k] if k >= 0 else ():
            stage(dz)

    def rows_of(ref):
        return ref[...].reshape(experts * capacity, -1)

    def packed(kind, cols):
        return r.pack[:, kind, :, cols].reshape(experts * capacity, -1)

    def grad_in(slope_ref, grad_ref, begin, end):
        def part(t, carry):
            cols = columns(t)
            grad_ref[cols, :] = dot(packed(0, cols), rows_of(slope_ref), 0, 0).astype(BF16)
            return carry

        lax.fori_loop(begin, end, part, 0)

    def grad_down(begin, end):
        def part(t, carry):
            cols = columns(t)
            r.grad_down[:, cols] = dot(rows_of(r.active), packed(1, cols), 0, 0).astype(BF16)
            return carry

        lax.fori_loop(begin, end, part, 0)

    def arrived(dz):
        only_wait(ring_block(r.pack, dz, None, x), r.a_recv.at[dz]).wait_recv()
        if dz in wide:
            for kind, part in enumerate((left, right, across)):
                only_wait(ring_block(r.pack, dz, None, part), r.wide_recv.at[kind, wide.index(dz)]).wait_recv()
        else:
            for way in (0, 1):
                own(dz, way, False).start()

    def work(k):
        expert_rows(chunks[k])
        sums(sum_one, k)

    for way in (0, 1):
        raw_step(0, way, True).wait_recv()
        raw_step(2, way, False).start()
    for way in (0, 1):
        raw_step(1, way, True).wait_recv()
        send_wide(way, sides[way])
    arrived(ring[0])
    for way in (0, 1):
        raw_step(2, way, True).wait_recv()
    send_wide(2, across)
    arrived(ring[1])
    hand_on(ring[0])
    arrived(wide[0])
    work(0)
    arrived(ring[2])
    hand_on(ring[1])
    settle(ring[0])
    arrived(ring[3])
    hand_on(ring[2])
    settle(ring[1])
    arrived(ring[4])
    sums(sum_two, 0)
    expert_rows(chunks[1])
    hand_on(ring[3])
    sums(sum_one, 1)
    settle(ring[2])
    hand_on(ring[4])
    expert_rows(chunks[2])
    sums(sum_two, 1)
    sums(sum_one, 2)
    sums(sum_three, 0)
    for dz in wide[1:]:
        arrived(dz)
    work(3)
    settle(ring[3])
    settle(ring[4])
    work(4)
    sums(sum_three, 1)
    sums(sum_two, 2)
    sums(sum_two, 3)
    grad_in(r.d_gate, r.grad_gate, 0, 2)
    sums(sum_two, 4)
    sums(sum_three, 2)
    sums(sum_three, 3)
    grad_in(r.d_gate, r.grad_gate, 2, nx)
    sums(sum_three, 4)
    grad_in(r.d_up, r.grad_up, 0, nx)

    only_wait(r.back_in, r.back_recv.at[0]).wait_recv()
    routed = dot(r.hits[...], r.back_in[...].reshape(experts * capacity, width), 0, 0)
    r.out_grad[:, columns(x)] = (raw_own[1][...].astype(F32) + routed).astype(BF16)

    grad_step = ring_gather(lambda rows, cols: r.out_grad.at[rows, cols], r.og_send, r.og_recv)
    for kind in (0, 1):
        for way in (0, 1):
            grad_step(kind, way, False).start()

    lines = r.proj_out.shape[0]
    pair = nz // nx

    def planes(t):
        return pl.ds(t * pair, pair)

    def core_sum(t):
        return remote(
            r.term.at[planes(t), :, twin],
            r.core_in.at[planes(t)],
            r.core_send.at[t],
            r.core_recv.at[t],
            (z, y, twin, x),
        )

    def line_half(t, way, arrives):
        return remote(
            r.core_out.at[t * pair + way, over],
            r.line_half.at[way, t],
            r.line_send.at[way, t],
            r.line_recv.at[way, t],
            (z, (down, up)[way] if arrives else (up, down)[way], c, x),
        )

    def line_unit(t, way, arrives):
        return remote(
            r.line_out.at[way, planes(t)],
            r.line_in.at[way, planes(t)],
            r.line_send.at[2 + way, t],
            r.line_recv.at[2 + way, t],
            (z, (down, up)[way] if arrives else (up, down)[way], c, x),
        )

    def start_term(t):
        value = dot(r.out_grad[:, columns(t)], r.mixed[...], 0, 0)
        r.term[planes(t)] = value.reshape(pair, ny, nc, lines, width).astype(BF16)
        core_sum(t).start()

    def add_core(t):
        core_sum(t).wait_recv()
        for k in range(pair):
            row = t * pair + k
            value = r.term[row, :, pl.ds(c, 1)].reshape(ny, lines, width).astype(F32)
            r.core_out[row] = (value + r.core_in[row].astype(F32)).astype(BF16)
        for way in (0, 1):
            line_half(t, way, False).start()

    def add_half(t):
        for way in (0, 1):
            line_half(t, way, True).wait_recv()
            target = (up, down)[way]
            for k in range(pair):
                row = t * pair + k
                value = r.core_out[row, target].astype(F32)
                if k == way:
                    value = value + r.line_half[way, t].astype(F32)
                r.line_out[way, row] = value.astype(BF16)
            line_unit(t, way, False).start()

    def add_line(t):
        for way in (0, 1):
            line_unit(t, way, True).wait_recv()
        for k in range(pair):
            row = t * pair + k
            value = r.core_out[row, y].astype(F32)
            for way in (0, 1):
                value = value + r.line_in[way, row].astype(F32)
            r.last_out[row] = value.astype(BF16)

            @pl.when(row != z)
            def _():
                remote(
                    r.last_out.at[row],
                    r.last_in.at[z],
                    r.last_send.at[0],
                    r.last_recv.at[0],
                    (row, y, c, x),
                ).start()

    def mix(t):
        cols = columns(t)
        return dot(r.out_grad[:, cols], r.out_proj_in[cols, :])

    start_term(x)
    grad_down(0, 2)
    add_core(x)
    r.d_mixed[...] = mix(x)
    for way in (0, 1):
        grad_step(0, way, True).wait_recv()
        grad_step(2, way, False).start()
    add_half(x)
    for way in (0, 1):
        grad_step(1, way, True).wait_recv()
        start_term(sides[way])
    r.d_mixed[...] += mix(left) + mix(right)
    add_core(left)
    add_core(right)
    for way in (0, 1):
        grad_step(2, way, True).wait_recv()
    start_term(across)

    d_mixed = r.d_mixed[...] + mix(across)
    r.gate_grad[...] = (d_mixed * r.by_gate[...]).astype(BF16)
    local_grad = d_mixed * r.gate[...]
    step, level = 1, 0
    while step < tokens:
        local_grad = local_grad + r.reach[level] * pltpu.roll(local_grad, tokens - step, 0)
        step *= 2
        level += 1
    r.local_grad[...] = local_grad
    head = r.first_decay[0:1, :]
    link = jnp.concatenate(
        [
            head * r.carry_weight[0:1, :],
            head * local_grad[0:1, :],
            jnp.zeros((6, width), F32),
        ],
        axis=0,
    )
    r.near_links[mine] = link

    def near_link(j):
        _, py, pc = partner(j, 1)
        here = r.near_links.at[mine]
        return remote(here, here, r.near_send.at[0], r.near_recv.at[0], (z, py, pc, x))

    for j in range(1, plane):
        near_link(j).start()
    add_core(across)
    add_half(left)
    add_half(right)
    add_half(across)

    only_wait(r.near_links.at[pl.ds(0, plane - 1)], r.near_recv.at[0]).wait_recv()
    one, zero = jnp.ones((1, width), F32), jnp.zeros((1, width), F32)
    all_weight, all_start, near_weight, near_start = one, zero, one, zero
    for q in range(plane - 1, -1, -1):
        a, b = r.near_links[q, 0:1, :], r.near_links[q, 1:2, :]
        all_weight, all_start = a * all_weight, b + a * all_start
        later = q > mine
        near_start = jnp.where(later, b + a * near_start, near_start)
        near_weight = jnp.where(later, a * near_weight, near_weight)
    r.far_links[z] = jnp.concatenate(
        [all_weight, all_start, jnp.zeros((6, width), F32)], axis=0
    )

    def far_link(dz):
        pz, _, _ = partner(dz * plane, 1)
        here = r.far_links.at[z]
        return remote(here, here, r.far_send.at[0], r.far_recv.at[0], (pz, y, c, x))

    for dz in range(1, nz):
        far_link(dz).start()
    add_line(x)
    add_line(left)
    add_line(right)
    grad_down(2, nx)
    add_line(across)

    ahead = pl.ds(0, experts // 2)
    ringed = len(ring) * plane
    only_wait(r.sending.at[pl.ds(0, experts - 1)], r.a_send.at[0]).wait_send()
    only_wait(r.back_out.at[pl.ds(0, experts - 1)], r.back_send.at[0]).wait_send()
    for way in (0, 1):
        only_wait(r.pack.at[pl.ds(0, ringed), :, :, columns(x)], r.own_send.at[way]).wait_send()
        only_wait(r.pack.at[pl.ds(0, ringed // 2), :, :, columns(x)], r.hand_send.at[way]).wait_send()
        only_wait(r.partial.at[ahead, :, columns(x)], r.half_send.at[way]).wait_send()
        only_wait(r.unit_out.at[way], r.unit_send.at[way]).wait_send()
        for kind in range(3):
            raw_step(kind, way, False).wait_send()
            grad_step(kind, way, False).wait_send()
    far = pl.ds(0, len(wide) * plane - 1)
    for kind in range(3):
        only_wait(r.pack.at[far, :, :, columns(x)], r.wide_send.at[kind]).wait_send()
    only_wait(r.near_links.at[pl.ds(0, plane - 1)], r.near_send.at[0]).wait_send()
    for t in range(nx):
        core_sum(t).wait_send()
        for way in (0, 1):
            line_half(t, way, False).wait_send()
            line_unit(t, way, False).wait_send()
    only_wait(r.far_links.at[pl.ds(0, nz - 1)], r.far_recv.at[0]).wait_recv()
    far_start = zero
    for q in range(nz - 1, -1, -1):
        a, b = r.far_links[q, 0:1, :], r.far_links[q, 1:2, :]
        far_start = jnp.where(q > z, b + a * far_start, far_start)
    incoming = near_start + near_weight * far_start
    state_grad = r.local_grad[...] + r.carry_weight[...] * incoming
    d_recur = (state_grad * r.by_recur[...]).astype(BF16)
    d_input = (state_grad * r.by_input[...]).astype(BF16)
    through = dot(d_recur, r.recur_map_in[0], 1, 1) + dot(d_input, r.input_map_in[0], 1, 1)
    r.conv_grad[...] = (state_grad * r.by_conv[...] + through).astype(BF16)

    only_wait(r.last_in.at[pl.ds(0, nz - 1)], r.last_recv.at[0]).wait_recv()
    total = r.last_out[z].astype(F32)
    for dz in range(1, nz):
        total = total + r.last_in[lax.rem(z + dz, nz)].astype(F32)
    r.proj_out[...] = total

    only_wait(r.far_links.at[pl.ds(0, nz - 1)], r.far_send.at[0]).wait_send()
    only_wait(r.last_out.at[pl.ds(0, nz - 1)], r.last_send.at[0]).wait_send()


HELD = ("ids", "weights", "mixer", "cot")
RECURRENCE = (
    "recur_gate", "decay_rate", "conv", "input_gate", "states", "gate_pre",
)
LOADED = (*HELD, *RECURRENCE, "w_gate", "w_up", "w_down", "out_proj", "recur_map", "input_map")
IN_NAMES = LOADED
OUT_NAMES = ("grad_gate", "grad_up", "grad_down", "proj_out", "conv_grad", "gate_grad")


def scratch_of(sizes, tokens, width, hidden, held):
    nz, ny, nc, nx = sizes
    plane = ny * nc
    experts = nz * plane
    capacity = 4 * tokens // experts
    features = nx * width
    lines = features // experts
    group = plane * capacity
    levels = tokens.bit_length() - 1
    dma = pltpu.SemaphoreType.DMA
    per_token = lambda kind: pltpu.VMEM((tokens, width), kind)
    shapes = {
        name + "_in": pltpu.VMEM(a.shape, a.dtype)
        for name, a in held.items()
        if name not in HELD[2:]
    }
    shapes |= dict(
        pack=pltpu.VMEM((experts, 2, capacity, features), BF16),
        raw=pltpu.VMEM((2, tokens, features), BF16),
        slot_weight=pltpu.VMEM((experts * capacity, 128), F32),
        wide=pltpu.VMEM((3, 3, plane, 2, capacity, width), BF16),
        sending=pltpu.VMEM((experts, 2, capacity, width), BF16),
        hits=pltpu.VMEM((experts * capacity, tokens), BF16),
        acc_gate=pltpu.VMEM((2 * group, hidden), F32),
        acc_up=pltpu.VMEM((2 * group, hidden), F32),
        acc_down=pltpu.VMEM((2 * group, hidden), F32),
        active=pltpu.VMEM((experts, capacity, hidden), BF16),
        d_gate=pltpu.VMEM((experts, capacity, hidden), BF16),
        d_up=pltpu.VMEM((experts, capacity, hidden), BF16),
        partial=pltpu.VMEM((experts, capacity, features), BF16),
        half_in=pltpu.VMEM((2, nz, plane // 2, capacity, width), BF16),
        unit_out=pltpu.VMEM((2, nz, plane, capacity, width), BF16),
        unit_in=pltpu.VMEM((2, nz, plane, capacity, width), BF16),
        back_out=pltpu.VMEM((experts, capacity, width), BF16),
        back_in=pltpu.VMEM((experts, capacity, width), BF16),
        out_grad=pltpu.VMEM((tokens, features), BF16),
        by_recur=per_token(F32),
        by_input=per_token(F32),
        by_conv=per_token(F32),
        by_gate=per_token(F32),
        gate=per_token(F32),
        mixed=per_token(BF16),
        first_decay=pltpu.VMEM((8, width), F32),
        reach=pltpu.VMEM((levels, tokens, width), F32),
        carry_weight=per_token(F32),
        d_mixed=per_token(F32),
        local_grad=per_token(F32),
        term=pltpu.VMEM((nz, ny, nc, lines, width), BF16),
        core_in=pltpu.VMEM((nz, ny, lines, width), BF16),
        core_out=pltpu.VMEM((nz, ny, lines, width), BF16),
        line_half=pltpu.VMEM((2, nx, lines, width), BF16),
        line_out=pltpu.VMEM((2, nz, lines, width), BF16),
        line_in=pltpu.VMEM((2, nz, lines, width), BF16),
        last_out=pltpu.VMEM((nz, lines, width), BF16),
        last_in=pltpu.VMEM((nz, lines, width), BF16),
        near_links=pltpu.VMEM((plane, 8, width), F32),
        far_links=pltpu.VMEM((nz, 8, width), F32),
        met=pltpu.SemaphoreType.REGULAR,
        load_sem=dma((len(held),)),
    )
    for name, (send, recv) in dict(
        a=((1,), (nz,)),
        own=((2,), (2, nz)),
        hand=((2,), (2, nz)),
        half=((2,), (2, nz)),
        unit=((2,), (2, nz)),
        back=((1,), (1,)),
        raw=((3, 2), (3, 2)),
        wide=((3,), (3, 3)),
        og=((3, 2), (3, 2)),
        near=((1,), (1,)),
        far=((1,), (1,)),
        core=((nx,), (nx,)),
        line=((4, nx), (4, nx)),
        last=((1,), (1,)),
    ).items():
        shapes[name + "_send"] = dma(send)
        shapes[name + "_recv"] = dma(recv)
    return shapes


SIZES = (8, 4, 2, 4)
SCRATCH_NAMES = tuple(
    scratch_of(SIZES, 128, 512, 256, {n: jax.ShapeDtypeStruct((8, 128), F32) for n in LOADED})
)


def layer(*loaded):
    sizes = tuple(lax.axis_size(a) for a in AXES)
    nz, ny, nc, nx = sizes
    named = dict(zip(LOADED, loaded, strict=True))
    tokens, width = loaded[3].shape
    hidden = named["w_gate"].shape[1]
    features = nx * width
    shapes = scratch_of(sizes, tokens, width, hidden, named)
    vmem = pl.BlockSpec(memory_space=pltpu.VMEM)
    left = pl.BlockSpec(memory_space=pltpu.HBM)
    return pl.pallas_call(
        functools.partial(layer_kernel, sizes),
        out_shape=tuple(
            pltpu.VMEM(shape, kind)
            for shape, kind in (
                ((features, hidden), BF16),
                ((features, hidden), BF16),
                ((hidden, features), BF16),
                ((features // (nz * ny * nc), width), F32),
                ((tokens, width), BF16),
                ((tokens, width), BF16),
            )
        ),
        in_specs=[left] * len(LOADED),
        out_specs=(vmem,) * len(OUT_NAMES),
        scratch_shapes=list(shapes.values()),
        compiler_params=pltpu.CompilerParams(
            collective_id=0, has_side_effects=True, vmem_limit_bytes=48 * 2**20
        ),
        name="layer",
    )(*(pltpu.with_memory_space_constraint(a, pltpu.HBM) for a in loaded))


def store_kernel(*refs):
    count = len(refs) // 2
    copies = [
        pltpu.make_async_copy(refs[k], refs[count + k], refs[-1].at[k]) for k in range(count)
    ]
    for copy in copies:
        copy.start()
    for copy in copies:
        copy.wait()


def stored(arrays):
    count = len(arrays)
    return pl.pallas_call(
        store_kernel,
        out_shape=tuple(jax.ShapeDtypeStruct(a.shape, a.dtype) for a in arrays),
        in_specs=[pl.BlockSpec(memory_space=pltpu.VMEM)] * count,
        out_specs=(pl.BlockSpec(memory_space=pl.ANY),) * count,
        scratch_shapes=[pltpu.SemaphoreType.DMA((count,))],
        name="store",
    )(*(pltpu.with_memory_space_constraint(a, pltpu.VMEM) for a in arrays))


def body(
    cotangent,
    mixer_out,
    route_ids,
    route_weights,
    conv_out,
    recur_gate,
    input_gate,
    gate_pre,
    states_before,
    decay_rate,
    out_proj,
    recur_map,
    input_map,
    expert_gate,
    expert_up,
    expert_down,
):
    grads = layer(
        route_ids.T,
        route_weights.T,
        mixer_out,
        cotangent,
        recur_gate,
        decay_rate[None, :],
        conv_out,
        input_gate,
        states_before,
        gate_pre,
        expert_gate[0],
        expert_up[0],
        expert_down[0],
        out_proj,
        recur_map,
        input_map,
    )
    grads = stored(grads)
    return (grads[0][None], grads[1][None], grads[2][None], *grads[3:])


def solution(mesh):
    torus = Mesh(mesh.devices.reshape(8, 4, 2, mesh.shape["tp"]), ("sp_0", "sp_1", "sp_2", "tp"))
    in_specs = (
        P(SP, "tp"),
        P(SP, "tp"),
        P(SP, None),
        P(SP, None),
        P(SP, "tp"),
        P(SP, "tp"),
        P(SP, "tp"),
        P(SP, "tp"),
        P(SP, "tp"),
        P("tp"),
        P(None, "tp"),
        P("tp", None, None),
        P("tp", None, None),
        P(SP, None, "tp"),
        P(SP, None, "tp"),
        P(SP, "tp", None),
    )
    out_specs = (
        P(SP, None, "tp"),
        P(SP, None, "tp"),
        P(SP, "tp", None),
        P(SP, "tp"),
        P(SP, "tp"),
        P(SP, "tp"),
    )
    return jax.shard_map(body, mesh=torus, in_specs=in_specs, out_specs=out_specs, check_vma=False)
```
